32 devices in a mesh: grp: 2 (over y), sp: 4 (over z), tp: 4 (over x, core).
Axes of the slice: x: 2, y: 2, z: 4, core: 2. Of those that a mesh axis runs over, the one named last changes fastest.
Arguments:
- tokens_in: bfloat16 [2048, 2048], P(('grp', 'sp'), 'tp'), parts along dimension 0, may hold values from -6 to 6
- norm_gain: float32 [3, 2048], replicated, may hold values from 0.1 to 1.9
- w_pool_in: bfloat16 [3, 2048, 1024], P(None, 'sp', 'tp'), may hold values from -0.125 to 0.125
- w_gate: bfloat16 [3, 2048, 2048], P(None, 'sp', 'tp'), may hold values from -0.125 to 0.125
- w_back: bfloat16 [3, 1024, 2048], P(None, 'tp', 'sp'), may hold values from -0.25 to 0.25
Outputs:
- tokens_out: bfloat16 [2048, 2048], P(('grp', 'sp'), 'tp'), parts along dimension 0
The draws below stay inside these ranges and needn't reach their ends.
There are 2 independent parts, one for each index of `grp`. The reference program is written for one: setup_inputs(seed, part) draws one part's arguments, and reference() takes and returns one part's arrays. A program takes and returns all parts, laid end to end along the dimension named above; an argument that names none is the same for every part. Nothing has to cross between parts.
All inputs are finite; a program needn't handle non-finite values.
Results may differ from the reference program's by a relative error of at most 0.017.
Values may be sent and summed in bfloat16 or wider, within the bound.
A program may use at most 64 MiB of HBM per device.

```python
import jax
import jax.numpy as jnp
from jax import lax

D = 2048
POOL_WIDTH = 1024
GROUPS = 4
GRID_W = 32
LAYERS = 3
TOKENS = 1024
N_TP = 4


def spiked(drawn, key, source, target, blocks, factor):
    def block_of(axis_at):
        return (jnp.arange(drawn.shape[axis_at]) // (drawn.shape[axis_at] // blocks)).reshape((-1,) + (1,) * (drawn.ndim - 1 - axis_at))

    near = jax.random.permutation(key, blocks)[block_of(target)]
    second = (block_of(target) + blocks // 2) % blocks
    return jnp.where((block_of(source) == near) | (block_of(source) == second), factor * drawn, drawn)


def shard_levels(own_key, shape, shards, smallest, top_value):
    loudness = 1.0
    for axis_at, shards_of in shards:
        heights = jax.random.uniform(jax.random.fold_in(jax.random.fold_in(own_key, 6), axis_at), (shards_of,), jnp.float32, smallest / len(shards), top_value / len(shards))
        loudness = loudness * jnp.repeat(jnp.exp(heights), shape[axis_at] // shards_of).reshape((-1,) + (1,) * (len(shape) - 1 - axis_at))
    return loudness


def normal_values(rng, dims, deviation, most, cuts=(), kind=jnp.bfloat16):
    array = jax.random.normal(rng, dims, jnp.float32) * deviation
    if len(cuts) > 0:
        array = shard_levels(rng, dims, cuts, -0.22, 0.18) * array
    return jnp.clip(array, min=-most, max=most).astype(kind)


def heavy_noise(stream_key, extent, width, bound, cuts, heavy, kind=jnp.bfloat16):
    drawn = width * jax.random.normal(stream_key, extent, jnp.float32)
    if cuts:
        drawn = drawn * shard_levels(stream_key, extent, cuts, -0.22, 0.18)
    return jnp.clip(spiked(drawn, jax.random.fold_in(stream_key, 3), *heavy), -bound, bound).astype(kind)


def setup_inputs(seed: int = 0, part: int = 0) -> dict:
    arg_keys = jax.random.split(jax.random.key(seed), 6)
    part_splits = jax.random.split(jax.random.fold_in(arg_keys[5], part), 6)
    return {
        "tokens_in": normal_values(part_splits[0], (TOKENS, D), 1.0, 6.0, ((0, 4), (1, 4))),
        "norm_gain": jnp.clip(1.0 + 0.18 * jax.random.normal(arg_keys[1], (LAYERS, D), jnp.float32), 0.1, 1.9),
        "w_pool_in": normal_values(arg_keys[2], (LAYERS, D, POOL_WIDTH), D ** -0.5, 0.125, ((1, 4), (2, 4))),
        "w_gate": normal_values(arg_keys[3], (LAYERS, D, D), D ** -0.5, 0.125, ((1, 4), (2, 4))),
        "w_back": heavy_noise(arg_keys[4], (LAYERS, POOL_WIDTH, D), POOL_WIDTH ** -0.5, 0.25, ((1, 4), (2, 4)), (1, 2, 4, 2.0)),
    }


pool_windows = (2, 4, 8, 16)
norm_eps = 1e-06

def window_means(padded, rows_here, first_row, total_rows, window):
    reach = max(pool_windows) // 2
    half_span = window // 2
    width_cols = padded.shape[1] - 2 * reach
    row_sums = padded[reach - half_span:reach - half_span + rows_here]
    for offset in range(1 - half_span, half_span):
        row_sums = row_sums + padded[reach + offset:reach + offset + rows_here]
    box_sums = row_sums[:, reach - half_span:reach - half_span + width_cols]
    for offset in range(1 - half_span, half_span):
        box_sums = box_sums + row_sums[:, reach + offset:reach + offset + width_cols]
    row_index = first_row + jnp.arange(rows_here, dtype=jnp.int32)
    col_index = jnp.arange(width_cols, dtype=jnp.int32)
    row_counts = jnp.minimum(row_index + half_span, total_rows) - jnp.maximum(row_index - half_span, 0)
    col_counts = jnp.minimum(col_index + half_span, width_cols) - jnp.maximum(col_index - half_span, 0)
    counts = (row_counts[:, None] * col_counts[None, :]).astype(jnp.float32)
    return box_sums / counts[:, :, None]

def reference(tokens_in, norm_gain, w_pool_in, w_gate, w_back):
    reach = max(pool_windows) // 2
    group_width = POOL_WIDTH // GROUPS
    total_rows = TOKENS // GRID_W
    block_width = POOL_WIDTH // N_TP
    state = tokens_in
    for layer_id in range(LAYERS):
        wide = state.astype(jnp.float32)
        normed = (wide * lax.rsqrt(lax.optimization_barrier(jnp.mean(wide * wide, axis=-1, keepdims=True)) + norm_eps) * norm_gain[layer_id]).astype(jnp.bfloat16)
        pool_in = jnp.dot(normed, w_pool_in[layer_id], preferred_element_type=jnp.float32).astype(jnp.bfloat16)
        gate = jax.nn.sigmoid(jnp.dot(normed, w_gate[layer_id], preferred_element_type=jnp.float32))
        cells = pool_in.astype(jnp.float32).reshape(total_rows, GRID_W, POOL_WIDTH)
        padded = jnp.pad(cells, ((reach, reach), (reach, reach), (0, 0)))
        pieces = []
        for group_id in range(GROUPS):
            chosen = padded[:, :, group_id * group_width:(group_id + 1) * group_width]
            pieces.append(window_means(chosen, total_rows, 0, total_rows, pool_windows[group_id]))
        means = jnp.concatenate(pieces, axis=2)
        pooled = (means - cells).reshape(TOKENS, POOL_WIDTH).astype(jnp.bfloat16)
        branch = jnp.zeros((TOKENS, D), jnp.float32)
        for block_id in range(N_TP):
            lower = block_id * block_width
            partial_value = jnp.dot(pooled[:, lower:lower + block_width], w_back[layer_id][lower:lower + block_width], preferred_element_type=jnp.float32).astype(jnp.bfloat16)
            branch = branch + lax.optimization_barrier(partial_value).astype(jnp.float32)
        state = (wide + gate * branch).astype(jnp.bfloat16)
    return state
```

```python
import jax
import jax.numpy as jnp
from jax import lax
from jax.experimental import pallas as pl
from jax.experimental.pallas import tpu as pltpu
from jax.sharding import PartitionSpec as P
import functools

POOL_WIDTH = 1024
GROUPS = 4
GRID_W = 32
LAYERS = 3


pool_windows = (2, 4, 8, 16)
norm_eps = 1e-06


def padded_2(value, sides, width):
    for axis, dim in sides:
        peers, length = (lax.axis_size(axis), value.shape[dim])
        up = [(i, (i + 1) % peers) for i in range(peers - 1)]
        down = [(j, i) for i, j in up]
        last = lax.slice_in_dim(value, length - width, length, axis=dim)
        initial = lax.slice_in_dim(value, 0, width, axis=dim)
        before = lax.ppermute(last, axis, up)
        after = lax.ppermute(initial, axis, down)
        value = jnp.concatenate([before, value, after], axis=dim)
    return value


def window_means(padded, rows_here, first_row, total_rows, window):
    reach = max(pool_windows) // 2
    half_span = window // 2
    width_cols = padded.shape[1] - 2 * reach
    row_sums = padded[reach - half_span : reach - half_span + rows_here]
    for offset in range(1 - half_span, half_span):
        row_sums = row_sums + padded[reach + offset : reach + offset + rows_here]
    box_sums = row_sums[:, reach - half_span : reach - half_span + width_cols]
    for offset in range(1 - half_span, half_span):
        box_sums = box_sums + row_sums[:, reach + offset : reach + offset + width_cols]
    row_index = first_row + jnp.arange(rows_here, dtype=jnp.int32)
    col_index = jnp.arange(width_cols, dtype=jnp.int32)
    row_counts = jnp.minimum(row_index + half_span, total_rows) - jnp.maximum(
        row_index - half_span, 0
    )
    col_counts = jnp.minimum(col_index + half_span, width_cols) - jnp.maximum(
        col_index - half_span, 0
    )
    counts = (row_counts[:, None] * col_counts[None, :]).astype(jnp.float32)
    return box_sums / counts[:, :, None]


def on_device(tokens_in, norm_gain, w_pool_in, w_gate, w_back):
    reach = max(pool_windows) // 2
    sp_count = lax.axis_size("sp")
    tp_count = lax.axis_size("tp")
    tp_pos = lax.axis_index("tp")
    sp_pos = lax.axis_index("sp")
    tok_rows = tokens_in.shape[0]
    rows_here = tok_rows // GRID_W
    total_rows = rows_here * sp_count
    first_row = sp_pos * rows_here
    local_pool = w_pool_in.shape[2]
    group_width = POOL_WIDTH // GROUPS
    channel_group = (tp_pos * local_pool + jnp.arange(local_pool, dtype=jnp.int32)) // group_width
    state = tokens_in
    for layer_id in range(LAYERS):
        whole_rows = lax.all_gather(state, "tp", axis=1, tiled=True)
        wide = whole_rows.astype(jnp.float32)
        normed = (
            wide
            * lax.rsqrt(jnp.mean(wide * wide, axis=-1, keepdims=True) + norm_eps)
            * norm_gain[layer_id]
        ).astype(jnp.bfloat16)
        pool_acc = jnp.dot(
            normed,
            lax.all_gather(w_pool_in[layer_id], "sp", axis=0, tiled=True),
            preferred_element_type=jnp.float32,
        )
        gate_acc = jnp.dot(
            normed,
            lax.all_gather(w_gate[layer_id], "sp", axis=0, tiled=True),
            preferred_element_type=jnp.float32,
        )
        pool_in = pool_acc.astype(jnp.bfloat16)
        gate = jax.nn.sigmoid(gate_acc)
        cells = pool_in.reshape(rows_here, GRID_W, local_pool)
        rimmed = padded_2(cells, (("sp", 0),), reach)
        padded = jnp.pad(rimmed.astype(jnp.float32), ((0, 0), (reach, reach), (0, 0)))
        means = jnp.zeros((rows_here, GRID_W, local_pool), jnp.float32)
        for group_id in range(GROUPS):
            in_group = (channel_group == group_id)[None, None, :]
            means = jnp.where(
                in_group,
                window_means(padded, rows_here, first_row, total_rows, pool_windows[group_id]),
                means,
            )
        pooled = (
            (means - cells.astype(jnp.float32)).reshape(tok_rows, local_pool).astype(jnp.bfloat16)
        )
        full_pooled = lax.all_gather(pooled, "tp", axis=1, tiled=True)
        back_rows = lax.all_gather(w_back[layer_id], "sp", axis=1, tiled=True)
        back_cols = lax.all_to_all(back_rows, "tp", split_axis=1, concat_axis=0, tiled=True)
        partials = jnp.einsum(
            "tnb,nbd->ntd",
            full_pooled.reshape(tok_rows, tp_count, local_pool),
            back_cols.reshape(tp_count, local_pool, back_cols.shape[1]),
            preferred_element_type=jnp.float32,
        ).astype(jnp.bfloat16)
        branch = jnp.sum(partials.astype(jnp.float32), axis=0)
        state = (state.astype(jnp.float32) + gate * branch).astype(jnp.bfloat16)
    return state


MESH = pl.DeviceIdType.MESH
POOL, GATE_A, GATE_B, BACK = range(4)
UNITS = {POOL: (0,), GATE_A: (1,), GATE_B: (2,), BACK: (3, 4)}
CHUNKS = 2
GUEST = LAYERS


def fused_kernel(
    sp_count, tp_count,
    tok_hbm, gain_ref, wp_hbm, wg_hbm, wb_hbm, out_ref,
    wp, wg, wb, wb_own, gathered, scaled, halo, gate_buf, own_part, box, counts,
    pair, parts, arrived, returned,
    load_sem, w_send, w_recv, bx_send, bx_recv, tk_send, tk_recv, rt_send, rt_recv,
    ag_send, ag_recv, h_send, h_recv, px_send, px_recv, rs_send, rs_recv,
):
    g = lax.axis_index("grp")
    s = lax.axis_index("sp")
    t = lax.axis_index("tp")
    other = 1 - g
    c = t % 2
    base = t - c
    t1 = base + 1 - c
    t2 = (t + 2) % tp_count
    t3 = (t1 + 2) % tp_count
    far_base = (base + 2) % tp_count
    last = sp_count - 1
    toks, feats = tok_hbm.shape
    local_pool = wp.shape[2]
    cols_k = feats // CHUNKS
    rows_here = toks // GRID_W
    total_rows = rows_here * sp_count
    bf, f32 = jnp.bfloat16, jnp.float32

    low = s < 2
    is_mid = jnp.logical_and(s > 0, s < last)
    is_end = jnp.logical_not(is_mid)
    end_here = jnp.where(low, 0, last)
    mid_here = jnp.where(low, 1, last - 1)
    end_far = last - end_here
    mid_far = last - mid_here
    blocks = (
        jnp.where(is_mid, end_here, mid_here),
        jnp.where(is_mid, mid_far, mid_far),
        end_far,
    )
    s_parity = s % 2

    p_rows, g_rows = wp_hbm.shape[1], wg_hbm.shape[1]
    b_rows = wb_hbm.shape[1]

    def view(layer, block, half, unit, row=None):
        if unit == 0:
            n = p_rows // 2
            return wp.at[layer, pl.ds(pl.multiple_of(block * p_rows + half * n, n), n), :]
        if unit in (1, 2):
            n = g_rows // 4
            at = block * g_rows + half * (2 * n) + (unit - 1) * n
            return wg.at[layer, pl.ds(pl.multiple_of(at, n), n), :]
        n = b_rows // 2
        row = unit - 3 if row is None else row
        return wb.at[layer, block // 2, pl.ds(pl.multiple_of(row * b_rows + half * n, n), n), :]

    def w_copy(layer, flow, block, half, unit, target):
        ref = view(layer, block, half, unit)
        return pltpu.make_async_remote_copy(
            src_ref=ref, dst_ref=ref,
            send_sem=w_send.at[layer, flow, unit], recv_sem=w_recv.at[layer, block, half, unit],
            device_id=target, device_id_type=MESH,
        )

    def own_copy(layer, flow, half, piece, plane):
        if piece != BACK:
            return w_copy(layer, flow, s, half, UNITS[piece][0], {"sp": plane})
        n = b_rows // 2
        return pltpu.make_async_remote_copy(
            src_ref=wb_own.at[layer, pl.ds(pl.multiple_of(half * n, n), n), :],
            dst_ref=view(layer, s, half, 3, row=c),
            send_sem=w_send.at[layer, flow, 3], recv_sem=w_recv.at[layer, s, half, 3 + c],
            device_id={"sp": plane, "tp": base + s_parity}, device_id_type=MESH,
        )

    def near_copy(layer, block, unit):
        target = {"grp": jnp.where(is_mid, g, other), "sp": jnp.where(is_mid, mid_far, s)}
        return w_copy(layer, 2, block, g, unit, target)

    def across_copy(layer, k, block, unit):
        return w_copy(layer, 2 + k, block, g, unit, {"grp": other})

    def outer_copy(layer, k, block, unit):
        return w_copy(layer, 4 + k, block, g, unit, {"sp": end_here})

    def holds(block, piece, fn):
        if piece == BACK:
            pl.when(c == block % 2)(fn)
        else:
            fn()

    def pump(layer, k, *pieces):
        block = blocks[k]
        for piece in pieces:
            def act(piece=piece):
                for unit in UNITS[piece]:
                    w_copy(layer, 0, block, g, unit, {"grp": other}).wait_recv()
                    if k == 0:
                        near_copy(layer, block, unit).start()
                    else:
                        across_copy(layer, k, block, unit).start()

                        @pl.when(jnp.logical_and(is_mid, layer > 0))
                        def _(unit=unit):
                            outer_copy(layer, k, block, unit).start()
            holds(block, piece, act)

    def bx_copy(layer):
        return pltpu.make_async_remote_copy(
            src_ref=wb_own.at[layer],
            dst_ref=wb.at[layer, s // 2, pl.ds(pl.multiple_of(c * b_rows, b_rows), b_rows), :],
            send_sem=bx_send.at[layer], recv_sem=bx_recv.at[layer],
            device_id={"tp": t1}, device_id_type=MESH,
        )

    def wb_load(layer):
        return pltpu.make_async_copy(
            wb_hbm.at[layer],
            wb.at[layer, s // 2, pl.ds(pl.multiple_of(c * b_rows, b_rows), b_rows), :],
            load_sem.at[layer, 3],
        )

    def load(layer, piece):
        if piece == 0:
            src, dst = wp_hbm.at[layer], wp.at[layer, pl.ds(pl.multiple_of(s * p_rows, p_rows), p_rows), :]
        elif piece == 1:
            src, dst = wg_hbm.at[layer], wg.at[layer, pl.ds(pl.multiple_of(s * g_rows, g_rows), g_rows), :]
        else:
            src, dst = wb_hbm.at[layer], wb_own.at[layer]
        return pltpu.make_async_copy(src, dst, load_sem.at[layer, piece])

    def ready(layer, *pieces):
        for piece in pieces:
            for k in range(3):
                block = blocks[k]

                def act(piece=piece, block=block):
                    for unit in UNITS[piece]:
                        w_copy(layer, 0, block, other, unit, {"grp": other}).wait_recv()
                holds(block, piece, act)
            if piece == BACK:
                @pl.when(c == s_parity)
                def _():
                    wb_load(layer).wait()
                    pltpu.make_async_remote_copy(
                        src_ref=wb_own.at[layer],
                        dst_ref=wb.at[layer, s // 2, pl.ds(pl.multiple_of((1 - c) * b_rows, b_rows), b_rows), :],
                        send_sem=bx_send.at[layer], recv_sem=bx_recv.at[layer],
                        device_id={"tp": t1}, device_id_type=MESH,
                    ).wait_recv()

    def tok_load(k):
        return pltpu.make_async_copy(
            tok_hbm.at[:, pl.ds(k * cols_k, cols_k)], gathered.at[0, t, k], load_sem.at[LAYERS, k]
        )

    def guest_copy(k):
        return pltpu.make_async_remote_copy(
            src_ref=gathered.at[0, t, k], dst_ref=gathered.at[GUEST, t, k],
            send_sem=tk_send.at[k], recv_sem=tk_recv.at[k],
            device_id={"sp": mid_here}, device_id_type=MESH,
        )

    def return_copy(k):
        return pltpu.make_async_remote_copy(
            src_ref=returned.at[k], dst_ref=gathered.at[1, t, k],
            send_sem=rt_send.at[k], recv_sem=rt_recv.at[k],
            device_id={"sp": end_here}, device_id_type=MESH,
        )

    def ag_copy(slot, which, k, block, target):
        return pltpu.make_async_remote_copy(
            src_ref=gathered.at[slot, block, k], dst_ref=gathered.at[slot, block, k],
            send_sem=ag_send.at[slot, which, k], recv_sem=ag_recv.at[slot, which, k],
            device_id={"tp": target}, device_id_type=MESH,
        )

    def start_gather(slot, k):
        ag_copy(slot, 0, k, t, t2).start()
        ag_copy(slot, 1, k, t, t1).start()

    spans = [w // 2 for w in pool_windows]

    def h_copy(layer, way, span):
        rows = (span if way == 0 else max(span - 1, 1)) * GRID_W
        at = toks - rows if way == 0 else 0
        return pltpu.make_async_remote_copy(
            src_ref=halo.at[layer, 1, pl.ds(at, rows), :],
            dst_ref=halo.at[layer, 0 if way == 0 else 2, pl.ds(at, rows), :],
            send_sem=h_send.at[layer, way], recv_sem=h_recv.at[layer, way],
            device_id={"sp": s + 1 if way == 0 else s - 1}, device_id_type=MESH,
        )

    def halo_do(layer, way, cond, op):
        for group_id, span in enumerate(spans):
            @pl.when(jnp.logical_and(cond, t == group_id))
            def _(span=span):
                op(h_copy(layer, way, span))

    def halo_start(layer):
        up_ok = jnp.logical_and(s < last, jnp.logical_or(layer > 0, s == 1))
        down_ok = jnp.logical_and(s > 0, jnp.logical_or(layer > 0, s == 2))
        halo_do(layer, 0, up_ok, lambda x: x.start())
        halo_do(layer, 1, down_ok, lambda x: x.start())

    def halo_wait(layer):
        from_up = jnp.logical_and(s > 0, jnp.logical_or(layer > 0, s == 2))
        from_down = jnp.logical_and(s < last, jnp.logical_or(layer > 0, s == 1))
        halo_do(layer, 0, from_up, lambda x: x.wait_recv())
        halo_do(layer, 1, from_down, lambda x: x.wait_recv())

    def px_copy(slot, row):
        return pltpu.make_async_remote_copy(
            src_ref=pair.at[slot, row], dst_ref=pair.at[slot, row],
            send_sem=px_send.at[slot], recv_sem=px_recv.at[slot],
            device_id={"tp": t1}, device_id_type=MESH,
        )

    def rs_copy(slot, k):
        return pltpu.make_async_remote_copy(
            src_ref=parts.at[slot, k], dst_ref=arrived.at[slot, k],
            send_sem=rs_send.at[slot, k], recv_sem=rs_recv.at[slot, k],
            device_id={"tp": t2}, device_id_type=MESH,
        )

    def absorb(layer, slot, which, block, total):
        for k in range(CHUNKS):
            at = pl.ds(pl.multiple_of(block * feats + k * cols_k, cols_k), cols_k)
            wide = gathered[slot, block, k].astype(f32)
            scaled[which, :, at] = (wide * gain_ref[pl.ds(layer, 1), at]).astype(bf)
            total = total + jnp.sum(wide * wide, axis=1, keepdims=True)
        return total

    def scale_of(total):
        return lax.rsqrt(total / (tp_count * feats) + norm_eps)

    def half_dot(layer, which, first, weights):
        at = pl.ds(pl.multiple_of(first * feats, feats), 2 * feats)
        return jnp.dot(scaled[which, :, at], weights[layer, at, :], preferred_element_type=f32)

    def gate_of(layer, which, scale):
        acc = jnp.dot(scaled[which], wg[layer], preferred_element_type=f32)
        value = jax.nn.sigmoid(acc * scale)
        for k in range(CHUNKS):
            gate_buf[which, k] = value[:, k * cols_k:(k + 1) * cols_k]

    def share_pooled(slot, which, sums, cells):
        pooled = (sums / counts[which] - cells.astype(f32)).astype(bf)
        pair[slot, c] = pooled
        px_copy(slot, c).start()

    def back_part(layer, slot, cols, k):
        at = pl.ds(k * cols_k, cols_k)
        acc = jnp.dot(pair[slot, 0], wb[layer, cols, 0:b_rows, at], preferred_element_type=f32)
        return acc + jnp.dot(
            pair[slot, 1], wb[layer, cols, b_rows:2 * b_rows, at], preferred_element_type=f32
        )

    def back(layer, slot, which):
        px_copy(slot, 1 - c).wait_recv()
        for k in range(CHUNKS):
            parts[slot, k] = back_part(layer, slot, far_base // 2, k).astype(bf)
            rs_copy(slot, k).start()
        for k in range(CHUNKS):
            own_part[which, k] = back_part(layer, slot, base // 2, k)

    def update(slot, which, k):
        rs_copy(slot, k).wait_recv()
        branch = own_part[which, k] + arrived[slot, k].astype(f32)
        return (gathered[slot, t, k].astype(f32) + gate_buf[which, k] * branch).astype(bf)

    for k in range(CHUNKS):
        tok_load(k).start()
    for layer in range(LAYERS):
        for piece in (0, 2, 1):
            load(layer, piece).start()

        @pl.when(jnp.logical_and(c == s_parity, jnp.logical_or(is_mid, layer > 0)))
        def _(layer=layer):
            wb_load(layer).start()
    for layer in range(LAYERS):
        for slot in (0, 2):
            halo[layer, slot] = jnp.zeros(halo.shape[2:], halo.dtype)

    barrier = pltpu.get_barrier_semaphore()
    for target in ({"grp": other}, {"tp": t1}, {"tp": t2}):
        pl.semaphore_signal(barrier, inc=1, device_id=target, device_id_type=MESH)

    @pl.when(s > 0)
    def _():
        for peer in (t, t1):
            pl.semaphore_signal(barrier, inc=1, device_id={"sp": s - 1, "tp": peer}, device_id_type=MESH)

    @pl.when(s < last)
    def _():
        for peer in (t, t1):
            pl.semaphore_signal(barrier, inc=1, device_id={"sp": s + 1, "tp": peer}, device_id_type=MESH)

    pl.semaphore_wait(barrier, 3 + jnp.where(s > 0, 2, 0) + jnp.where(s < last, 2, 0))

    def own_loads(layer):
        for piece in (0, 2, 1):
            load(layer, piece).wait()

        @pl.when(c != s_parity)
        def _():
            bx_copy(layer).start()

    PIECES = (POOL, BACK, GATE_A, GATE_B)

    def end_own(layer, mine, *pieces):
        for piece in pieces:
            half = g if mine else other
            own_copy(layer, 0 if mine else 1, half, piece, mid_here).start()

    def mid_own(layer, flow, *pieces):
        plane = mid_far if flow == 0 else end_here
        for piece in pieces:
            own_copy(layer, flow, g, piece, plane).start()

    def setup():
        half_span = jnp.int32(spans[0])
        for group_id in range(1, GROUPS):
            half_span = jnp.where(t == group_id, spans[group_id], half_span)
        shift = GRID_W.bit_length() - 1
        out_tok = lax.broadcasted_iota(jnp.int32, (toks, toks), 0)
        in_tok = lax.broadcasted_iota(jnp.int32, (toks, toks), 1)
        out_row = lax.shift_right_logical(out_tok, shift)
        out_col = lax.bitwise_and(out_tok, GRID_W - 1)
        in_col = lax.bitwise_and(in_tok, GRID_W - 1)
        near_col = (in_col >= out_col - half_span) & (in_col < out_col + half_span)
        for slot in range(3):
            in_row = (slot - 1) * rows_here + lax.shift_right_logical(in_tok, shift)
            inside = near_col & (in_row >= out_row - half_span) & (in_row < out_row + half_span)
            box[slot] = jnp.where(inside, 1.0, 0.0).astype(bf)
        tok_at = lax.broadcasted_iota(jnp.int32, counts.shape[1:], 0)
        col_at = lax.bitwise_and(tok_at, GRID_W - 1)
        col_counts = jnp.minimum(col_at + half_span, GRID_W) - jnp.maximum(col_at - half_span, 0)
        for which, plane in ((0, s), (1, end_here)):
            row_at = plane * rows_here + lax.shift_right_logical(tok_at, shift)
            row_counts = jnp.minimum(row_at + half_span, total_rows) - jnp.maximum(row_at - half_span, 0)
            counts[which] = (row_counts * col_counts).astype(f32)

    def box_dot(slot, value):
        return jnp.dot(box[slot], value, preferred_element_type=f32)

    for k in range(CHUNKS):
        tok_load(k).wait()

    @pl.when(is_end)
    def _():
        load(0, 0).wait()
        end_own(0, True, POOL)
        for k in range(CHUNKS):
            guest_copy(k).start()
        end_own(0, False, POOL)
        load(0, 2).wait()
        end_own(0, True, BACK)
        load(0, 1).wait()
        end_own(0, True, GATE_A, GATE_B)
        end_own(0, False, BACK, GATE_A, GATE_B)
        own_loads(1)
        own_loads(2)
        setup()
        pump(1, 0, POOL, BACK, GATE_A, GATE_B)
        pump(2, 0, POOL)
        end_own(1, True, POOL, BACK)
        pump(2, 0, BACK, GATE_A, GATE_B)
        end_own(1, True, GATE_A, GATE_B)
        end_own(1, False, POOL, BACK)
        for k in range(CHUNKS):
            return_copy(k).wait_recv()
            start_gather(1, k)
        pump(1, 1, POOL)

    @pl.when(is_mid)
    def _():
        guest_side = jnp.where(low, 0, 2)
        for k in range(CHUNKS):
            start_gather(0, k)
        load(0, 0).wait()
        mid_own(0, 0, POOL)
        load(0, 2).wait()
        mid_own(0, 0, BACK)
        load(0, 1).wait()
        mid_own(0, 0, GATE_A, GATE_B)

        @pl.when(c != s_parity)
        def _():
            bx_copy(0).start()
        own_loads(1)
        own_loads(2)
        mid_own(1, 1, *PIECES)
        mid_own(2, 1, *PIECES)
        zero = jnp.zeros((toks, 1), f32)
        total = absorb(0, 0, 0, t, zero)
        pump(0, 1, POOL)
        pump(0, 0, POOL)
        setup()
        for k in range(CHUNKS):
            guest_copy(k).wait_recv()
            start_gather(GUEST, k)
        for k in range(CHUNKS):
            ag_copy(0, 1, k, t1, t1).wait_recv()
            ag_copy(0, 0, k, t2, t2).wait_recv()
            ag_copy(0, 2, k, t2, t1).start()
        total = absorb(0, 0, 0, t1, total)
        pump(0, 1, BACK)
        pump(0, 2, POOL)
        total = absorb(0, 0, 0, t2, total)
        for k in range(CHUNKS):
            ag_copy(0, 2, k, t3, t1).wait_recv()
        total = absorb(0, 0, 0, t3, total)
        scale = scale_of(total)
        guest_total = absorb(0, GUEST, 1, t, zero)
        pump(0, 1, GATE_A)
        for k in range(CHUNKS):
            ag_copy(GUEST, 1, k, t1, t1).wait_recv()
            ag_copy(GUEST, 0, k, t2, t2).wait_recv()
            ag_copy(GUEST, 2, k, t2, t1).start()
        pump(0, 0, BACK)
        guest_total = absorb(0, GUEST, 1, t1, guest_total)
        guest_total = absorb(0, GUEST, 1, t2, guest_total)
        ready(0, POOL)
        acc = half_dot(0, 0, base, wp) + half_dot(0, 0, far_base, wp)
        halo[0, 1] = (acc * scale).astype(bf)
        halo_start(0)
        for k in range(CHUNKS):
            ag_copy(GUEST, 2, k, t3, t1).wait_recv()
        guest_total = absorb(0, GUEST, 1, t3, guest_total)
        guest_scale = scale_of(guest_total)
        acc = half_dot(0, 1, base, wp) + half_dot(0, 1, far_base, wp)
        halo[0, guest_side] = (acc * guest_scale).astype(bf)
        cells = halo[0, guest_side]
        own_cells = halo[0, 1]
        share_pooled(GUEST, 1, box_dot(1, cells) + box_dot(2 - guest_side, own_cells), cells)
        pump(0, 1, GATE_B)
        pump(0, 0, GATE_A)
        pump(0, 2, BACK)
        halo_wait(0)
        sums = box_dot(0, halo[0, 0]) + box_dot(1, own_cells) + box_dot(2, halo[0, 2])
        share_pooled(0, 0, sums, own_cells)
        pump(0, 0, GATE_B)
        mid_own(1, 0, *PIECES)
        ready(0, BACK)
        back(0, GUEST, 1)
        back(0, 0, 0)
        pump(0, 2, GATE_A, GATE_B)
        ready(0, GATE_A, GATE_B)
        gate_of(0, 1, guest_scale)
        for k in range(CHUNKS):
            returned[k] = update(GUEST, 1, k)
            return_copy(k).start()
        gate_of(0, 0, scale)
        for k in range(CHUNKS):
            gathered[1, t, k] = update(0, 0, k)
            start_gather(1, k)
        pump(1, 1, POOL)

    def one_layer(layer, _):
        more = layer + 1 < LAYERS
        @pl.when(jnp.logical_and(is_mid, layer == 1))
        def _():
            pump(layer, 0, POOL)
        pump(layer, 2, POOL)
        total = absorb(layer, layer, 0, t, jnp.zeros((toks, 1), f32))
        pump(layer, 1, BACK)
        for k in range(CHUNKS):
            ag_copy(layer, 1, k, t1, t1).wait_recv()
        total = absorb(layer, layer, 0, t1, total)
        for k in range(CHUNKS):
            ag_copy(layer, 0, k, t2, t2).wait_recv()
            ag_copy(layer, 2, k, t2, t1).start()
        total = absorb(layer, layer, 0, t2, total)
        ready(layer, POOL)
        acc = half_dot(layer, 0, base, wp)
        for k in range(CHUNKS):
            ag_copy(layer, 2, k, t3, t1).wait_recv()
        total = absorb(layer, layer, 0, t3, total)
        scale = scale_of(total)
        acc = acc + half_dot(layer, 0, far_base, wp)
        halo[layer, 1] = (acc * scale).astype(bf)
        halo_start(layer)

        @pl.when(is_end)
        def _():
            end_own(layer, False, GATE_A, GATE_B)

            @pl.when(more)
            def _():
                end_own(layer + 1, True, POOL, BACK)
                end_own(layer + 1, False, POOL, BACK)
                end_own(layer + 1, True, GATE_A, GATE_B)

        @pl.when(is_mid)
        def _():
            pump(layer, 0, BACK)
        pump(layer, 2, BACK)

        @pl.when(is_mid)
        def _():
            pump(layer, 0, GATE_A)
        pump(layer, 1, GATE_A)
        cells = halo[layer, 1]
        sums = box_dot(1, cells)
        halo_wait(layer)
        sums = sums + box_dot(0, halo[layer, 0]) + box_dot(2, halo[layer, 2])
        share_pooled(layer, 0, sums, cells)

        @pl.when(is_mid)
        def _():
            pump(layer, 0, GATE_B)
        pump(layer, 1, GATE_B)

        @pl.when(jnp.logical_and(is_mid, more))
        def _():
            mid_own(layer + 1, 0, *PIECES)
        ready(layer, BACK)
        back(layer, layer, 0)
        pump(layer, 2, GATE_A, GATE_B)

        @pl.when(more)
        def _():
            pump(layer + 1, 1, POOL)

            @pl.when(is_mid)
            def _():
                pump(layer + 1, 0, POOL)
        ready(layer, GATE_A, GATE_B)
        gate_of(layer, 0, scale)
        for k in range(CHUNKS):
            state = update(layer, 0, k)

            @pl.when(more)
            def _(k=k, state=state):
                gathered[layer + 1, t, k] = state
                start_gather(layer + 1, k)

            @pl.when(jnp.logical_not(more))
            def _(k=k, state=state):
                out_ref[:, k * cols_k:(k + 1) * cols_k] = state
        return 0

    lax.fori_loop(1, LAYERS, one_layer, 0)

    def drain_own(layer, flow, half, plane):
        for piece in PIECES:
            own_copy(layer, flow, half, piece, plane).wait_send()

    def drain_slot(slot):
        for k in range(CHUNKS):
            ag_copy(slot, 0, k, t, t2).wait_send()
            ag_copy(slot, 1, k, t, t1).wait_send()
            ag_copy(slot, 2, k, t2, t1).wait_send()
            rs_copy(slot, k).wait_send()
        px_copy(slot, c).wait_send()

    def drain_blocks(layer):
        for k in range(3):
            for piece in PIECES:
                def act(k=k, piece=piece):
                    for unit in UNITS[piece]:
                        if k == 0:
                            near_copy(layer, blocks[0], unit).wait_send()
                        else:
                            across_copy(layer, k, blocks[k], unit).wait_send()

                            @pl.when(jnp.logical_and(is_mid, layer > 0))
                            def _(unit=unit):
                                outer_copy(layer, k, blocks[k], unit).wait_send()
                holds(blocks[k], piece, act)

    def drain(layer, _):
        @pl.when(jnp.logical_and(c != s_parity, jnp.logical_or(is_mid, layer > 0)))
        def _():
            bx_copy(layer).wait_send()

        @pl.when(is_end)
        def _():
            drain_own(layer, 0, g, mid_here)
            drain_own(layer, 1, other, mid_here)

        @pl.when(is_mid)
        def _():
            drain_own(layer, 0, g, mid_far)

            @pl.when(layer > 0)
            def _():
                drain_own(layer, 1, g, end_here)

        @pl.when(jnp.logical_or(is_mid, layer > 0))
        def _():
            drain_blocks(layer)
            drain_slot(layer)
        up_ok = jnp.logical_and(s < last, jnp.logical_or(layer > 0, s == 1))
        down_ok = jnp.logical_and(s > 0, jnp.logical_or(layer > 0, s == 2))
        halo_do(layer, 0, up_ok, lambda x: x.wait_send())
        halo_do(layer, 1, down_ok, lambda x: x.wait_send())
        return 0

    lax.fori_loop(0, LAYERS, drain, 0)

    @pl.when(is_mid)
    def _():
        drain_slot(GUEST)
        for k in range(CHUNKS):
            return_copy(k).wait_send()

    @pl.when(is_end)
    def _():
        for k in range(CHUNKS):
            guest_copy(k).wait_send()


def fused(tokens_in, norm_gain, w_pool_in, w_gate, w_back):
    sp_count, tp_count = lax.axis_size("sp"), lax.axis_size("tp")
    toks, feats = tokens_in.shape
    _, depth, local_pool = w_pool_in.shape
    b_rows, b_cols = w_back.shape[1:]
    cols_k = feats // CHUNKS
    bf, f32 = jnp.bfloat16, jnp.float32
    dma = pltpu.SemaphoreType.DMA
    slots = LAYERS + 1
    hbm = pl.BlockSpec(memory_space=pltpu.HBM)
    vmem = pl.BlockSpec(memory_space=pltpu.VMEM)
    return pl.pallas_call(
        functools.partial(fused_kernel, sp_count, tp_count),
        out_shape=jax.ShapeDtypeStruct((toks, feats), bf),
        in_specs=[hbm, vmem, hbm, hbm, hbm],
        out_specs=vmem,
        scratch_shapes=[
            pltpu.VMEM((LAYERS, sp_count * depth, local_pool), bf),
            pltpu.VMEM((LAYERS, sp_count * depth, w_gate.shape[2]), bf),
            pltpu.VMEM((LAYERS, 2, 2 * b_rows, b_cols), bf),
            pltpu.VMEM((LAYERS, b_rows, b_cols), bf),
            pltpu.VMEM((slots, tp_count, CHUNKS, toks, cols_k), bf),
            pltpu.VMEM((2, toks, tp_count * feats), bf),
            pltpu.VMEM((LAYERS, 3, toks, local_pool), bf),
            pltpu.VMEM((2, CHUNKS, toks, cols_k), f32),
            pltpu.VMEM((2, CHUNKS, toks, cols_k), f32),
            pltpu.VMEM((3, toks, toks), bf),
            pltpu.VMEM((2, toks, local_pool), f32),
            pltpu.VMEM((slots, 2, toks, local_pool), bf),
            pltpu.VMEM((slots, CHUNKS, toks, cols_k), bf),
            pltpu.VMEM((slots, CHUNKS, toks, cols_k), bf),
            pltpu.VMEM((CHUNKS, toks, cols_k), bf),
            dma((LAYERS + 1, 4)),
            dma((LAYERS, 7, 5)), dma((LAYERS, sp_count, 2, 5)),
            dma((LAYERS,)), dma((LAYERS,)),
            dma((CHUNKS,)), dma((CHUNKS,)), dma((CHUNKS,)), dma((CHUNKS,)),
            dma((slots, 3, CHUNKS)), dma((slots, 3, CHUNKS)),
            dma((LAYERS, 2)), dma((LAYERS, 2)),
            dma((slots,)), dma((slots,)),
            dma((slots, CHUNKS)), dma((slots, CHUNKS)),
        ],
        compiler_params=pltpu.CompilerParams(
            collective_id=0, has_side_effects=True, vmem_limit_bytes=56 * 1024 * 1024
        ),
    )(tokens_in, norm_gain, w_pool_in, w_gate, w_back)


def dispatch(tokens_in, norm_gain, w_pool_in, w_gate, w_back):
    fits = (
        lax.axis_size("grp") == 2
        and lax.axis_size("tp") == GROUPS == 4
        and lax.axis_size("sp") == lax.axis_size("tp")
        and w_pool_in.shape[2] * GROUPS == POOL_WIDTH
        and w_pool_in.shape[1] == tokens_in.shape[1]
        and tokens_in.shape[0] // GRID_W >= max(pool_windows) // 2
    )
    step = fused if fits else on_device
    return step(tokens_in, norm_gain, w_pool_in, w_gate, w_back)


def solution(mesh):
    return jax.shard_map(
        dispatch,
        mesh=mesh,
        in_specs=(
            P(("grp", "sp"), "tp"),
            P(),
            P(None, "sp", "tp"),
            P(None, "sp", "tp"),
            P(None, "tp", "sp"),
        ),
        out_specs=P(("grp", "sp"), "tp"),
        check_vma=False,
    )
```

```python
import jax
import jax.numpy as jnp
from jax import lax
from jax.experimental import pallas as pl
from jax.experimental.pallas import tpu as pltpu
from jax.sharding import PartitionSpec as P
import functools

POOL_WIDTH = 1024
GROUPS = 4
GRID_W = 32
LAYERS = 3


pool_windows = (2, 4, 8, 16)
norm_eps = 1e-06


def padded_2(value, sides, width):
    for axis, dim in sides:
        peers, length = (lax.axis_size(axis), value.shape[dim])
        up = [(i, (i + 1) % peers) for i in range(peers - 1)]
        down = [(j, i) for i, j in up]
        last = lax.slice_in_dim(value, length - width, length, axis=dim)
        initial = lax.slice_in_dim(value, 0, width, axis=dim)
        before = lax.ppermute(last, axis, up)
        after = lax.ppermute(initial, axis, down)
        value = jnp.concatenate([before, value, after], axis=dim)
    return value


def window_means(padded, rows_here, first_row, total_rows, window):
    reach = max(pool_windows) // 2
    half_span = window // 2
    width_cols = padded.shape[1] - 2 * reach
    row_sums = padded[reach - half_span : reach - half_span + rows_here]
    for offset in range(1 - half_span, half_span):
        row_sums = row_sums + padded[reach + offset : reach + offset + rows_here]
    box_sums = row_sums[:, reach - half_span : reach - half_span + width_cols]
    for offset in range(1 - half_span, half_span):
        box_sums = box_sums + row_sums[:, reach + offset : reach + offset + width_cols]
    row_index = first_row + jnp.arange(rows_here, dtype=jnp.int32)
    col_index = jnp.arange(width_cols, dtype=jnp.int32)
    row_counts = jnp.minimum(row_index + half_span, total_rows) - jnp.maximum(
        row_index - half_span, 0
    )
    col_counts = jnp.minimum(col_index + half_span, width_cols) - jnp.maximum(
        col_index - half_span, 0
    )
    counts = (row_counts[:, None] * col_counts[None, :]).astype(jnp.float32)
    return box_sums / counts[:, :, None]


def on_device(tokens_in, norm_gain, w_pool_in, w_gate, w_back):
    reach = max(pool_windows) // 2
    sp_count = lax.axis_size("sp")
    tp_count = lax.axis_size("tp")
    tp_pos = lax.axis_index("tp")
    sp_pos = lax.axis_index("sp")
    tok_rows = tokens_in.shape[0]
    rows_here = tok_rows // GRID_W
    total_rows = rows_here * sp_count
    first_row = sp_pos * rows_here
    local_pool = w_pool_in.shape[2]
    group_width = POOL_WIDTH // GROUPS
    channel_group = (tp_pos * local_pool + jnp.arange(local_pool, dtype=jnp.int32)) // group_width
    state = tokens_in
    for layer_id in range(LAYERS):
        whole_rows = lax.all_gather(state, "tp", axis=1, tiled=True)
        wide = whole_rows.astype(jnp.float32)
        normed = (
            wide
            * lax.rsqrt(jnp.mean(wide * wide, axis=-1, keepdims=True) + norm_eps)
            * norm_gain[layer_id]
        ).astype(jnp.bfloat16)
        pool_acc = jnp.dot(
            normed,
            lax.all_gather(w_pool_in[layer_id], "sp", axis=0, tiled=True),
            preferred_element_type=jnp.float32,
        )
        gate_acc = jnp.dot(
            normed,
            lax.all_gather(w_gate[layer_id], "sp", axis=0, tiled=True),
            preferred_element_type=jnp.float32,
        )
        pool_in = pool_acc.astype(jnp.bfloat16)
        gate = jax.nn.sigmoid(gate_acc)
        cells = pool_in.reshape(rows_here, GRID_W, local_pool)
        rimmed = padded_2(cells, (("sp", 0),), reach)
        padded = jnp.pad(rimmed.astype(jnp.float32), ((0, 0), (reach, reach), (0, 0)))
        means = jnp.zeros((rows_here, GRID_W, local_pool), jnp.float32)
        for group_id in range(GROUPS):
            in_group = (channel_group == group_id)[None, None, :]
            means = jnp.where(
                in_group,
                window_means(padded, rows_here, first_row, total_rows, pool_windows[group_id]),
                means,
            )
        pooled = (
            (means - cells.astype(jnp.float32)).reshape(tok_rows, local_pool).astype(jnp.bfloat16)
        )
        full_pooled = lax.all_gather(pooled, "tp", axis=1, tiled=True)
        back_rows = lax.all_gather(w_back[layer_id], "sp", axis=1, tiled=True)
        back_cols = lax.all_to_all(back_rows, "tp", split_axis=1, concat_axis=0, tiled=True)
        partials = jnp.einsum(
            "tnb,nbd->ntd",
            full_pooled.reshape(tok_rows, tp_count, local_pool),
            back_cols.reshape(tp_count, local_pool, back_cols.shape[1]),
            preferred_element_type=jnp.float32,
        ).astype(jnp.bfloat16)
        branch = jnp.sum(partials.astype(jnp.float32), axis=0)
        state = (state.astype(jnp.float32) + gate * branch).astype(jnp.bfloat16)
    return state


MESH = pl.DeviceIdType.MESH
POOL, GATE_A, GATE_B, BACK = range(4)
UNITS = {POOL: (0,), GATE_A: (1,), GATE_B: (2,), BACK: (3, 4)}
CHUNKS = 2
GUEST = LAYERS


MID_FIRST = (
    ("own", 0, 0, 0), ("own", 0, 0, 3), ("own", 1, 1, 0), ("gstart", 0), ("own", 1, 0, 2),
    ("pump", 0, 0, 0), ("pump", 0, 1, 3), ("own", 2, 1, 3), ("own", 2, 1, 1), ("agf", 0, 0), ("guest", 0),
    ("own", 2, 1, 0), ("pump", 1, 1, 2), ("own", 2, 1, 2), ("own", 1, 1, 2), ("agf", 0, 1),
    ("pump", 0, 0, 3), ("pump", 0, 2, 3), ("own", 1, 1, 3), ("own", 1, 1, 1), ("pump", 0, 1, 0),
    ("own", 0, 0, 2), ("guest", 1), ("pump", 0, 2, 0), ("own", 0, 0, 1), ("pool", 0), ("pump", 0, 0, 2),
    ("pump", 0, 0, 1), ("pump", 0, 1, 2), ("own", 1, 0, 0), ("pump", 1, 0, 0), ("agf", 3, 0), ("agf", 3, 1),
    ("pump", 0, 1, 1), ("pool", 3), ("pump", 0, 2, 2), ("pump", 0, 2, 1), ("box", 0), ("back", 3),
    ("pump", 1, 1, 0), ("pump", 1, 2, 0), ("own", 1, 0, 1), ("pump", 1, 0, 1), ("back", 0), ("gate", 3),
    ("upd", 3, 0), ("upd", 3, 1), ("own", 1, 0, 3), ("pump", 1, 0, 2), ("own", 2, 0, 3), ("pump", 1, 0, 3),
    ("gate", 0), ("upd", 0, 0), ("pump", 1, 1, 1), ("own", 2, 0, 0), ("pump", 1, 2, 1), ("upd", 0, 1),
)
END_FIRST = (
    ("own", 0, 0, 0), ("own", 0, 0, 3), ("tok", 0), ("tok", 1), ("pump", 1, 0, 0), ("own", 0, 0, 2),
    ("own", 0, 1, 0), ("own", 0, 0, 1), ("pump", 1, 1, 2), ("own", 1, 0, 0), ("pump", 2, 0, 1),
    ("own", 1, 0, 1), ("own", 0, 1, 3), ("own", 0, 1, 1), ("pump", 2, 0, 3), ("own", 0, 1, 2),
    ("pump", 1, 0, 1), ("own", 1, 0, 3), ("own", 1, 0, 2), ("pump", 2, 0, 0), ("pump", 1, 0, 2),
    ("pump", 1, 1, 0), ("own", 1, 1, 0), ("pump", 2, 0, 2), ("pump", 1, 0, 3), ("own", 2, 0, 0),
    ("own", 2, 0, 1), ("own", 1, 1, 1), ("pump", 1, 2, 0), ("ret", 0), ("ret", 1),
)
MID_REST = (
    (
        ("pump", 1, 2, 3), ("pump", 1, 1, 3), ("pump", 2, 0, 0), ("pump", 1, 2, 2),
    ),
    (),
    (
        ("pump", 2, 1, 0), ("pump", 2, 2, 0),
    ),
    (
        ("pump", 2, 0, 2), ("pump", 2, 0, 3), ("pump", 2, 1, 3), ("own", 2, 0, 1), ("pump", 2, 0, 1),
    ),
    (
        ("pump", 2, 2, 2), ("pump", 2, 2, 3),
    ),
    (),
    (),
    (),
    (
        ("pump", 2, 1, 1), ("own", 2, 0, 2),
    ),
    (
        ("pump", 2, 2, 1),
    ),
    (),
    (
        ("pump", 2, 1, 2),
    ),
    (),
    (),
    (),
    (),
)
END_REST = (
    (
        ("pump", 1, 1, 1), ("pump", 1, 1, 3), ("own", 1, 1, 3),
    ),
    (
        ("own", 2, 0, 2),
    ),
    (
        ("pump", 1, 2, 3), ("pump", 1, 2, 2), ("own", 2, 0, 3), ("own", 1, 1, 2), ("own", 2, 1, 3),
        ("pump", 1, 2, 1),
    ),
    (),
    (),
    (
        ("own", 2, 1, 1), ("pump", 2, 1, 0), ("pump", 2, 1, 3), ("pump", 2, 2, 0),
    ),
    (),
    (
        ("own", 2, 1, 0), ("own", 2, 1, 2), ("pump", 2, 2, 2),
    ),
    (),
    (
        ("pump", 2, 2, 3),
    ),
    (
        ("pump", 2, 1, 1), ("pump", 2, 2, 1),
    ),
    (),
    (
        ("pump", 2, 1, 2),
    ),
    (),
    (),
    (),
)
FIRST_BACK, FIRST_GATE = 3, 3


def fused_kernel(
    sp_count, tp_count,
    tok_hbm, gain_ref, wp_hbm, wg_hbm, wb_hbm, out_ref,
    wp, wg, wb, wb_own, gathered, scaled, halo, gate_buf, own_part, box, counts,
    pair, parts, arrived, returned,
    load_sem, w_send, z_recv, y_recv, bx_send, bx_recv, tk_send, tk_recv, rt_send, rt_recv,
    ag_send, ag_recv, h_send, h_recv, px_send, px_recv, rs_send, rs_recv,
):
    g = lax.axis_index("grp")
    s = lax.axis_index("sp")
    t = lax.axis_index("tp")
    other = 1 - g
    c = t % 2
    base = t - c
    t1 = base + 1 - c
    t2 = (t + 2) % tp_count
    t3 = (t1 + 2) % tp_count
    far_base = (base + 2) % tp_count
    last = sp_count - 1
    toks, feats = tok_hbm.shape
    local_pool = wp.shape[2]
    cols_k = feats // CHUNKS
    rows_here = toks // GRID_W
    total_rows = rows_here * sp_count
    bf, f32 = jnp.bfloat16, jnp.float32

    low = s < 2
    is_mid = jnp.logical_and(s > 0, s < last)
    is_end = jnp.logical_not(is_mid)
    end_here = jnp.where(low, 0, last)
    mid_here = jnp.where(low, 1, last - 1)
    end_far = last - end_here
    mid_far = last - mid_here
    blocks = (
        jnp.where(is_mid, end_here, mid_here),
        jnp.where(is_mid, mid_far, mid_far),
        end_far,
    )
    s_parity = s % 2

    p_rows, g_rows = wp_hbm.shape[1], wg_hbm.shape[1]
    b_rows = wb_hbm.shape[1]

    def view(layer, block, half, unit, row=None):
        if unit == 0:
            n = p_rows // 2
            return wp.at[layer, pl.ds(pl.multiple_of(block * p_rows + half * n, n), n), :]
        if unit in (1, 2):
            n = g_rows // 4
            at = block * g_rows + half * (2 * n) + (unit - 1) * n
            return wg.at[layer, pl.ds(pl.multiple_of(at, n), n), :]
        n = b_rows // 2
        row = unit - 3 if row is None else row
        return wb.at[layer, block // 2, pl.ds(pl.multiple_of(row * b_rows + half * n, n), n), :]

    unit_rows = g_rows // 4

    def units(sem, count):
        ref = wg.at[pl.ds(0, -(-count // 16)), pl.ds(0, unit_rows * (count if count <= 16 else count // 2)), :]
        return pltpu.make_async_remote_copy(
            src_ref=ref, dst_ref=ref, send_sem=sem, recv_sem=sem,
            device_id={"grp": other}, device_id_type=MESH,
        )

    def w_copy(layer, flow, block, half, unit, target, recv):
        ref = view(layer, block, half, unit)
        return pltpu.make_async_remote_copy(
            src_ref=ref, dst_ref=ref, send_sem=w_send.at[flow], recv_sem=recv,
            device_id=target, device_id_type=MESH,
        )

    def kind(piece):
        return {POOL: 0, GATE_A: 1, GATE_B: 1, BACK: 2}[piece]

    def own_copy(layer, flow, half, piece, plane, recv):
        if piece != BACK:
            return w_copy(layer, flow, s, half, UNITS[piece][0], {"sp": plane}, recv)
        n = b_rows // 2
        return pltpu.make_async_remote_copy(
            src_ref=wb_own.at[layer, pl.ds(pl.multiple_of(half * n, n), n), :],
            dst_ref=view(layer, s, half, 3, row=c),
            send_sem=w_send.at[flow], recv_sem=recv,
            device_id={"sp": plane, "tp": base + s_parity}, device_id_type=MESH,
        )

    def holds(block, piece, fn):
        if piece == BACK:
            pl.when(c == block % 2)(fn)
        else:
            fn()

    def pump(mid, layer, k, piece):
        block = blocks[k]

        def act():
            units(z_recv.at[layer, k, piece], len(UNITS[piece])).wait_recv()
            for unit in UNITS[piece]:
                if k == 0 and mid:
                    w_copy(layer, 2, block, g, unit, {"sp": mid_far}, z_recv.at[layer, 2, piece]).start()
                    continue
                w_copy(
                    layer, 2 + k, block, g, unit, {"grp": other}, y_recv.at[layer, kind(piece)]
                ).start()
                if mid and layer > 0:
                    w_copy(
                        layer, 4 + k, block, g, unit, {"sp": end_here}, z_recv.at[layer, k, piece]
                    ).start()
        holds(block, piece, act)

    def own(mid, waited, layer, flow, piece):
        if (layer, kind(piece)) not in waited:
            waited.add((layer, kind(piece)))
            load(layer, kind(piece)).wait()
            if piece == BACK and (mid or layer > 0):
                @pl.when(c != s_parity)
                def _():
                    bx_copy(layer).start()
        if mid and flow == 0:
            own_copy(layer, 0, g, piece, mid_far, z_recv.at[layer, 1, piece]).start()
        elif mid:
            own_copy(layer, 1, g, piece, end_here, z_recv.at[layer, 0, piece]).start()
        elif flow == 0:
            own_copy(layer, 0, g, piece, mid_here, z_recv.at[layer, 0, piece]).start()
        else:
            own_copy(layer, 1, other, piece, mid_here, y_recv.at[layer, kind(piece)]).start()

    def bx_copy(layer):
        return pltpu.make_async_remote_copy(
            src_ref=wb_own.at[layer],
            dst_ref=wb.at[layer, s // 2, pl.ds(pl.multiple_of(c * b_rows, b_rows), b_rows), :],
            send_sem=bx_send.at[0], recv_sem=bx_recv.at[layer],
            device_id={"tp": t1}, device_id_type=MESH,
        )

    def wb_load(layer):
        return pltpu.make_async_copy(
            wb_hbm.at[layer],
            wb.at[layer, s // 2, pl.ds(pl.multiple_of(c * b_rows, b_rows), b_rows), :],
            load_sem.at[layer, 3],
        )

    def load(layer, piece):
        if piece == 0:
            src, dst = wp_hbm.at[layer], wp.at[layer, pl.ds(pl.multiple_of(s * p_rows, p_rows), p_rows), :]
        elif piece == 1:
            src, dst = wg_hbm.at[layer], wg.at[layer, pl.ds(pl.multiple_of(s * g_rows, g_rows), g_rows), :]
        else:
            src, dst = wb_hbm.at[layer], wb_own.at[layer]
        return pltpu.make_async_copy(src, dst, load_sem.at[layer, piece])

    def ready(layer, which):
        if which < 2:
            units(y_recv.at[layer, which], 3 * (1 + which)).wait_recv()
            return

        @pl.when(c == s_parity)
        def _():
            units(y_recv.at[layer, 2], 2).wait_recv()
            wb_load(layer).wait()
            units(bx_recv.at[layer], 2).wait_recv()

        @pl.when(c != s_parity)
        def _():
            units(y_recv.at[layer, 2], 4).wait_recv()

    def tok_load(k):
        return pltpu.make_async_copy(
            tok_hbm.at[:, pl.ds(k * cols_k, cols_k)], gathered.at[0, t, k], load_sem.at[LAYERS, k]
        )

    def guest_copy(k):
        return pltpu.make_async_remote_copy(
            src_ref=gathered.at[0, t, k], dst_ref=gathered.at[GUEST, t, k],
            send_sem=tk_send.at[0], recv_sem=tk_recv.at[k],
            device_id={"sp": mid_here}, device_id_type=MESH,
        )

    def return_copy(k):
        return pltpu.make_async_remote_copy(
            src_ref=returned.at[k], dst_ref=gathered.at[1, t, k],
            send_sem=rt_send.at[0], recv_sem=rt_recv.at[k],
            device_id={"sp": end_here}, device_id_type=MESH,
        )

    def ag_copy(slot, k, block, target, recv):
        return pltpu.make_async_remote_copy(
            src_ref=gathered.at[slot, block, k], dst_ref=gathered.at[slot, block, k],
            send_sem=ag_send.at[0], recv_sem=ag_recv.at[slot, recv],
            device_id={"tp": target}, device_id_type=MESH,
        )

    def start_gather(slot, k):
        ag_copy(slot, k, t, t2, k).start()
        ag_copy(slot, k, t, t1, 3).start()

    def pass_on(slot, k):
        units(ag_recv.at[slot, k], 1).wait_recv()
        ag_copy(slot, k, t2, t1, 2).start()

    spans = [w // 2 for w in pool_windows]

    def h_copy(layer, way, span):
        rows = (span if way == 0 else max(span - 1, 1)) * GRID_W
        at = toks - rows if way == 0 else 0
        return pltpu.make_async_remote_copy(
            src_ref=halo.at[layer, 1, pl.ds(at, rows), :],
            dst_ref=halo.at[layer, 0 if way == 0 else 2, pl.ds(at, rows), :],
            send_sem=h_send.at[layer, way], recv_sem=h_recv.at[layer, way],
            device_id={"sp": s + 1 if way == 0 else s - 1}, device_id_type=MESH,
        )

    def halo_do(layer, way, cond, op):
        for group_id, span in enumerate(spans):
            @pl.when(jnp.logical_and(cond, t == group_id))
            def _(span=span):
                op(h_copy(layer, way, span))

    def halo_start(layer):
        up_ok = jnp.logical_and(s < last, jnp.logical_or(layer > 0, s == 1))
        down_ok = jnp.logical_and(s > 0, jnp.logical_or(layer > 0, s == 2))
        halo_do(layer, 0, up_ok, lambda x: x.start())
        halo_do(layer, 1, down_ok, lambda x: x.start())

    def halo_wait(layer):
        from_up = jnp.logical_and(s > 0, jnp.logical_or(layer > 0, s == 2))
        from_down = jnp.logical_and(s < last, jnp.logical_or(layer > 0, s == 1))
        halo_do(layer, 0, from_up, lambda x: x.wait_recv())
        halo_do(layer, 1, from_down, lambda x: x.wait_recv())

    def px_copy(slot, row):
        return pltpu.make_async_remote_copy(
            src_ref=pair.at[slot, row], dst_ref=pair.at[slot, row],
            send_sem=px_send.at[0], recv_sem=px_recv.at[slot],
            device_id={"tp": t1}, device_id_type=MESH,
        )

    def rs_copy(slot, k):
        return pltpu.make_async_remote_copy(
            src_ref=parts.at[slot, k], dst_ref=arrived.at[slot, k],
            send_sem=rs_send.at[0], recv_sem=rs_recv.at[slot, k],
            device_id={"tp": t2}, device_id_type=MESH,
        )

    def absorb(layer, slot, which, block, total):
        for k in range(CHUNKS):
            at = pl.ds(pl.multiple_of(block * feats + k * cols_k, cols_k), cols_k)
            wide = gathered[slot, block, k].astype(f32)
            scaled[which, :, at] = (wide * gain_ref[pl.ds(layer, 1), at]).astype(bf)
            total = total + jnp.sum(wide * wide, axis=1, keepdims=True)
        return total

    def scale_of(total):
        return lax.rsqrt(total / (tp_count * feats) + norm_eps)

    def half_dot(layer, which, first, weights):
        at = pl.ds(pl.multiple_of(first * feats, feats), 2 * feats)
        return jnp.dot(scaled[which, :, at], weights[layer, at, :], preferred_element_type=f32)

    def gate_of(layer, which, scale):
        acc = jnp.dot(scaled[which], wg[layer], preferred_element_type=f32)
        value = jax.nn.sigmoid(acc * scale)
        for k in range(CHUNKS):
            gate_buf[which, k] = value[:, k * cols_k:(k + 1) * cols_k]

    def share_pooled(slot, which, sums, cells):
        pooled = (sums / counts[which] - cells.astype(f32)).astype(bf)
        pair[slot, c] = pooled
        px_copy(slot, c).start()

    def back_part(layer, slot, cols, k):
        at = pl.ds(k * cols_k, cols_k)
        acc = jnp.dot(pair[slot, 0], wb[layer, cols, 0:b_rows, at], preferred_element_type=f32)
        return acc + jnp.dot(
            pair[slot, 1], wb[layer, cols, b_rows:2 * b_rows, at], preferred_element_type=f32
        )

    def back(layer, slot, which):
        units(px_recv.at[slot], 1).wait_recv()
        for k in range(CHUNKS):
            parts[slot, k] = back_part(layer, slot, far_base // 2, k).astype(bf)
            rs_copy(slot, k).start()
        for k in range(CHUNKS):
            own_part[which, k] = back_part(layer, slot, base // 2, k)

    def update(slot, which, k):
        units(rs_recv.at[slot, k], 1).wait_recv()
        branch = own_part[which, k] + arrived[slot, k].astype(f32)
        return (gathered[slot, t, k].astype(f32) + gate_buf[which, k] * branch).astype(bf)

    for k in range(CHUNKS):
        tok_load(k).start()
    for layer in range(LAYERS):
        for piece in (0, 2, 1):
            load(layer, piece).start()

        @pl.when(jnp.logical_and(c == s_parity, jnp.logical_or(is_mid, layer > 0)))
        def _(layer=layer):
            wb_load(layer).start()
    for layer in range(LAYERS):
        for slot in (0, 2):
            halo[layer, slot] = jnp.zeros(halo.shape[2:], halo.dtype)

    barrier = pltpu.get_barrier_semaphore()
    for target in ({"grp": other}, {"tp": t1}, {"tp": t2}):
        pl.semaphore_signal(barrier, inc=1, device_id=target, device_id_type=MESH)

    @pl.when(s > 0)
    def _():
        for peer in (t, t1):
            pl.semaphore_signal(barrier, inc=1, device_id={"sp": s - 1, "tp": peer}, device_id_type=MESH)

    @pl.when(s < last)
    def _():
        for peer in (t, t1):
            pl.semaphore_signal(barrier, inc=1, device_id={"sp": s + 1, "tp": peer}, device_id_type=MESH)

    pl.semaphore_wait(barrier, 3 + jnp.where(s > 0, 2, 0) + jnp.where(s < last, 2, 0))

    def setup():
        half_span = jnp.int32(spans[0])
        for group_id in range(1, GROUPS):
            half_span = jnp.where(t == group_id, spans[group_id], half_span)
        shift = GRID_W.bit_length() - 1
        out_tok = lax.broadcasted_iota(jnp.int32, (toks, toks), 0)
        in_tok = lax.broadcasted_iota(jnp.int32, (toks, toks), 1)
        out_row = lax.shift_right_logical(out_tok, shift)
        out_col = lax.bitwise_and(out_tok, GRID_W - 1)
        in_col = lax.bitwise_and(in_tok, GRID_W - 1)
        near_col = (in_col >= out_col - half_span) & (in_col < out_col + half_span)
        for slot in range(3):
            in_row = (slot - 1) * rows_here + lax.shift_right_logical(in_tok, shift)
            inside = near_col & (in_row >= out_row - half_span) & (in_row < out_row + half_span)
            box[slot] = jnp.where(inside, 1.0, 0.0).astype(bf)
        tok_at = lax.broadcasted_iota(jnp.int32, counts.shape[1:], 0)
        col_at = lax.bitwise_and(tok_at, GRID_W - 1)
        col_counts = jnp.minimum(col_at + half_span, GRID_W) - jnp.maximum(col_at - half_span, 0)
        for which, plane in ((0, s), (1, end_here)):
            row_at = plane * rows_here + lax.shift_right_logical(tok_at, shift)
            row_counts = jnp.minimum(row_at + half_span, total_rows) - jnp.maximum(row_at - half_span, 0)
            counts[which] = (row_counts * col_counts).astype(f32)

    def box_dot(slot, value):
        return jnp.dot(box[slot], value, preferred_element_type=f32)

    for k in range(CHUNKS):
        tok_load(k).wait()
    waited_mid, waited_end = set(), set()
    zero = jnp.zeros((toks, 1), f32)

    def relay(mid, item):
        if item[0] == "own":
            own(mid, waited_mid if mid else waited_end, *item[1:])
        else:
            pump(mid, *item[1:])

    def gather_step(layer, slot, which, k, total):
        if k == 0:
            total = absorb(layer, slot, which, t, zero)
            units(ag_recv.at[slot, 3], 2).wait_recv()
            total = absorb(layer, slot, which, t1, total)
        pass_on(slot, k)
        if k == CHUNKS - 1:
            total = absorb(layer, slot, which, t2, total)
        return total

    def pool_step(layer, slot, which, total):
        ready(layer, 0)
        acc = half_dot(layer, which, base, wp)
        units(ag_recv.at[slot, 2], 2).wait_recv()
        total = absorb(layer, slot, which, t3, total)
        scale = scale_of(total)
        acc = acc + half_dot(layer, which, far_base, wp)
        return (acc * scale).astype(bf), scale

    @pl.when(is_end)
    def _():
        for item in END_FIRST:
            if item[0] == "tok":
                guest_copy(item[1]).start()
            elif item[0] == "ret":
                if item[1] == 0:
                    setup()
                return_copy(item[1]).wait_recv()
                start_gather(1, item[1])
            else:
                relay(False, item)

    @pl.when(is_mid)
    def _():
        guest_side = jnp.where(low, 0, 2)
        total, scale = {}, {}
        for item in MID_FIRST:
            name = item[0]
            slot = item[1]
            which = 1 if slot == GUEST else 0
            if name == "gstart":
                for k in range(CHUNKS):
                    start_gather(0, k)
            elif name == "guest":
                guest_copy(slot).wait_recv()
                start_gather(GUEST, slot)
            elif name == "agf":
                if item == ("agf", 0, 0):
                    setup()
                total[slot] = gather_step(0, slot, which, item[2], total.get(slot))
            elif name == "pool" and slot == 0:
                halo[0, 1], scale[0] = pool_step(0, 0, 0, total[0])
                halo_start(0)
            elif name == "pool":
                units(ag_recv.at[GUEST, 2], 2).wait_recv()
                total[slot] = absorb(0, GUEST, 1, t3, total[slot])
                scale[slot] = scale_of(total[slot])
                acc = half_dot(0, 1, base, wp) + half_dot(0, 1, far_base, wp)
                halo[0, guest_side] = (acc * scale[slot]).astype(bf)
                cells = halo[0, guest_side]
                sums = box_dot(1, cells) + box_dot(2 - guest_side, halo[0, 1])
                share_pooled(GUEST, 1, sums, cells)
            elif name == "box":
                halo_wait(0)
                cells = halo[0, 1]
                sums = box_dot(0, halo[0, 0]) + box_dot(1, cells) + box_dot(2, halo[0, 2])
                share_pooled(0, 0, sums, cells)
            elif name == "back":
                if slot == FIRST_BACK:
                    ready(0, 2)
                back(0, slot, which)
            elif name == "gate":
                if slot == FIRST_GATE:
                    ready(0, 1)
                gate_of(0, which, scale[slot])
            elif name == "upd":
                k = item[2]
                value = update(slot, which, k)
                if slot == GUEST:
                    returned[k] = value
                    return_copy(k).start()
                else:
                    gathered[1, t, k] = value
                    start_gather(1, k)
            else:
                relay(True, item)

    steps = iter(zip(MID_REST, END_REST))

    def relays():
        for mid, items in zip((True, False), next(steps)):
            if items:
                @pl.when(is_mid if mid else is_end)
                def _(mid=mid, items=items):
                    for item in items:
                        relay(mid, item)

    for layer in range(1, LAYERS):
        total = None
        for k in range(CHUNKS):
            total = gather_step(layer, layer, 0, k, total)
            relays()
        cells, scale = pool_step(layer, layer, 0, total)
        halo[layer, 1] = cells
        halo_start(layer)
        relays()
        cells = halo[layer, 1]
        sums = box_dot(1, cells)
        halo_wait(layer)
        sums = sums + box_dot(0, halo[layer, 0]) + box_dot(2, halo[layer, 2])
        share_pooled(layer, 0, sums, cells)
        relays()
        ready(layer, 2)
        back(layer, layer, 0)
        relays()
        ready(layer, 1)
        gate_of(layer, 0, scale)
        relays()
        for k in range(CHUNKS):
            state = update(layer, 0, k)
            if layer + 1 < LAYERS:
                gathered[layer + 1, t, k] = state
                start_gather(layer + 1, k)
            else:
                out_ref[:, k * cols_k:(k + 1) * cols_k] = state
            relays()

    def sent(sem, count):
        units(sem, count).wait_send()

    def sent_blocks(flow, k, layers):
        @pl.when(c == blocks[k] % 2)
        def _():
            sent(w_send.at[flow], 5 * layers)

        @pl.when(c != blocks[k] % 2)
        def _():
            sent(w_send.at[flow], 3 * layers)

    def sent_chain(layers, slots):
        @pl.when(c != s_parity)
        def _():
            sent(bx_send.at[0], 2 * layers)
        sent(ag_send.at[0], 6 * slots)
        sent(rs_send.at[0], 2 * slots)
        sent(px_send.at[0], slots)

    @pl.when(is_mid)
    def _():
        sent(w_send.at[0], 4 * LAYERS)
        sent(w_send.at[1], 4 * (LAYERS - 1))
        for k in range(3):
            sent_blocks(2 + k, k, LAYERS)
        for k in (1, 2):
            sent_blocks(4 + k, k, LAYERS - 1)
        sent(rt_send.at[0], CHUNKS)
        sent_chain(LAYERS, LAYERS + 1)

    @pl.when(is_end)
    def _():
        sent(w_send.at[0], 4 * LAYERS)
        sent(w_send.at[1], 4 * LAYERS)
        for k in range(3):
            sent_blocks(2 + k, k, LAYERS - 1)
        sent(tk_send.at[0], CHUNKS)
        sent_chain(LAYERS - 1, LAYERS - 1)
    for layer in range(LAYERS):
        outward = layer > 0
        halo_do(layer, 0, (s < last) if outward else (s == 1), lambda x: x.wait_send())
        halo_do(layer, 1, (s > 0) if outward else (s == 2), lambda x: x.wait_send())


def fused(tokens_in, norm_gain, w_pool_in, w_gate, w_back):
    sp_count, tp_count = lax.axis_size("sp"), lax.axis_size("tp")
    toks, feats = tokens_in.shape
    _, depth, local_pool = w_pool_in.shape
    b_rows, b_cols = w_back.shape[1:]
    cols_k = feats // CHUNKS
    bf, f32 = jnp.bfloat16, jnp.float32
    dma = pltpu.SemaphoreType.DMA
    slots = LAYERS + 1
    hbm = pl.BlockSpec(memory_space=pltpu.HBM)
    vmem = pl.BlockSpec(memory_space=pltpu.VMEM)
    return pl.pallas_call(
        functools.partial(fused_kernel, sp_count, tp_count),
        out_shape=jax.ShapeDtypeStruct((toks, feats), bf),
        in_specs=[hbm, vmem, hbm, hbm, hbm],
        out_specs=vmem,
        scratch_shapes=[
            pltpu.VMEM((LAYERS, sp_count * depth, local_pool), bf),
            pltpu.VMEM((LAYERS, sp_count * depth, w_gate.shape[2]), bf),
            pltpu.VMEM((LAYERS, 2, 2 * b_rows, b_cols), bf),
            pltpu.VMEM((LAYERS, b_rows, b_cols), bf),
            pltpu.VMEM((slots, tp_count, CHUNKS, toks, cols_k), bf),
            pltpu.VMEM((2, toks, tp_count * feats), bf),
            pltpu.VMEM((LAYERS, 3, toks, local_pool), bf),
            pltpu.VMEM((2, CHUNKS, toks, cols_k), f32),
            pltpu.VMEM((2, CHUNKS, toks, cols_k), f32),
            pltpu.VMEM((3, toks, toks), bf),
            pltpu.VMEM((2, toks, local_pool), f32),
            pltpu.VMEM((slots, 2, toks, local_pool), bf),
            pltpu.VMEM((slots, CHUNKS, toks, cols_k), bf),
            pltpu.VMEM((slots, CHUNKS, toks, cols_k), bf),
            pltpu.VMEM((CHUNKS, toks, cols_k), bf),
            dma((LAYERS + 1, 4)),
            dma((7,)), dma((LAYERS, 3, 4)), dma((LAYERS, 3)),
            dma((1,)), dma((LAYERS,)),
            dma((1,)), dma((CHUNKS,)), dma((1,)), dma((CHUNKS,)),
            dma((1,)), dma((slots, 4)),
            dma((LAYERS, 2)), dma((LAYERS, 2)),
            dma((1,)), dma((slots,)),
            dma((1,)), dma((slots, CHUNKS)),
        ],
        compiler_params=pltpu.CompilerParams(
            collective_id=0, has_side_effects=True, vmem_limit_bytes=56 * 1024 * 1024
        ),
    )(tokens_in, norm_gain, w_pool_in, w_gate, w_back)


def dispatch(tokens_in, norm_gain, w_pool_in, w_gate, w_back):
    fits = (
        lax.axis_size("grp") == 2
        and lax.axis_size("tp") == GROUPS == 4
        and lax.axis_size("sp") == lax.axis_size("tp")
        and w_pool_in.shape[2] * GROUPS == POOL_WIDTH
        and w_pool_in.shape[1] == tokens_in.shape[1] == w_gate.shape[2] == w_back.shape[2]
        and tokens_in.shape[1] == 2 * tokens_in.shape[0] == 2 * w_pool_in.shape[2]
        and tokens_in.shape[0] // GRID_W >= max(pool_windows) // 2
    )
    step = fused if fits else on_device
    return step(tokens_in, norm_gain, w_pool_in, w_gate, w_back)


def solution(mesh):
    return jax.shard_map(
        dispatch,
        mesh=mesh,
        in_specs=(
            P(("grp", "sp"), "tp"),
            P(),
            P(None, "sp", "tp"),
            P(None, "sp", "tp"),
            P(None, "tp", "sp"),
        ),
        out_specs=P(("grp", "sp"), "tp"),
        check_vma=False,
    )
```

```python
import jax
import jax.numpy as jnp
from jax import lax
from jax.experimental import pallas as pl
from jax.experimental.pallas import tpu as pltpu
from jax.sharding import PartitionSpec as P
import functools

POOL_WIDTH = 1024
GROUPS = 4
GRID_W = 32
LAYERS = 3


pool_windows = (2, 4, 8, 16)
norm_eps = 1e-06


def padded_2(value, sides, width):
    for axis, dim in sides:
        peers, length = (lax.axis_size(axis), value.shape[dim])
        up = [(i, (i + 1) % peers) for i in range(peers - 1)]
        down = [(j, i) for i, j in up]
        last = lax.slice_in_dim(value, length - width, length, axis=dim)
        initial = lax.slice_in_dim(value, 0, width, axis=dim)
        before = lax.ppermute(last, axis, up)
        after = lax.ppermute(initial, axis, down)
        value = jnp.concatenate([before, value, after], axis=dim)
    return value


def window_means(padded, rows_here, first_row, total_rows, window):
    reach = max(pool_windows) // 2
    half_span = window // 2
    width_cols = padded.shape[1] - 2 * reach
    row_sums = padded[reach - half_span : reach - half_span + rows_here]
    for offset in range(1 - half_span, half_span):
        row_sums = row_sums + padded[reach + offset : reach + offset + rows_here]
    box_sums = row_sums[:, reach - half_span : reach - half_span + width_cols]
    for offset in range(1 - half_span, half_span):
        box_sums = box_sums + row_sums[:, reach + offset : reach + offset + width_cols]
    row_index = first_row + jnp.arange(rows_here, dtype=jnp.int32)
    col_index = jnp.arange(width_cols, dtype=jnp.int32)
    row_counts = jnp.minimum(row_index + half_span, total_rows) - jnp.maximum(
        row_index - half_span, 0
    )
    col_counts = jnp.minimum(col_index + half_span, width_cols) - jnp.maximum(
        col_index - half_span, 0
    )
    counts = (row_counts[:, None] * col_counts[None, :]).astype(jnp.float32)
    return box_sums / counts[:, :, None]


def on_device(tokens_in, norm_gain, w_pool_in, w_gate, w_back):
    reach = max(pool_windows) // 2
    sp_count = lax.axis_size("sp")
    tp_count = lax.axis_size("tp")
    tp_pos = lax.axis_index("tp")
    sp_pos = lax.axis_index("sp")
    tok_rows = tokens_in.shape[0]
    rows_here = tok_rows // GRID_W
    total_rows = rows_here * sp_count
    first_row = sp_pos * rows_here
    local_pool = w_pool_in.shape[2]
    group_width = POOL_WIDTH // GROUPS
    channel_group = (tp_pos * local_pool + jnp.arange(local_pool, dtype=jnp.int32)) // group_width
    state = tokens_in
    for layer_id in range(LAYERS):
        whole_rows = lax.all_gather(state, "tp", axis=1, tiled=True)
        wide = whole_rows.astype(jnp.float32)
        normed = (
            wide
            * lax.rsqrt(jnp.mean(wide * wide, axis=-1, keepdims=True) + norm_eps)
            * norm_gain[layer_id]
        ).astype(jnp.bfloat16)
        pool_acc = jnp.dot(
            normed,
            lax.all_gather(w_pool_in[layer_id], "sp", axis=0, tiled=True),
            preferred_element_type=jnp.float32,
        )
        gate_acc = jnp.dot(
            normed,
            lax.all_gather(w_gate[layer_id], "sp", axis=0, tiled=True),
            preferred_element_type=jnp.float32,
        )
        pool_in = pool_acc.astype(jnp.bfloat16)
        gate = jax.nn.sigmoid(gate_acc)
        cells = pool_in.reshape(rows_here, GRID_W, local_pool)
        rimmed = padded_2(cells, (("sp", 0),), reach)
        padded = jnp.pad(rimmed.astype(jnp.float32), ((0, 0), (reach, reach), (0, 0)))
        means = jnp.zeros((rows_here, GRID_W, local_pool), jnp.float32)
        for group_id in range(GROUPS):
            in_group = (channel_group == group_id)[None, None, :]
            means = jnp.where(
                in_group,
                window_means(padded, rows_here, first_row, total_rows, pool_windows[group_id]),
                means,
            )
        pooled = (
            (means - cells.astype(jnp.float32)).reshape(tok_rows, local_pool).astype(jnp.bfloat16)
        )
        full_pooled = lax.all_gather(pooled, "tp", axis=1, tiled=True)
        back_rows = lax.all_gather(w_back[layer_id], "sp", axis=1, tiled=True)
        back_cols = lax.all_to_all(back_rows, "tp", split_axis=1, concat_axis=0, tiled=True)
        partials = jnp.einsum(
            "tnb,nbd->ntd",
            full_pooled.reshape(tok_rows, tp_count, local_pool),
            back_cols.reshape(tp_count, local_pool, back_cols.shape[1]),
            preferred_element_type=jnp.float32,
        ).astype(jnp.bfloat16)
        branch = jnp.sum(partials.astype(jnp.float32), axis=0)
        state = (state.astype(jnp.float32) + gate * branch).astype(jnp.bfloat16)
    return state


MESH = pl.DeviceIdType.MESH
POOL, GATE_A, GATE_B, BACK = range(4)
UNITS = {POOL: (0,), GATE_A: (1,), GATE_B: (2,), BACK: (3, 4)}
CHUNKS = 2
GUEST = LAYERS


MID_FIRST = (
    ("own", 1, 1, 1), ("own", 0, 0, 3), ("own", 0, 0, 0), ("own", 2, 0, 3), ("own", 1, 1, 2), ("gstart", 0),
    ("own", 1, 0, 2), ("pump", 0, 1, 3), ("pump", 0, 0, 0), ("pump", 0, 1, 0), ("pump", 2, 1, 3),
    ("guest", 0), ("own", 2, 1, 3), ("own", 1, 0, 3), ("own", 2, 1, 0), ("agf", 0, 0), ("agf", 0, 1),
    ("own", 1, 0, 0), ("pump", 1, 1, 2), ("guest", 1), ("pump", 0, 2, 0), ("own", 0, 0, 1),
    ("pump", 1, 1, 3), ("own", 2, 1, 1), ("pump", 1, 1, 0), ("agf", 3, 0), ("agf", 3, 1), ("pump", 0, 0, 3),
    ("own", 1, 1, 3), ("own", 0, 0, 2), ("pool", 0), ("pump", 0, 0, 1), ("pump", 0, 1, 1),
    ("pump", 0, 0, 2), ("pool", 3), ("own", 1, 0, 1), ("own", 2, 1, 2), ("pump", 0, 2, 3),
    ("pump", 1, 0, 0), ("pump", 0, 1, 2), ("own", 1, 1, 0), ("box", 0), ("back", 3), ("pump", 0, 2, 1),
    ("pump", 0, 2, 2), ("back", 0), ("pump", 2, 0, 0), ("pump", 1, 0, 3), ("pump", 1, 1, 1),
    ("pump", 1, 2, 0), ("gate", 3), ("upd", 3, 0), ("upd", 3, 1), ("gate", 0), ("upd", 0, 0), ("upd", 0, 1),
    ("pump", 1, 0, 2), ("pump", 1, 2, 3), ("pump", 1, 0, 1),
)
END_FIRST = (
    ("tok", 0), ("own", 0, 0, 0), ("tok", 1), ("own", 0, 1, 2), ("own", 0, 0, 3), ("own", 0, 1, 0),
    ("pump", 2, 1, 3), ("pump", 1, 0, 2), ("own", 0, 0, 2), ("pump", 1, 0, 1), ("own", 0, 0, 1),
    ("pump", 1, 1, 2), ("pump", 2, 0, 3), ("own", 1, 0, 0), ("own", 0, 1, 3), ("own", 1, 0, 3),
    ("own", 2, 0, 0), ("own", 0, 1, 1), ("pump", 1, 1, 3), ("own", 1, 0, 2), ("pump", 2, 0, 0),
    ("own", 2, 0, 1), ("pump", 1, 1, 0), ("pump", 1, 0, 3), ("pump", 2, 0, 2), ("own", 1, 0, 1),
    ("pump", 2, 0, 1), ("pump", 1, 2, 0), ("pump", 1, 0, 0), ("own", 1, 1, 0), ("own", 2, 0, 2),
    ("own", 1, 1, 3), ("ret", 0), ("pump", 1, 1, 1), ("own", 2, 0, 3), ("ret", 1),
)
MID_REST = (
    (
        ("pump", 1, 2, 2),
    ),
    (
        ("own", 2, 0, 0),
    ),
    (
        ("pump", 2, 0, 1), ("pump", 1, 2, 1), ("pump", 2, 1, 0), ("pump", 2, 0, 3),
    ),
    (
        ("pump", 2, 2, 0),
    ),
    (
        ("pump", 2, 2, 1), ("pump", 2, 0, 2),
    ),
    (),
    (
        ("pump", 2, 2, 3),
    ),
    (
        ("pump", 2, 2, 2), ("own", 2, 0, 2), ("pump", 2, 1, 2),
    ),
    (
        ("own", 2, 0, 1),
    ),
    (),
    (
        ("pump", 2, 1, 1),
    ),
    (),
    (),
    (),
    (),
    (),
)
END_REST = (
    (),
    (
        ("pump", 1, 2, 3),
    ),
    (),
    (
        ("own", 1, 1, 1), ("pump", 1, 2, 2), ("pump", 1, 2, 1), ("own", 1, 1, 2),
    ),
    (
        ("pump", 2, 1, 0),
    ),
    (
        ("own", 2, 1, 0),
    ),
    (),
    (
        ("pump", 2, 2, 0), ("own", 2, 1, 1), ("pump", 2, 2, 3), ("pump", 2, 2, 1),
    ),
    (),
    (),
    (
        ("pump", 2, 1, 2), ("own", 2, 1, 3), ("pump", 2, 2, 2), ("own", 2, 1, 2),
    ),
    (),
    (
        ("pump", 2, 1, 1),
    ),
    (),
    (),
    (),
)
FIRST_BACK, FIRST_GATE = 3, 3


def fused_kernel(
    sp_count, tp_count,
    tok_hbm, gain_ref, wp_hbm, wg_hbm, wb_hbm, out_ref,
    wp, wg, wb, wb_own, gathered, scaled, halo, gate_buf, own_part, box, counts,
    pair, parts, arrived, returned,
    load_sem, w_send, z_recv, y_recv, bx_send, bx_recv, tk_send, tk_recv, rt_send, rt_recv,
    ag_send, ag_recv, h_send, h_recv, px_send, px_recv, rs_send, rs_recv,
):
    g = lax.axis_index("grp")
    s = lax.axis_index("sp")
    t = lax.axis_index("tp")
    other = 1 - g
    c = t % 2
    base = t - c
    t1 = base + 1 - c
    t2 = (t + 2) % tp_count
    t3 = (t1 + 2) % tp_count
    far_base = (base + 2) % tp_count
    last = sp_count - 1
    toks, feats = tok_hbm.shape
    local_pool = wp.shape[2]
    cols_k = feats // CHUNKS
    rows_here = toks // GRID_W
    total_rows = rows_here * sp_count
    bf, f32 = jnp.bfloat16, jnp.float32

    low = s < 2
    is_mid = jnp.logical_and(s > 0, s < last)
    is_end = jnp.logical_not(is_mid)
    end_here = jnp.where(low, 0, last)
    mid_here = jnp.where(low, 1, last - 1)
    end_far = last - end_here
    mid_far = last - mid_here
    blocks = (
        jnp.where(is_mid, end_here, mid_here),
        jnp.where(is_mid, mid_far, mid_far),
        end_far,
    )
    s_parity = s % 2

    p_rows, g_rows = wp_hbm.shape[1], wg_hbm.shape[1]
    b_rows = wb_hbm.shape[1]

    def view(layer, block, half, unit, row=None):
        if unit == 0:
            n = p_rows // 2
            return wp.at[layer, pl.ds(pl.multiple_of(block * p_rows + half * n, n), n), :]
        if unit in (1, 2):
            n = g_rows // 4
            at = block * g_rows + half * (2 * n) + (unit - 1) * n
            return wg.at[layer, pl.ds(pl.multiple_of(at, n), n), :]
        n = b_rows // 2
        row = unit - 3 if row is None else row
        return wb.at[layer, block // 2, pl.ds(pl.multiple_of(row * b_rows + half * n, n), n), :]

    unit_rows = g_rows // 4

    def units(sem, count):
        ref = wg.at[pl.ds(0, -(-count // 16)), pl.ds(0, unit_rows * (count if count <= 16 else count // 2)), :]
        return pltpu.make_async_remote_copy(
            src_ref=ref, dst_ref=ref, send_sem=sem, recv_sem=sem,
            device_id={"grp": other}, device_id_type=MESH,
        )

    def w_copy(layer, flow, block, half, unit, target, recv):
        ref = view(layer, block, half, unit)
        return pltpu.make_async_remote_copy(
            src_ref=ref, dst_ref=ref, send_sem=w_send.at[flow], recv_sem=recv,
            device_id=target, device_id_type=MESH,
        )

    def kind(piece):
        return {POOL: 0, GATE_A: 1, GATE_B: 1, BACK: 2}[piece]

    def own_copy(layer, flow, half, piece, plane, recv):
        if piece != BACK:
            return w_copy(layer, flow, s, half, UNITS[piece][0], {"sp": plane}, recv)
        n = b_rows // 2
        return pltpu.make_async_remote_copy(
            src_ref=wb_own.at[layer, pl.ds(pl.multiple_of(half * n, n), n), :],
            dst_ref=view(layer, s, half, 3, row=c),
            send_sem=w_send.at[flow], recv_sem=recv,
            device_id={"sp": plane, "tp": base + s_parity}, device_id_type=MESH,
        )

    def holds(block, piece, fn):
        if piece == BACK:
            pl.when(c == block % 2)(fn)
        else:
            fn()

    def pump(mid, layer, k, piece):
        block = blocks[k]

        def act():
            units(z_recv.at[layer, k, piece], len(UNITS[piece])).wait_recv()
            for unit in UNITS[piece]:
                if k == 0 and mid:
                    w_copy(layer, 2, block, g, unit, {"sp": mid_far}, z_recv.at[layer, 2, piece]).start()
                    continue
                w_copy(
                    layer, 2 + k, block, g, unit, {"grp": other}, y_recv.at[layer, kind(piece)]
                ).start()
                if mid and layer > 0:
                    w_copy(
                        layer, 4 + k, block, g, unit, {"sp": end_here}, z_recv.at[layer, k, piece]
                    ).start()
        holds(block, piece, act)

    def own(mid, waited, layer, flow, piece):
        if (layer, kind(piece)) not in waited:
            waited.add((layer, kind(piece)))
            load(layer, kind(piece)).wait()
            if piece == BACK and (mid or layer > 0):
                @pl.when(c != s_parity)
                def _():
                    bx_copy(layer).start()
        if mid and flow == 0:
            own_copy(layer, 0, g, piece, mid_far, z_recv.at[layer, 1, piece]).start()
        elif mid:
            own_copy(layer, 1, g, piece, end_here, z_recv.at[layer, 0, piece]).start()
        elif flow == 0:
            own_copy(layer, 0, g, piece, mid_here, z_recv.at[layer, 0, piece]).start()
        else:
            own_copy(layer, 1, other, piece, mid_here, y_recv.at[layer, kind(piece)]).start()

    def bx_copy(layer):
        return pltpu.make_async_remote_copy(
            src_ref=wb_own.at[layer],
            dst_ref=wb.at[layer, s // 2, pl.ds(pl.multiple_of(c * b_rows, b_rows), b_rows), :],
            send_sem=bx_send.at[0], recv_sem=bx_recv.at[layer],
            device_id={"tp": t1}, device_id_type=MESH,
        )

    def wb_load(layer):
        return pltpu.make_async_copy(
            wb_hbm.at[layer],
            wb.at[layer, s // 2, pl.ds(pl.multiple_of(c * b_rows, b_rows), b_rows), :],
            load_sem.at[layer, 3],
        )

    def load(layer, piece):
        if piece == 0:
            src, dst = wp_hbm.at[layer], wp.at[layer, pl.ds(pl.multiple_of(s * p_rows, p_rows), p_rows), :]
        elif piece == 1:
            src, dst = wg_hbm.at[layer], wg.at[layer, pl.ds(pl.multiple_of(s * g_rows, g_rows), g_rows), :]
        else:
            src, dst = wb_hbm.at[layer], wb_own.at[layer]
        return pltpu.make_async_copy(src, dst, load_sem.at[layer, piece])

    def ready(layer, which):
        if which < 2:
            units(y_recv.at[layer, which], 3 * (1 + which)).wait_recv()
            return

        @pl.when(c == s_parity)
        def _():
            units(y_recv.at[layer, 2], 2).wait_recv()
            wb_load(layer).wait()
            units(bx_recv.at[layer], 2).wait_recv()

        @pl.when(c != s_parity)
        def _():
            units(y_recv.at[layer, 2], 4).wait_recv()

    def tok_load(k):
        return pltpu.make_async_copy(
            tok_hbm.at[:, pl.ds(k * cols_k, cols_k)], gathered.at[0, t, k], load_sem.at[LAYERS, k]
        )

    def guest_copy(k):
        return pltpu.make_async_remote_copy(
            src_ref=gathered.at[0, t, k], dst_ref=gathered.at[GUEST, t, k],
            send_sem=tk_send.at[0], recv_sem=tk_recv.at[k],
            device_id={"sp": mid_here}, device_id_type=MESH,
        )

    def return_copy(k):
        return pltpu.make_async_remote_copy(
            src_ref=returned.at[k], dst_ref=gathered.at[1, t, k],
            send_sem=rt_send.at[0], recv_sem=rt_recv.at[k],
            device_id={"sp": end_here}, device_id_type=MESH,
        )

    def ag_copy(slot, k, block, target, recv):
        return pltpu.make_async_remote_copy(
            src_ref=gathered.at[slot, block, k], dst_ref=gathered.at[slot, block, k],
            send_sem=ag_send.at[0], recv_sem=ag_recv.at[slot, recv],
            device_id={"tp": target}, device_id_type=MESH,
        )

    def start_gather(slot, k):
        ag_copy(slot, k, t, t2, k).start()
        ag_copy(slot, k, t, t1, 3).start()

    def pass_on(slot, k):
        units(ag_recv.at[slot, k], 1).wait_recv()
        ag_copy(slot, k, t2, t1, 2).start()

    spans = [w // 2 for w in pool_windows]

    def h_copy(layer, way, span):
        rows = (span if way == 0 else max(span - 1, 1)) * GRID_W
        at = toks - rows if way == 0 else 0
        return pltpu.make_async_remote_copy(
            src_ref=halo.at[layer, 1, pl.ds(at, rows), :],
            dst_ref=halo.at[layer, 0 if way == 0 else 2, pl.ds(at, rows), :],
            send_sem=h_send.at[layer, way], recv_sem=h_recv.at[layer, way],
            device_id={"sp": s + 1 if way == 0 else s - 1}, device_id_type=MESH,
        )

    def halo_do(layer, way, cond, op):
        for group_id, span in enumerate(spans):
            @pl.when(jnp.logical_and(cond, t == group_id))
            def _(span=span):
                op(h_copy(layer, way, span))

    def halo_start(layer):
        up_ok = jnp.logical_and(s < last, jnp.logical_or(layer > 0, s == 1))
        down_ok = jnp.logical_and(s > 0, jnp.logical_or(layer > 0, s == 2))
        halo_do(layer, 0, up_ok, lambda x: x.start())
        halo_do(layer, 1, down_ok, lambda x: x.start())

    def halo_wait(layer):
        from_up = jnp.logical_and(s > 0, jnp.logical_or(layer > 0, s == 2))
        from_down = jnp.logical_and(s < last, jnp.logical_or(layer > 0, s == 1))
        halo_do(layer, 0, from_up, lambda x: x.wait_recv())
        halo_do(layer, 1, from_down, lambda x: x.wait_recv())

    def px_copy(slot, row):
        return pltpu.make_async_remote_copy(
            src_ref=pair.at[slot, row], dst_ref=pair.at[slot, row],
            send_sem=px_send.at[0], recv_sem=px_recv.at[slot],
            device_id={"tp": t1}, device_id_type=MESH,
        )

    def rs_copy(slot, k):
        return pltpu.make_async_remote_copy(
            src_ref=parts.at[slot, k], dst_ref=arrived.at[slot, k],
            send_sem=rs_send.at[0], recv_sem=rs_recv.at[slot, k],
            device_id={"tp": t2}, device_id_type=MESH,
        )

    def absorb(layer, slot, which, block, total):
        for k in range(CHUNKS):
            at = pl.ds(pl.multiple_of(block * feats + k * cols_k, cols_k), cols_k)
            wide = gathered[slot, block, k].astype(f32)
            scaled[which, :, at] = (wide * gain_ref[pl.ds(layer, 1), at]).astype(bf)
            total = total + jnp.sum(wide * wide, axis=1, keepdims=True)
        return total

    def scale_of(total):
        return lax.rsqrt(total / (tp_count * feats) + norm_eps)

    def half_dot(layer, which, first, weights):
        at = pl.ds(pl.multiple_of(first * feats, feats), 2 * feats)
        return jnp.dot(scaled[which, :, at], weights[layer, at, :], preferred_element_type=f32)

    def gate_of(layer, which, scale):
        acc = jnp.dot(scaled[which], wg[layer], preferred_element_type=f32)
        value = jax.nn.sigmoid(acc * scale)
        for k in range(CHUNKS):
            gate_buf[which, k] = value[:, k * cols_k:(k + 1) * cols_k]

    def share_pooled(slot, which, sums, cells):
        pooled = (sums / counts[which] - cells.astype(f32)).astype(bf)
        pair[slot, c] = pooled
        px_copy(slot, c).start()

    def back_part(layer, slot, cols, k):
        at = pl.ds(k * cols_k, cols_k)
        acc = jnp.dot(pair[slot, 0], wb[layer, cols, 0:b_rows, at], preferred_element_type=f32)
        return acc + jnp.dot(
            pair[slot, 1], wb[layer, cols, b_rows:2 * b_rows, at], preferred_element_type=f32
        )

    def back(layer, slot, which):
        units(px_recv.at[slot], 1).wait_recv()
        for k in range(CHUNKS):
            parts[slot, k] = back_part(layer, slot, far_base // 2, k).astype(bf)
            rs_copy(slot, k).start()
        for k in range(CHUNKS):
            own_part[which, k] = back_part(layer, slot, base // 2, k)

    def update(slot, which, k):
        units(rs_recv.at[slot, k], 1).wait_recv()
        branch = own_part[which, k] + arrived[slot, k].astype(f32)
        return (gathered[slot, t, k].astype(f32) + gate_buf[which, k] * branch).astype(bf)

    for k in range(CHUNKS):
        tok_load(k).start()
    for layer in range(LAYERS):
        for piece in (0, 2, 1):
            load(layer, piece).start()

        @pl.when(jnp.logical_and(c == s_parity, jnp.logical_or(is_mid, layer > 0)))
        def _(layer=layer):
            wb_load(layer).start()
    for layer in range(LAYERS):
        for slot in (0, 2):
            halo[layer, slot] = jnp.zeros(halo.shape[2:], halo.dtype)

    barrier = pltpu.get_barrier_semaphore()
    for target in ({"grp": other}, {"tp": t1}, {"tp": t2}):
        pl.semaphore_signal(barrier, inc=1, device_id=target, device_id_type=MESH)

    @pl.when(s > 0)
    def _():
        for peer in (t, t1):
            pl.semaphore_signal(barrier, inc=1, device_id={"sp": s - 1, "tp": peer}, device_id_type=MESH)

    @pl.when(s < last)
    def _():
        for peer in (t, t1):
            pl.semaphore_signal(barrier, inc=1, device_id={"sp": s + 1, "tp": peer}, device_id_type=MESH)

    pl.semaphore_wait(barrier, 3 + jnp.where(s > 0, 2, 0) + jnp.where(s < last, 2, 0))

    def setup():
        half_span = jnp.int32(spans[0])
        for group_id in range(1, GROUPS):
            half_span = jnp.where(t == group_id, spans[group_id], half_span)
        shift = GRID_W.bit_length() - 1
        out_tok = lax.broadcasted_iota(jnp.int32, (toks, toks), 0)
        in_tok = lax.broadcasted_iota(jnp.int32, (toks, toks), 1)
        out_row = lax.shift_right_logical(out_tok, shift)
        out_col = lax.bitwise_and(out_tok, GRID_W - 1)
        in_col = lax.bitwise_and(in_tok, GRID_W - 1)
        near_col = (in_col >= out_col - half_span) & (in_col < out_col + half_span)
        for slot in range(3):
            in_row = (slot - 1) * rows_here + lax.shift_right_logical(in_tok, shift)
            inside = near_col & (in_row >= out_row - half_span) & (in_row < out_row + half_span)
            box[slot] = jnp.where(inside, 1.0, 0.0).astype(bf)
        tok_at = lax.broadcasted_iota(jnp.int32, counts.shape[1:], 0)
        col_at = lax.bitwise_and(tok_at, GRID_W - 1)
        col_counts = jnp.minimum(col_at + half_span, GRID_W) - jnp.maximum(col_at - half_span, 0)
        for which, plane in ((0, s), (1, end_here)):
            row_at = plane * rows_here + lax.shift_right_logical(tok_at, shift)
            row_counts = jnp.minimum(row_at + half_span, total_rows) - jnp.maximum(row_at - half_span, 0)
            counts[which] = (row_counts * col_counts).astype(f32)

    def box_dot(slot, value):
        return jnp.dot(box[slot], value, preferred_element_type=f32)

    for k in range(CHUNKS):
        tok_load(k).wait()
    waited_mid, waited_end = set(), set()
    zero = jnp.zeros((toks, 1), f32)

    def relay(mid, item):
        if item[0] == "own":
            own(mid, waited_mid if mid else waited_end, *item[1:])
        else:
            pump(mid, *item[1:])

    def gather_step(layer, slot, which, k, total):
        if k == 0:
            total = absorb(layer, slot, which, t, zero)
            units(ag_recv.at[slot, 3], 2).wait_recv()
            total = absorb(layer, slot, which, t1, total)
        pass_on(slot, k)
        if k == CHUNKS - 1:
            total = absorb(layer, slot, which, t2, total)
        return total

    def pool_step(layer, slot, which, total):
        ready(layer, 0)
        acc = half_dot(layer, which, base, wp)
        units(ag_recv.at[slot, 2], 2).wait_recv()
        total = absorb(layer, slot, which, t3, total)
        scale = scale_of(total)
        acc = acc + half_dot(layer, which, far_base, wp)
        return (acc * scale).astype(bf), scale

    @pl.when(is_end)
    def _():
        for item in END_FIRST:
            if item[0] == "tok":
                guest_copy(item[1]).start()
            elif item[0] == "ret":
                if item[1] == 0:
                    setup()
                return_copy(item[1]).wait_recv()
                start_gather(1, item[1])
            else:
                relay(False, item)

    @pl.when(is_mid)
    def _():
        guest_side = jnp.where(low, 0, 2)
        total, scale = {}, {}
        for item in MID_FIRST:
            name = item[0]
            slot = item[1]
            which = 1 if slot == GUEST else 0
            if name == "gstart":
                for k in range(CHUNKS):
                    start_gather(0, k)
            elif name == "guest":
                guest_copy(slot).wait_recv()
                start_gather(GUEST, slot)
            elif name == "agf":
                if item == ("agf", 0, 0):
                    setup()
                total[slot] = gather_step(0, slot, which, item[2], total.get(slot))
            elif name == "pool" and slot == 0:
                halo[0, 1], scale[0] = pool_step(0, 0, 0, total[0])
                halo_start(0)
            elif name == "pool":
                units(ag_recv.at[GUEST, 2], 2).wait_recv()
                total[slot] = absorb(0, GUEST, 1, t3, total[slot])
                scale[slot] = scale_of(total[slot])
                acc = half_dot(0, 1, base, wp) + half_dot(0, 1, far_base, wp)
                halo[0, guest_side] = (acc * scale[slot]).astype(bf)
                cells = halo[0, guest_side]
                sums = box_dot(1, cells) + box_dot(2 - guest_side, halo[0, 1])
                share_pooled(GUEST, 1, sums, cells)
            elif name == "box":
                halo_wait(0)
                cells = halo[0, 1]
                sums = box_dot(0, halo[0, 0]) + box_dot(1, cells) + box_dot(2, halo[0, 2])
                share_pooled(0, 0, sums, cells)
            elif name == "back":
                if slot == FIRST_BACK:
                    ready(0, 2)
                back(0, slot, which)
            elif name == "gate":
                if slot == FIRST_GATE:
                    ready(0, 1)
                gate_of(0, which, scale[slot])
            elif name == "upd":
                k = item[2]
                value = update(slot, which, k)
                if slot == GUEST:
                    returned[k] = value
                    return_copy(k).start()
                else:
                    gathered[1, t, k] = value
                    start_gather(1, k)
            else:
                relay(True, item)

    steps = iter(zip(MID_REST, END_REST))

    def relays():
        for mid, items in zip((True, False), next(steps)):
            if items:
                @pl.when(is_mid if mid else is_end)
                def _(mid=mid, items=items):
                    for item in items:
                        relay(mid, item)

    for layer in range(1, LAYERS):
        total = None
        for k in range(CHUNKS):
            total = gather_step(layer, layer, 0, k, total)
            relays()
        cells, scale = pool_step(layer, layer, 0, total)
        halo[layer, 1] = cells
        halo_start(layer)
        relays()
        cells = halo[layer, 1]
        sums = box_dot(1, cells)
        halo_wait(layer)
        sums = sums + box_dot(0, halo[layer, 0]) + box_dot(2, halo[layer, 2])
        share_pooled(layer, 0, sums, cells)
        relays()
        ready(layer, 2)
        back(layer, layer, 0)
        relays()
        ready(layer, 1)
        gate_of(layer, 0, scale)
        relays()
        for k in range(CHUNKS):
            state = update(layer, 0, k)
            if layer + 1 < LAYERS:
                gathered[layer + 1, t, k] = state
                start_gather(layer + 1, k)
            else:
                out_ref[:, k * cols_k:(k + 1) * cols_k] = state
            relays()

    def sent(sem, count):
        units(sem, count).wait_send()

    def sent_blocks(flow, k, layers):
        @pl.when(c == blocks[k] % 2)
        def _():
            sent(w_send.at[flow], 5 * layers)

        @pl.when(c != blocks[k] % 2)
        def _():
            sent(w_send.at[flow], 3 * layers)

    def sent_chain(layers, slots):
        @pl.when(c != s_parity)
        def _():
            sent(bx_send.at[0], 2 * layers)
        sent(ag_send.at[0], 6 * slots)
        sent(rs_send.at[0], 2 * slots)
        sent(px_send.at[0], slots)

    @pl.when(is_mid)
    def _():
        sent(w_send.at[0], 4 * LAYERS)
        sent(w_send.at[1], 4 * (LAYERS - 1))
        for k in range(3):
            sent_blocks(2 + k, k, LAYERS)
        for k in (1, 2):
            sent_blocks(4 + k, k, LAYERS - 1)
        sent(rt_send.at[0], CHUNKS)
        sent_chain(LAYERS, LAYERS + 1)

    @pl.when(is_end)
    def _():
        sent(w_send.at[0], 4 * LAYERS)
        sent(w_send.at[1], 4 * LAYERS)
        for k in range(3):
            sent_blocks(2 + k, k, LAYERS - 1)
        sent(tk_send.at[0], CHUNKS)
        sent_chain(LAYERS - 1, LAYERS - 1)
    for layer in range(LAYERS):
        outward = layer > 0
        halo_do(layer, 0, (s < last) if outward else (s == 1), lambda x: x.wait_send())
        halo_do(layer, 1, (s > 0) if outward else (s == 2), lambda x: x.wait_send())


def fused(tokens_in, norm_gain, w_pool_in, w_gate, w_back):
    sp_count, tp_count = lax.axis_size("sp"), lax.axis_size("tp")
    toks, feats = tokens_in.shape
    _, depth, local_pool = w_pool_in.shape
    b_rows, b_cols = w_back.shape[1:]
    cols_k = feats // CHUNKS
    bf, f32 = jnp.bfloat16, jnp.float32
    dma = pltpu.SemaphoreType.DMA
    slots = LAYERS + 1
    hbm = pl.BlockSpec(memory_space=pltpu.HBM)
    vmem = pl.BlockSpec(memory_space=pltpu.VMEM)
    return pl.pallas_call(
        functools.partial(fused_kernel, sp_count, tp_count),
        out_shape=jax.ShapeDtypeStruct((toks, feats), bf),
        in_specs=[hbm, vmem, hbm, hbm, hbm],
        out_specs=vmem,
        scratch_shapes=[
            pltpu.VMEM((LAYERS, sp_count * depth, local_pool), bf),
            pltpu.VMEM((LAYERS, sp_count * depth, w_gate.shape[2]), bf),
            pltpu.VMEM((LAYERS, 2, 2 * b_rows, b_cols), bf),
            pltpu.VMEM((LAYERS, b_rows, b_cols), bf),
            pltpu.VMEM((slots, tp_count, CHUNKS, toks, cols_k), bf),
            pltpu.VMEM((2, toks, tp_count * feats), bf),
            pltpu.VMEM((LAYERS, 3, toks, local_pool), bf),
            pltpu.VMEM((2, CHUNKS, toks, cols_k), f32),
            pltpu.VMEM((2, CHUNKS, toks, cols_k), f32),
            pltpu.VMEM((3, toks, toks), bf),
            pltpu.VMEM((2, toks, local_pool), f32),
            pltpu.VMEM((slots, 2, toks, local_pool), bf),
            pltpu.VMEM((slots, CHUNKS, toks, cols_k), bf),
            pltpu.VMEM((slots, CHUNKS, toks, cols_k), bf),
            pltpu.VMEM((CHUNKS, toks, cols_k), bf),
            dma((LAYERS + 1, 4)),
            dma((7,)), dma((LAYERS, 3, 4)), dma((LAYERS, 3)),
            dma((1,)), dma((LAYERS,)),
            dma((1,)), dma((CHUNKS,)), dma((1,)), dma((CHUNKS,)),
            dma((1,)), dma((slots, 4)),
            dma((LAYERS, 2)), dma((LAYERS, 2)),
            dma((1,)), dma((slots,)),
            dma((1,)), dma((slots, CHUNKS)),
        ],
        compiler_params=pltpu.CompilerParams(
            collective_id=0, has_side_effects=True, vmem_limit_bytes=56 * 1024 * 1024
        ),
    )(tokens_in, norm_gain, w_pool_in, w_gate, w_back)


def dispatch(tokens_in, norm_gain, w_pool_in, w_gate, w_back):
    fits = (
        lax.axis_size("grp") == 2
        and lax.axis_size("tp") == GROUPS == 4
        and lax.axis_size("sp") == lax.axis_size("tp")
        and w_pool_in.shape[2] * GROUPS == POOL_WIDTH
        and w_pool_in.shape[1] == tokens_in.shape[1] == w_gate.shape[2] == w_back.shape[2]
        and tokens_in.shape[1] == 2 * tokens_in.shape[0] == 2 * w_pool_in.shape[2]
        and tokens_in.shape[0] // GRID_W >= max(pool_windows) // 2
    )
    step = fused if fits else on_device
    return step(tokens_in, norm_gain, w_pool_in, w_gate, w_back)


def solution(mesh):
    return jax.shard_map(
        dispatch,
        mesh=mesh,
        in_specs=(
            P(("grp", "sp"), "tp"),
            P(),
            P(None, "sp", "tp"),
            P(None, "sp", "tp"),
            P(None, "tp", "sp"),
        ),
        out_specs=P(("grp", "sp"), "tp"),
        check_vma=False,
    )
```

```python
import jax
import jax.numpy as jnp
from jax import lax
from jax.experimental import pallas as pl
from jax.experimental.pallas import tpu as pltpu
from jax.sharding import PartitionSpec as P
import functools

POOL_WIDTH = 1024
GROUPS = 4
GRID_W = 32
LAYERS = 3


pool_windows = (2, 4, 8, 16)
norm_eps = 1e-06


def padded_2(value, sides, width):
    for axis, dim in sides:
        peers, length = (lax.axis_size(axis), value.shape[dim])
        up = [(i, (i + 1) % peers) for i in range(peers - 1)]
        down = [(j, i) for i, j in up]
        last = lax.slice_in_dim(value, length - width, length, axis=dim)
        initial = lax.slice_in_dim(value, 0, width, axis=dim)
        before = lax.ppermute(last, axis, up)
        after = lax.ppermute(initial, axis, down)
        value = jnp.concatenate([before, value, after], axis=dim)
    return value


def window_means(padded, rows_here, first_row, total_rows, window):
    reach = max(pool_windows) // 2
    half_span = window // 2
    width_cols = padded.shape[1] - 2 * reach
    row_sums = padded[reach - half_span : reach - half_span + rows_here]
    for offset in range(1 - half_span, half_span):
        row_sums = row_sums + padded[reach + offset : reach + offset + rows_here]
    box_sums = row_sums[:, reach - half_span : reach - half_span + width_cols]
    for offset in range(1 - half_span, half_span):
        box_sums = box_sums + row_sums[:, reach + offset : reach + offset + width_cols]
    row_index = first_row + jnp.arange(rows_here, dtype=jnp.int32)
    col_index = jnp.arange(width_cols, dtype=jnp.int32)
    row_counts = jnp.minimum(row_index + half_span, total_rows) - jnp.maximum(
        row_index - half_span, 0
    )
    col_counts = jnp.minimum(col_index + half_span, width_cols) - jnp.maximum(
        col_index - half_span, 0
    )
    counts = (row_counts[:, None] * col_counts[None, :]).astype(jnp.float32)
    return box_sums / counts[:, :, None]


def on_device(tokens_in, norm_gain, w_pool_in, w_gate, w_back):
    reach = max(pool_windows) // 2
    sp_count = lax.axis_size("sp")
    tp_count = lax.axis_size("tp")
    tp_pos = lax.axis_index("tp")
    sp_pos = lax.axis_index("sp")
    tok_rows = tokens_in.shape[0]
    rows_here = tok_rows // GRID_W
    total_rows = rows_here * sp_count
    first_row = sp_pos * rows_here
    local_pool = w_pool_in.shape[2]
    group_width = POOL_WIDTH // GROUPS
    channel_group = (tp_pos * local_pool + jnp.arange(local_pool, dtype=jnp.int32)) // group_width
    state = tokens_in
    for layer_id in range(LAYERS):
        whole_rows = lax.all_gather(state, "tp", axis=1, tiled=True)
        wide = whole_rows.astype(jnp.float32)
        normed = (
            wide
            * lax.rsqrt(jnp.mean(wide * wide, axis=-1, keepdims=True) + norm_eps)
            * norm_gain[layer_id]
        ).astype(jnp.bfloat16)
        pool_acc = jnp.dot(
            normed,
            lax.all_gather(w_pool_in[layer_id], "sp", axis=0, tiled=True),
            preferred_element_type=jnp.float32,
        )
        gate_acc = jnp.dot(
            normed,
            lax.all_gather(w_gate[layer_id], "sp", axis=0, tiled=True),
            preferred_element_type=jnp.float32,
        )
        pool_in = pool_acc.astype(jnp.bfloat16)
        gate = jax.nn.sigmoid(gate_acc)
        cells = pool_in.reshape(rows_here, GRID_W, local_pool)
        rimmed = padded_2(cells, (("sp", 0),), reach)
        padded = jnp.pad(rimmed.astype(jnp.float32), ((0, 0), (reach, reach), (0, 0)))
        means = jnp.zeros((rows_here, GRID_W, local_pool), jnp.float32)
        for group_id in range(GROUPS):
            in_group = (channel_group == group_id)[None, None, :]
            means = jnp.where(
                in_group,
                window_means(padded, rows_here, first_row, total_rows, pool_windows[group_id]),
                means,
            )
        pooled = (
            (means - cells.astype(jnp.float32)).reshape(tok_rows, local_pool).astype(jnp.bfloat16)
        )
        full_pooled = lax.all_gather(pooled, "tp", axis=1, tiled=True)
        back_rows = lax.all_gather(w_back[layer_id], "sp", axis=1, tiled=True)
        back_cols = lax.all_to_all(back_rows, "tp", split_axis=1, concat_axis=0, tiled=True)
        partials = jnp.einsum(
            "tnb,nbd->ntd",
            full_pooled.reshape(tok_rows, tp_count, local_pool),
            back_cols.reshape(tp_count, local_pool, back_cols.shape[1]),
            preferred_element_type=jnp.float32,
        ).astype(jnp.bfloat16)
        branch = jnp.sum(partials.astype(jnp.float32), axis=0)
        state = (state.astype(jnp.float32) + gate * branch).astype(jnp.bfloat16)
    return state


MESH = pl.DeviceIdType.MESH
POOL, GATE_A, GATE_B, BACK = range(4)
UNITS = {POOL: (0,), GATE_A: (1,), GATE_B: (2,), BACK: (3, 4), 4: (5,), 5: (6,)}
GATE_PART = {1: 0, 2: 1, 5: 2, 6: 3}
CHUNKS = 2
GUEST = LAYERS


MID_FIRST = (
    ("own", 1, 1, 1), ("own", 0, 0, 3), ("own", 0, 0, 0), ("own", 2, 0, 3), ("own", 1, 1, 2), ("gstart", 0),
    ("own", 1, 0, 2), ("pump", 0, 1, 3), ("pump", 0, 0, 0), ("pump", 0, 1, 0), ("pump", 2, 1, 3),
    ("guest", 0), ("own", 2, 1, 3), ("own", 1, 0, 3), ("own", 2, 1, 0), ("agf", 0, 0), ("agf", 0, 1),
    ("own", 1, 0, 0), ("pump", 1, 1, 2), ("guest", 1), ("pump", 0, 2, 0), ("own", 0, 0, 1),
    ("pump", 1, 1, 3), ("own", 2, 1, 1), ("own", 2, 1, 4), ("pump", 1, 1, 0), ("agf", 3, 0), ("agf", 3, 1),
    ("pump", 0, 0, 3), ("own", 1, 1, 3), ("own", 0, 0, 2), ("pool", 0), ("pump", 0, 0, 1),
    ("pump", 0, 1, 1), ("pump", 0, 0, 2), ("pool", 3), ("own", 1, 0, 1), ("own", 2, 1, 2), ("own", 2, 1, 5),
    ("pump", 0, 2, 3), ("pump", 1, 0, 0), ("pump", 0, 1, 2), ("own", 1, 1, 0), ("box", 0), ("back", 3),
    ("pump", 0, 2, 1), ("pump", 0, 2, 2), ("back", 0), ("pump", 2, 0, 0), ("pump", 1, 0, 3),
    ("pump", 1, 1, 1), ("pump", 1, 2, 0), ("gate", 3), ("upd", 3, 0), ("upd", 3, 1), ("gate", 0),
    ("upd", 0, 0), ("upd", 0, 1), ("pump", 1, 0, 2), ("pump", 1, 2, 3), ("pump", 1, 0, 1),
)
END_FIRST = (
    ("tok", 0), ("own", 0, 0, 0), ("tok", 1), ("own", 0, 1, 2), ("own", 0, 0, 3), ("own", 0, 1, 0),
    ("pump", 2, 1, 3), ("pump", 1, 0, 2), ("own", 0, 0, 2), ("pump", 1, 0, 1), ("own", 0, 0, 1),
    ("pump", 1, 1, 2), ("pump", 2, 0, 3), ("own", 1, 0, 0), ("own", 0, 1, 3), ("own", 1, 0, 3),
    ("own", 2, 0, 0), ("own", 0, 1, 1), ("pump", 1, 1, 3), ("own", 1, 0, 2), ("pump", 2, 0, 0),
    ("own", 2, 0, 1), ("own", 2, 0, 4), ("pump", 1, 1, 0), ("pump", 1, 0, 3), ("pump", 2, 0, 2),
    ("pump", 2, 0, 5), ("own", 1, 0, 1), ("pump", 2, 0, 1), ("pump", 2, 0, 4), ("pump", 1, 2, 0),
    ("pump", 1, 0, 0), ("own", 1, 1, 0), ("own", 2, 0, 2), ("own", 2, 0, 5), ("own", 1, 1, 3), ("ret", 0),
    ("pump", 1, 1, 1), ("own", 2, 0, 3), ("ret", 1),
)
MID_REST = (
    (
        ("pump", 1, 2, 2),
    ),
    (
        ("own", 2, 0, 0),
    ),
    (
        ("pump", 2, 0, 1), ("pump", 2, 0, 4), ("pump", 1, 2, 1), ("pump", 2, 1, 0), ("pump", 2, 0, 3),
    ),
    (
        ("pump", 2, 2, 0),
    ),
    (
        ("pump", 2, 2, 1), ("pump", 2, 2, 4), ("pump", 2, 0, 2), ("pump", 2, 0, 5),
    ),
    (),
    (
        ("pump", 2, 2, 3),
    ),
    (
        ("pump", 2, 2, 2), ("pump", 2, 2, 5), ("own", 2, 0, 2), ("own", 2, 0, 5), ("pump", 2, 1, 2),
        ("pump", 2, 1, 5),
    ),
    (
        ("own", 2, 0, 1), ("own", 2, 0, 4),
    ),
    (),
    (
        ("pump", 2, 1, 1), ("pump", 2, 1, 4),
    ),
    (),
    (),
    (),
    (),
    (),
)
END_REST = (
    (),
    (
        ("pump", 1, 2, 3),
    ),
    (),
    (
        ("own", 1, 1, 1), ("pump", 1, 2, 2), ("pump", 1, 2, 1), ("own", 1, 1, 2),
    ),
    (
        ("pump", 2, 1, 0),
    ),
    (
        ("own", 2, 1, 0),
    ),
    (),
    (
        ("pump", 2, 2, 0), ("own", 2, 1, 1), ("own", 2, 1, 4), ("pump", 2, 2, 3), ("pump", 2, 2, 1),
        ("pump", 2, 2, 4),
    ),
    (),
    (),
    (
        ("pump", 2, 1, 2), ("pump", 2, 1, 5), ("own", 2, 1, 3), ("pump", 2, 2, 2), ("pump", 2, 2, 5),
        ("own", 2, 1, 2), ("own", 2, 1, 5),
    ),
    (),
    (
        ("pump", 2, 1, 1), ("pump", 2, 1, 4),
    ),
    (),
    (),
    (),
)
FIRST_BACK, FIRST_GATE = 3, 3


def fused_kernel(
    sp_count, tp_count,
    tok_hbm, gain_hbm, wp_hbm, wg_hbm, wb_hbm, out_hbm,
    wp, wg, wb, wb_own, gathered, scaled, halo, gate_buf, own_part, box, counts,
    pair, parts, arrived, returned, gain_ref, final,
    load_sem, w_send, z_recv, z_fine, y_recv, bx_send, bx_recv, tk_send, tk_recv, rt_send, rt_recv,
    ag_send, ag_recv, h_send, h_recv, px_send, px_recv, rs_send, rs_recv,
):
    g = lax.axis_index("grp")
    s = lax.axis_index("sp")
    t = lax.axis_index("tp")
    other = 1 - g
    c = t % 2
    base = t - c
    t1 = base + 1 - c
    t2 = (t + 2) % tp_count
    t3 = (t1 + 2) % tp_count
    far_base = (base + 2) % tp_count
    last = sp_count - 1
    toks, feats = tok_hbm.shape
    local_pool = wp.shape[2]
    cols_k = feats // CHUNKS
    rows_here = toks // GRID_W
    total_rows = rows_here * sp_count
    bf, f32 = jnp.bfloat16, jnp.float32

    low = s < 2
    is_mid = jnp.logical_and(s > 0, s < last)
    is_end = jnp.logical_not(is_mid)
    end_here = jnp.where(low, 0, last)
    mid_here = jnp.where(low, 1, last - 1)
    end_far = last - end_here
    mid_far = last - mid_here
    blocks = (
        jnp.where(is_mid, end_here, mid_here),
        jnp.where(is_mid, mid_far, mid_far),
        end_far,
    )
    s_parity = s % 2

    p_rows, g_rows = wp_hbm.shape[1], wg_hbm.shape[1]
    b_rows = wb_hbm.shape[1]

    def gate_cuts(layer):
        return 8 if layer == LAYERS - 1 else 4

    def view(layer, block, half, unit, row=None):
        if unit == 0:
            n = p_rows // 2
            return wp.at[layer, pl.ds(pl.multiple_of(block * p_rows + half * n, n), n), :]
        if unit in GATE_PART:
            n = g_rows // gate_cuts(layer)
            at = block * g_rows + half * (g_rows // 2) + GATE_PART[unit] * n
            return wg.at[layer, pl.ds(pl.multiple_of(at, n), n), :]
        n = b_rows // 2
        row = unit - 3 if row is None else row
        return wb.at[layer, block // 2, pl.ds(pl.multiple_of(row * b_rows + half * n, n), n), :]

    unit_rows = g_rows // 4

    def units(sem, count):
        ref = wg.at[pl.ds(0, 2 if count > 16 else 1), pl.ds(0, int(unit_rows * (count if count <= 16 else count // 2))), :]
        return pltpu.make_async_remote_copy(
            src_ref=ref, dst_ref=ref, send_sem=sem, recv_sem=sem,
            device_id={"grp": other}, device_id_type=MESH,
        )

    def w_copy(layer, flow, block, half, unit, target, recv):
        ref = view(layer, block, half, unit)
        return pltpu.make_async_remote_copy(
            src_ref=ref, dst_ref=ref, send_sem=w_send.at[flow], recv_sem=recv,
            device_id=target, device_id_type=MESH,
        )

    def kind(piece):
        return {POOL: 0, BACK: 2}.get(piece, 1)

    def z_sem(layer, k, piece):
        return z_recv.at[layer, k, piece] if piece < 4 else z_fine.at[k, piece - 4]

    def amount(layer, piece):
        if piece == BACK:
            return 2
        return 1 if piece == POOL else 4 / gate_cuts(layer)

    def own_copy(layer, flow, half, piece, plane, recv):
        if piece != BACK:
            return w_copy(layer, flow, s, half, UNITS[piece][0], {"sp": plane}, recv)
        n = b_rows // 2
        return pltpu.make_async_remote_copy(
            src_ref=wb_own.at[layer, pl.ds(pl.multiple_of(half * n, n), n), :],
            dst_ref=view(layer, s, half, 3, row=c),
            send_sem=w_send.at[flow], recv_sem=recv,
            device_id={"sp": plane, "tp": base + s_parity}, device_id_type=MESH,
        )

    def holds(block, piece, fn):
        if piece == BACK:
            pl.when(c == block % 2)(fn)
        else:
            fn()

    def pump(mid, layer, k, piece):
        block = blocks[k]

        def act():
            units(z_sem(layer, k, piece), amount(layer, piece)).wait_recv()
            for unit in UNITS[piece]:
                if k == 0 and mid:
                    w_copy(layer, 2, block, g, unit, {"sp": mid_far}, z_sem(layer, 2, piece)).start()
                    continue
                w_copy(
                    layer, 2 + k, block, g, unit, {"grp": other}, y_recv.at[layer, kind(piece)]
                ).start()
                if mid and layer > 0:
                    w_copy(
                        layer, 4 + k, block, g, unit, {"sp": end_here}, z_sem(layer, k, piece)
                    ).start()
        holds(block, piece, act)

    def own(mid, waited, layer, flow, piece):
        if (layer, kind(piece)) not in waited:
            waited.add((layer, kind(piece)))
            load(layer, kind(piece)).wait()
            if piece == BACK and (mid or layer > 0):
                @pl.when(c != s_parity)
                def _():
                    bx_copy(layer).start()
        if mid and flow == 0:
            own_copy(layer, 0, g, piece, mid_far, z_sem(layer, 1, piece)).start()
        elif mid:
            own_copy(layer, 1, g, piece, end_here, z_sem(layer, 0, piece)).start()
        elif flow == 0:
            own_copy(layer, 0, g, piece, mid_here, z_sem(layer, 0, piece)).start()
        else:
            own_copy(layer, 1, other, piece, mid_here, y_recv.at[layer, kind(piece)]).start()

    def bx_copy(layer):
        return pltpu.make_async_remote_copy(
            src_ref=wb_own.at[layer],
            dst_ref=wb.at[layer, s // 2, pl.ds(pl.multiple_of(c * b_rows, b_rows), b_rows), :],
            send_sem=bx_send.at[0], recv_sem=bx_recv.at[layer],
            device_id={"tp": t1}, device_id_type=MESH,
        )

    def wb_load(layer):
        return pltpu.make_async_copy(
            wb_hbm.at[layer],
            wb.at[layer, s // 2, pl.ds(pl.multiple_of(c * b_rows, b_rows), b_rows), :],
            load_sem.at[layer, 3],
        )

    def load(layer, piece):
        if piece == 0:
            src, dst = wp_hbm.at[layer], wp.at[layer, pl.ds(pl.multiple_of(s * p_rows, p_rows), p_rows), :]
        elif piece == 1:
            src, dst = wg_hbm.at[layer], wg.at[layer, pl.ds(pl.multiple_of(s * g_rows, g_rows), g_rows), :]
        else:
            src, dst = wb_hbm.at[layer], wb_own.at[layer]
        return pltpu.make_async_copy(src, dst, load_sem.at[layer, piece])

    def ready(layer, which):
        if which < 2:
            units(y_recv.at[layer, which], 3 * (1 + which)).wait_recv()
            return

        @pl.when(c == s_parity)
        def _():
            units(y_recv.at[layer, 2], 2).wait_recv()
            wb_load(layer).wait()
            units(bx_recv.at[layer], 2).wait_recv()

        @pl.when(c != s_parity)
        def _():
            units(y_recv.at[layer, 2], 4).wait_recv()

    def tok_load(k):
        return pltpu.make_async_copy(
            tok_hbm.at[:, pl.ds(k * cols_k, cols_k)], gathered.at[0, t, k], load_sem.at[LAYERS, k]
        )

    gain_load = pltpu.make_async_copy(gain_hbm, gain_ref, load_sem.at[LAYERS, CHUNKS])

    def out_copy(k):
        return pltpu.make_async_copy(
            final.at[k], out_hbm.at[:, pl.ds(k * cols_k, cols_k)], load_sem.at[0, k]
        )

    def guest_copy(k):
        return pltpu.make_async_remote_copy(
            src_ref=gathered.at[0, t, k], dst_ref=gathered.at[GUEST, t, k],
            send_sem=tk_send.at[0], recv_sem=tk_recv.at[k],
            device_id={"sp": mid_here}, device_id_type=MESH,
        )

    def return_copy(k):
        return pltpu.make_async_remote_copy(
            src_ref=returned.at[k], dst_ref=gathered.at[1, t, k],
            send_sem=rt_send.at[0], recv_sem=rt_recv.at[k],
            device_id={"sp": end_here}, device_id_type=MESH,
        )

    def ag_copy(slot, k, block, target, recv):
        return pltpu.make_async_remote_copy(
            src_ref=gathered.at[slot, block, k], dst_ref=gathered.at[slot, block, k],
            send_sem=ag_send.at[0], recv_sem=ag_recv.at[slot, recv],
            device_id={"tp": target}, device_id_type=MESH,
        )

    def start_gather(slot, k):
        ag_copy(slot, k, t, t2, k).start()
        ag_copy(slot, k, t, t1, 3).start()

    def pass_on(slot, k):
        units(ag_recv.at[slot, k], 1).wait_recv()
        ag_copy(slot, k, t2, t1, 2).start()

    spans = [w // 2 for w in pool_windows]

    def h_copy(layer, way, span):
        rows = (span if way == 0 else max(span - 1, 1)) * GRID_W
        at = toks - rows if way == 0 else 0
        return pltpu.make_async_remote_copy(
            src_ref=halo.at[layer, 1, pl.ds(at, rows), :],
            dst_ref=halo.at[layer, 0 if way == 0 else 2, pl.ds(at, rows), :],
            send_sem=h_send.at[layer, way], recv_sem=h_recv.at[layer, way],
            device_id={"sp": s + 1 if way == 0 else s - 1}, device_id_type=MESH,
        )

    def halo_do(layer, way, cond, op):
        for group_id, span in enumerate(spans):
            @pl.when(jnp.logical_and(cond, t == group_id))
            def _(span=span):
                op(h_copy(layer, way, span))

    def halo_start(layer):
        up_ok = jnp.logical_and(s < last, jnp.logical_or(layer > 0, s == 1))
        down_ok = jnp.logical_and(s > 0, jnp.logical_or(layer > 0, s == 2))
        halo_do(layer, 0, up_ok, lambda x: x.start())
        halo_do(layer, 1, down_ok, lambda x: x.start())

    def halo_wait(layer):
        from_up = jnp.logical_and(s > 0, jnp.logical_or(layer > 0, s == 2))
        from_down = jnp.logical_and(s < last, jnp.logical_or(layer > 0, s == 1))
        halo_do(layer, 0, from_up, lambda x: x.wait_recv())
        halo_do(layer, 1, from_down, lambda x: x.wait_recv())

    def px_copy(slot, row):
        return pltpu.make_async_remote_copy(
            src_ref=pair.at[slot, row], dst_ref=pair.at[slot, row],
            send_sem=px_send.at[0], recv_sem=px_recv.at[slot],
            device_id={"tp": t1}, device_id_type=MESH,
        )

    def rs_copy(slot, k):
        return pltpu.make_async_remote_copy(
            src_ref=parts.at[slot, k], dst_ref=arrived.at[slot, k],
            send_sem=rs_send.at[0], recv_sem=rs_recv.at[slot, k],
            device_id={"tp": t2}, device_id_type=MESH,
        )

    def absorb(layer, slot, which, block, total):
        for k in range(CHUNKS):
            at = pl.ds(pl.multiple_of(block * feats + k * cols_k, cols_k), cols_k)
            wide = gathered[slot, block, k].astype(f32)
            scaled[which, :, at] = (wide * gain_ref[pl.ds(layer, 1), at]).astype(bf)
            total = total + jnp.sum(wide * wide, axis=1, keepdims=True)
        return total

    def scale_of(total):
        return lax.rsqrt(total / (tp_count * feats) + norm_eps)

    def half_dot(layer, which, first, weights):
        at = pl.ds(pl.multiple_of(first * feats, feats), 2 * feats)
        return jnp.dot(scaled[which, :, at], weights[layer, at, :], preferred_element_type=f32)

    def gate_of(layer, which, scale):
        acc = jnp.dot(scaled[which], wg[layer], preferred_element_type=f32)
        value = jax.nn.sigmoid(acc * scale)
        for k in range(CHUNKS):
            gate_buf[which, k] = value[:, k * cols_k:(k + 1) * cols_k]

    def share_pooled(slot, which, sums, cells):
        pooled = (sums / counts[which] - cells.astype(f32)).astype(bf)
        pair[slot, c] = pooled
        px_copy(slot, c).start()

    def back_part(layer, slot, cols, k):
        at = pl.ds(k * cols_k, cols_k)
        acc = jnp.dot(pair[slot, 0], wb[layer, cols, 0:b_rows, at], preferred_element_type=f32)
        return acc + jnp.dot(
            pair[slot, 1], wb[layer, cols, b_rows:2 * b_rows, at], preferred_element_type=f32
        )

    def back(layer, slot, which):
        units(px_recv.at[slot], 1).wait_recv()
        for k in range(CHUNKS):
            parts[slot, k] = back_part(layer, slot, far_base // 2, k).astype(bf)
            rs_copy(slot, k).start()
        for k in range(CHUNKS):
            own_part[which, k] = back_part(layer, slot, base // 2, k)

    def update(slot, which, k):
        units(rs_recv.at[slot, k], 1).wait_recv()
        branch = own_part[which, k] + arrived[slot, k].astype(f32)
        return (gathered[slot, t, k].astype(f32) + gate_buf[which, k] * branch).astype(bf)

    for k in range(CHUNKS):
        tok_load(k).start()
    gain_load.start()
    for layer in range(LAYERS):
        for piece in (0, 2, 1):
            load(layer, piece).start()

        @pl.when(jnp.logical_and(c == s_parity, jnp.logical_or(is_mid, layer > 0)))
        def _(layer=layer):
            wb_load(layer).start()
    for layer in range(LAYERS):
        for slot in (0, 2):
            halo[layer, slot] = jnp.zeros(halo.shape[2:], halo.dtype)

    barrier = pltpu.get_barrier_semaphore()
    for target in ({"grp": other}, {"tp": t1}, {"tp": t2}):
        pl.semaphore_signal(barrier, inc=1, device_id=target, device_id_type=MESH)

    @pl.when(s > 0)
    def _():
        for peer in (t, t1):
            pl.semaphore_signal(barrier, inc=1, device_id={"sp": s - 1, "tp": peer}, device_id_type=MESH)

    @pl.when(s < last)
    def _():
        for peer in (t, t1):
            pl.semaphore_signal(barrier, inc=1, device_id={"sp": s + 1, "tp": peer}, device_id_type=MESH)

    pl.semaphore_wait(barrier, 3 + jnp.where(s > 0, 2, 0) + jnp.where(s < last, 2, 0))

    def setup():
        half_span = jnp.int32(spans[0])
        for group_id in range(1, GROUPS):
            half_span = jnp.where(t == group_id, spans[group_id], half_span)
        shift = GRID_W.bit_length() - 1
        out_tok = lax.broadcasted_iota(jnp.int32, (toks, toks), 0)
        in_tok = lax.broadcasted_iota(jnp.int32, (toks, toks), 1)
        out_row = lax.shift_right_logical(out_tok, shift)
        out_col = lax.bitwise_and(out_tok, GRID_W - 1)
        in_col = lax.bitwise_and(in_tok, GRID_W - 1)
        near_col = (in_col >= out_col - half_span) & (in_col < out_col + half_span)
        for slot in range(3):
            in_row = (slot - 1) * rows_here + lax.shift_right_logical(in_tok, shift)
            inside = near_col & (in_row >= out_row - half_span) & (in_row < out_row + half_span)
            box[slot] = jnp.where(inside, 1.0, 0.0).astype(bf)
        tok_at = lax.broadcasted_iota(jnp.int32, counts.shape[1:], 0)
        col_at = lax.bitwise_and(tok_at, GRID_W - 1)
        col_counts = jnp.minimum(col_at + half_span, GRID_W) - jnp.maximum(col_at - half_span, 0)
        for which, plane in ((0, s), (1, end_here)):
            row_at = plane * rows_here + lax.shift_right_logical(tok_at, shift)
            row_counts = jnp.minimum(row_at + half_span, total_rows) - jnp.maximum(row_at - half_span, 0)
            counts[which] = (row_counts * col_counts).astype(f32)

    def box_dot(slot, value):
        return jnp.dot(box[slot], value, preferred_element_type=f32)

    for k in range(CHUNKS):
        tok_load(k).wait()
    gain_load.wait()
    waited_mid, waited_end = set(), set()
    zero = jnp.zeros((toks, 1), f32)

    def relay(mid, item):
        if item[0] == "own":
            own(mid, waited_mid if mid else waited_end, *item[1:])
        else:
            pump(mid, *item[1:])

    def gather_step(layer, slot, which, k, total):
        if k == 0:
            total = absorb(layer, slot, which, t, zero)
            units(ag_recv.at[slot, 3], 2).wait_recv()
            total = absorb(layer, slot, which, t1, total)
        pass_on(slot, k)
        if k == CHUNKS - 1:
            total = absorb(layer, slot, which, t2, total)
        return total

    def pool_step(layer, slot, which, total):
        ready(layer, 0)
        acc = half_dot(layer, which, base, wp)
        units(ag_recv.at[slot, 2], 2).wait_recv()
        total = absorb(layer, slot, which, t3, total)
        scale = scale_of(total)
        acc = acc + half_dot(layer, which, far_base, wp)
        return (acc * scale).astype(bf), scale

    @pl.when(is_end)
    def _():
        for item in END_FIRST:
            if item[0] == "tok":
                guest_copy(item[1]).start()
            elif item[0] == "ret":
                if item[1] == 0:
                    setup()
                return_copy(item[1]).wait_recv()
                start_gather(1, item[1])
            else:
                relay(False, item)

    @pl.when(is_mid)
    def _():
        guest_side = jnp.where(low, 0, 2)
        total, scale = {}, {}
        for item in MID_FIRST:
            name = item[0]
            slot = item[1]
            which = 1 if slot == GUEST else 0
            if name == "gstart":
                for k in range(CHUNKS):
                    start_gather(0, k)
            elif name == "guest":
                guest_copy(slot).wait_recv()
                start_gather(GUEST, slot)
            elif name == "agf":
                if item == ("agf", 0, 0):
                    setup()
                total[slot] = gather_step(0, slot, which, item[2], total.get(slot))
            elif name == "pool" and slot == 0:
                halo[0, 1], scale[0] = pool_step(0, 0, 0, total[0])
                halo_start(0)
            elif name == "pool":
                units(ag_recv.at[GUEST, 2], 2).wait_recv()
                total[slot] = absorb(0, GUEST, 1, t3, total[slot])
                scale[slot] = scale_of(total[slot])
                acc = half_dot(0, 1, base, wp) + half_dot(0, 1, far_base, wp)
                halo[0, guest_side] = (acc * scale[slot]).astype(bf)
                cells = halo[0, guest_side]
                sums = box_dot(1, cells) + box_dot(2 - guest_side, halo[0, 1])
                share_pooled(GUEST, 1, sums, cells)
            elif name == "box":
                halo_wait(0)
                cells = halo[0, 1]
                sums = box_dot(0, halo[0, 0]) + box_dot(1, cells) + box_dot(2, halo[0, 2])
                share_pooled(0, 0, sums, cells)
            elif name == "back":
                if slot == FIRST_BACK:
                    ready(0, 2)
                back(0, slot, which)
            elif name == "gate":
                if slot == FIRST_GATE:
                    ready(0, 1)
                gate_of(0, which, scale[slot])
            elif name == "upd":
                k = item[2]
                value = update(slot, which, k)
                if slot == GUEST:
                    returned[k] = value
                    return_copy(k).start()
                else:
                    gathered[1, t, k] = value
                    start_gather(1, k)
            else:
                relay(True, item)

    steps = iter(zip(MID_REST, END_REST))

    def relays():
        for mid, items in zip((True, False), next(steps)):
            if items:
                @pl.when(is_mid if mid else is_end)
                def _(mid=mid, items=items):
                    for item in items:
                        relay(mid, item)

    for layer in range(1, LAYERS):
        total = None
        for k in range(CHUNKS):
            total = gather_step(layer, layer, 0, k, total)
            relays()
        cells, scale = pool_step(layer, layer, 0, total)
        halo[layer, 1] = cells
        halo_start(layer)
        relays()
        cells = halo[layer, 1]
        sums = box_dot(1, cells)
        halo_wait(layer)
        sums = sums + box_dot(0, halo[layer, 0]) + box_dot(2, halo[layer, 2])
        share_pooled(layer, 0, sums, cells)
        relays()
        ready(layer, 2)
        back(layer, layer, 0)
        relays()
        ready(layer, 1)
        gate_of(layer, 0, scale)
        relays()
        for k in range(CHUNKS):
            state = update(layer, 0, k)
            if layer + 1 < LAYERS:
                gathered[layer + 1, t, k] = state
                start_gather(layer + 1, k)
            else:
                final[k] = state
                out_copy(k).start()
            relays()

    def sent(sem, count):
        units(sem, count).wait_send()

    def sent_blocks(flow, k, layers):
        @pl.when(c == blocks[k] % 2)
        def _():
            sent(w_send.at[flow], 5 * layers)

        @pl.when(c != blocks[k] % 2)
        def _():
            sent(w_send.at[flow], 3 * layers)

    def sent_chain(layers, slots):
        @pl.when(c != s_parity)
        def _():
            sent(bx_send.at[0], 2 * layers)
        sent(ag_send.at[0], 6 * slots)
        sent(rs_send.at[0], 2 * slots)
        sent(px_send.at[0], slots)

    @pl.when(is_mid)
    def _():
        sent(w_send.at[0], 4 * LAYERS)
        sent(w_send.at[1], 4 * (LAYERS - 1))
        for k in range(3):
            sent_blocks(2 + k, k, LAYERS)
        for k in (1, 2):
            sent_blocks(4 + k, k, LAYERS - 1)
        sent(rt_send.at[0], CHUNKS)
        sent_chain(LAYERS, LAYERS + 1)

    @pl.when(is_end)
    def _():
        sent(w_send.at[0], 4 * LAYERS)
        sent(w_send.at[1], 4 * LAYERS)
        for k in range(3):
            sent_blocks(2 + k, k, LAYERS - 1)
        sent(tk_send.at[0], CHUNKS)
        sent_chain(LAYERS - 1, LAYERS - 1)
    for layer in range(LAYERS):
        outward = layer > 0
        halo_do(layer, 0, (s < last) if outward else (s == 1), lambda x: x.wait_send())
        halo_do(layer, 1, (s > 0) if outward else (s == 2), lambda x: x.wait_send())
    for k in range(CHUNKS):
        out_copy(k).wait()


def fused(tokens_in, norm_gain, w_pool_in, w_gate, w_back):
    sp_count, tp_count = lax.axis_size("sp"), lax.axis_size("tp")
    toks, feats = tokens_in.shape
    _, depth, local_pool = w_pool_in.shape
    b_rows, b_cols = w_back.shape[1:]
    cols_k = feats // CHUNKS
    bf, f32 = jnp.bfloat16, jnp.float32
    dma = pltpu.SemaphoreType.DMA
    slots = LAYERS + 1
    hbm = pl.BlockSpec(memory_space=pltpu.HBM)
    return pl.pallas_call(
        functools.partial(fused_kernel, sp_count, tp_count),
        out_shape=jax.ShapeDtypeStruct((toks, feats), bf),
        in_specs=[hbm] * 5,
        out_specs=hbm,
        scratch_shapes=[
            pltpu.VMEM((LAYERS, sp_count * depth, local_pool), bf),
            pltpu.VMEM((LAYERS, sp_count * depth, w_gate.shape[2]), bf),
            pltpu.VMEM((LAYERS, 2, 2 * b_rows, b_cols), bf),
            pltpu.VMEM((LAYERS, b_rows, b_cols), bf),
            pltpu.VMEM((slots, tp_count, CHUNKS, toks, cols_k), bf),
            pltpu.VMEM((2, toks, tp_count * feats), bf),
            pltpu.VMEM((LAYERS, 3, toks, local_pool), bf),
            pltpu.VMEM((2, CHUNKS, toks, cols_k), f32),
            pltpu.VMEM((2, CHUNKS, toks, cols_k), f32),
            pltpu.VMEM((3, toks, toks), bf),
            pltpu.VMEM((2, toks, local_pool), f32),
            pltpu.VMEM((slots, 2, toks, local_pool), bf),
            pltpu.VMEM((slots, CHUNKS, toks, cols_k), bf),
            pltpu.VMEM((slots, CHUNKS, toks, cols_k), bf),
            pltpu.VMEM((CHUNKS, toks, cols_k), bf),
            pltpu.VMEM(norm_gain.shape, f32),
            pltpu.VMEM((CHUNKS, toks, cols_k), bf),
            dma((LAYERS + 1, 4)),
            dma((7,)), dma((LAYERS, 3, 4)), dma((3, 2)), dma((LAYERS, 3)),
            dma((1,)), dma((LAYERS,)),
            dma((1,)), dma((CHUNKS,)), dma((1,)), dma((CHUNKS,)),
            dma((1,)), dma((slots, 4)),
            dma((LAYERS, 2)), dma((LAYERS, 2)),
            dma((1,)), dma((slots,)),
            dma((1,)), dma((slots, CHUNKS)),
        ],
        compiler_params=pltpu.CompilerParams(
            collective_id=0, has_side_effects=True, vmem_limit_bytes=56 * 1024 * 1024
        ),
    )(tokens_in, norm_gain, w_pool_in, w_gate, w_back)

def dispatch(tokens_in, norm_gain, w_pool_in, w_gate, w_back):
    fits = (
        lax.axis_size("grp") == 2
        and lax.axis_size("tp") == GROUPS == 4
        and lax.axis_size("sp") == lax.axis_size("tp")
        and w_pool_in.shape[2] * GROUPS == POOL_WIDTH
        and w_pool_in.shape[1] == tokens_in.shape[1] == w_gate.shape[2] == w_back.shape[2]
        and tokens_in.shape[1] == 2 * tokens_in.shape[0] == 2 * w_pool_in.shape[2]
        and tokens_in.shape[0] // GRID_W >= max(pool_windows) // 2
    )
    step = fused if fits else on_device
    return step(tokens_in, norm_gain, w_pool_in, w_gate, w_back)


def solution(mesh):
    return jax.shard_map(
        dispatch,
        mesh=mesh,
        in_specs=(
            P(("grp", "sp"), "tp"),
            P(),
            P(None, "sp", "tp"),
            P(None, "sp", "tp"),
            P(None, "tp", "sp"),
        ),
        out_specs=P(("grp", "sp"), "tp"),
        check_vma=False,
    )
```

```python
import jax
import jax.numpy as jnp
from jax import lax
from jax.experimental import pallas as pl
from jax.experimental.pallas import tpu as pltpu
from jax.sharding import PartitionSpec as P
import functools

POOL_WIDTH = 1024
GROUPS = 4
GRID_W = 32
LAYERS = 3


pool_windows = (2, 4, 8, 16)
norm_eps = 1e-06


def padded_2(value, sides, width):
    for axis, dim in sides:
        peers, length = (lax.axis_size(axis), value.shape[dim])
        up = [(i, (i + 1) % peers) for i in range(peers - 1)]
        down = [(j, i) for i, j in up]
        last = lax.slice_in_dim(value, length - width, length, axis=dim)
        initial = lax.slice_in_dim(value, 0, width, axis=dim)
        before = lax.ppermute(last, axis, up)
        after = lax.ppermute(initial, axis, down)
        value = jnp.concatenate([before, value, after], axis=dim)
    return value


def window_means(padded, rows_here, first_row, total_rows, window):
    reach = max(pool_windows) // 2
    half_span = window // 2
    width_cols = padded.shape[1] - 2 * reach
    row_sums = padded[reach - half_span : reach - half_span + rows_here]
    for offset in range(1 - half_span, half_span):
        row_sums = row_sums + padded[reach + offset : reach + offset + rows_here]
    box_sums = row_sums[:, reach - half_span : reach - half_span + width_cols]
    for offset in range(1 - half_span, half_span):
        box_sums = box_sums + row_sums[:, reach + offset : reach + offset + width_cols]
    row_index = first_row + jnp.arange(rows_here, dtype=jnp.int32)
    col_index = jnp.arange(width_cols, dtype=jnp.int32)
    row_counts = jnp.minimum(row_index + half_span, total_rows) - jnp.maximum(
        row_index - half_span, 0
    )
    col_counts = jnp.minimum(col_index + half_span, width_cols) - jnp.maximum(
        col_index - half_span, 0
    )
    counts = (row_counts[:, None] * col_counts[None, :]).astype(jnp.float32)
    return box_sums / counts[:, :, None]


def on_device(tokens_in, norm_gain, w_pool_in, w_gate, w_back):
    reach = max(pool_windows) // 2
    sp_count = lax.axis_size("sp")
    tp_count = lax.axis_size("tp")
    tp_pos = lax.axis_index("tp")
    sp_pos = lax.axis_index("sp")
    tok_rows = tokens_in.shape[0]
    rows_here = tok_rows // GRID_W
    total_rows = rows_here * sp_count
    first_row = sp_pos * rows_here
    local_pool = w_pool_in.shape[2]
    group_width = POOL_WIDTH // GROUPS
    channel_group = (tp_pos * local_pool + jnp.arange(local_pool, dtype=jnp.int32)) // group_width
    state = tokens_in
    for layer_id in range(LAYERS):
        whole_rows = lax.all_gather(state, "tp", axis=1, tiled=True)
        wide = whole_rows.astype(jnp.float32)
        normed = (
            wide
            * lax.rsqrt(jnp.mean(wide * wide, axis=-1, keepdims=True) + norm_eps)
            * norm_gain[layer_id]
        ).astype(jnp.bfloat16)
        pool_acc = jnp.dot(
            normed,
            lax.all_gather(w_pool_in[layer_id], "sp", axis=0, tiled=True),
            preferred_element_type=jnp.float32,
        )
        gate_acc = jnp.dot(
            normed,
            lax.all_gather(w_gate[layer_id], "sp", axis=0, tiled=True),
            preferred_element_type=jnp.float32,
        )
        pool_in = pool_acc.astype(jnp.bfloat16)
        gate = jax.nn.sigmoid(gate_acc)
        cells = pool_in.reshape(rows_here, GRID_W, local_pool)
        rimmed = padded_2(cells, (("sp", 0),), reach)
        padded = jnp.pad(rimmed.astype(jnp.float32), ((0, 0), (reach, reach), (0, 0)))
        means = jnp.zeros((rows_here, GRID_W, local_pool), jnp.float32)
        for group_id in range(GROUPS):
            in_group = (channel_group == group_id)[None, None, :]
            means = jnp.where(
                in_group,
                window_means(padded, rows_here, first_row, total_rows, pool_windows[group_id]),
                means,
            )
        pooled = (
            (means - cells.astype(jnp.float32)).reshape(tok_rows, local_pool).astype(jnp.bfloat16)
        )
        full_pooled = lax.all_gather(pooled, "tp", axis=1, tiled=True)
        back_rows = lax.all_gather(w_back[layer_id], "sp", axis=1, tiled=True)
        back_cols = lax.all_to_all(back_rows, "tp", split_axis=1, concat_axis=0, tiled=True)
        partials = jnp.einsum(
            "tnb,nbd->ntd",
            full_pooled.reshape(tok_rows, tp_count, local_pool),
            back_cols.reshape(tp_count, local_pool, back_cols.shape[1]),
            preferred_element_type=jnp.float32,
        ).astype(jnp.bfloat16)
        branch = jnp.sum(partials.astype(jnp.float32), axis=0)
        state = (state.astype(jnp.float32) + gate * branch).astype(jnp.bfloat16)
    return state


MESH = pl.DeviceIdType.MESH
POOL, GATE_A, GATE_B, BACK = range(4)
UNITS = {POOL: (0,), GATE_A: (1,), GATE_B: (2,), BACK: (3, 4), 4: (5,), 5: (6,)}
GATE_PART = {1: 0, 2: 1, 5: 2, 6: 3}
CHUNKS = 2
GUEST = LAYERS


MID_FIRST = (
    ("own", 1, 1, 0), ("own", 1, 0, 1), ("own", 0, 0, 2), ("own", 2, 1, 4), ("gstart", 0), ("own", 1, 1, 1),
    ("own", 2, 1, 0), ("own", 0, 0, 0), ("own", 0, 0, 3), ("own", 2, 1, 5), ("pump", 0, 0, 3),
    ("own", 1, 1, 3), ("own", 2, 1, 2), ("pump", 0, 0, 0), ("own", 1, 1, 2), ("pump", 1, 1, 1),
    ("own", 0, 0, 1), ("pump", 0, 1, 0), ("guest", 0), ("pump", 0, 1, 3), ("own", 2, 1, 3),
    ("pump", 0, 1, 2), ("guest", 1), ("agf", 0, 0), ("pump", 0, 2, 0), ("agf", 0, 1), ("pump", 0, 0, 1),
    ("pump", 0, 0, 2), ("pump", 0, 2, 3), ("own", 2, 1, 1), ("agf", 3, 0), ("own", 1, 0, 0), ("agf", 3, 1),
    ("pump", 0, 1, 1), ("pool", 0), ("pool", 3), ("pump", 1, 0, 3), ("pump", 0, 2, 1), ("pump", 0, 2, 2),
    ("back", 3), ("pump", 1, 1, 0), ("box", 0), ("pump", 1, 2, 3), ("pump", 1, 0, 0), ("own", 1, 0, 3),
    ("back", 0), ("gate", 3), ("upd", 3, 0), ("upd", 3, 1), ("own", 1, 0, 2), ("gate", 0),
    ("pump", 1, 2, 0), ("upd", 0, 0), ("pump", 1, 0, 1), ("upd", 0, 1), ("pump", 1, 1, 3), ("own", 2, 0, 0),
    ("pump", 1, 2, 1), ("pump", 1, 0, 2),
)
END_FIRST = (
    ("own", 0, 0, 0), ("own", 0, 0, 3), ("tok", 0), ("tok", 1), ("own", 0, 1, 0), ("own", 0, 0, 1),
    ("own", 0, 0, 2), ("own", 0, 1, 3), ("own", 1, 0, 3), ("own", 1, 0, 0), ("own", 0, 1, 2),
    ("own", 0, 1, 1), ("own", 1, 0, 1), ("own", 1, 0, 2), ("pump", 1, 0, 0), ("own", 1, 1, 0),
    ("own", 2, 0, 3), ("pump", 2, 0, 5), ("own", 2, 0, 0), ("pump", 1, 0, 2), ("pump", 1, 1, 1),
    ("own", 1, 1, 3), ("pump", 2, 0, 2), ("pump", 1, 0, 3), ("pump", 1, 0, 1), ("pump", 2, 0, 3),
    ("pump", 2, 0, 4), ("own", 2, 0, 4), ("own", 2, 0, 2), ("pump", 1, 2, 3), ("ret", 0), ("pump", 2, 0, 0),
    ("pump", 1, 1, 0), ("ret", 1), ("pump", 1, 2, 0),
)
MID_REST = (
    (),
    (),
    (
        ("pump", 2, 0, 0), ("pump", 2, 0, 3), ("pump", 1, 2, 2), ("pump", 1, 1, 2), ("own", 2, 0, 5),
        ("own", 2, 0, 3),
    ),
    (
        ("pump", 2, 1, 0),
    ),
    (
        ("pump", 2, 2, 0), ("pump", 2, 2, 3), ("pump", 2, 0, 2), ("own", 2, 0, 2), ("pump", 2, 0, 4),
        ("own", 2, 0, 4), ("pump", 2, 1, 3),
    ),
    (),
    (),
    (
        ("pump", 2, 2, 4), ("pump", 2, 0, 5), ("own", 2, 0, 1), ("pump", 2, 0, 1), ("pump", 2, 2, 2),
        ("pump", 2, 1, 2),
    ),
    (
        ("pump", 2, 1, 4),
    ),
    (),
    (
        ("pump", 2, 2, 5), ("pump", 2, 2, 1), ("pump", 2, 1, 5), ("pump", 2, 1, 1),
    ),
    (),
    (),
    (),
    (),
    (),
)
END_REST = (
    (
        ("pump", 1, 1, 3), ("pump", 2, 0, 1),
    ),
    (),
    (
        ("pump", 1, 2, 1), ("own", 1, 1, 2),
    ),
    (
        ("pump", 1, 2, 2), ("own", 1, 1, 1),
    ),
    (
        ("own", 2, 1, 1), ("pump", 1, 1, 2), ("own", 2, 0, 5), ("own", 2, 0, 1), ("pump", 2, 1, 0),
        ("own", 2, 1, 5),
    ),
    (),
    (
        ("pump", 2, 2, 0), ("own", 2, 1, 0), ("own", 2, 1, 2),
    ),
    (
        ("pump", 2, 1, 3), ("pump", 2, 2, 3),
    ),
    (),
    (
        ("own", 2, 1, 4), ("pump", 2, 2, 4),
    ),
    (
        ("pump", 2, 2, 2), ("pump", 2, 1, 2), ("pump", 2, 1, 4), ("own", 2, 1, 3),
    ),
    (
        ("pump", 2, 2, 5), ("pump", 2, 2, 1),
    ),
    (
        ("pump", 2, 1, 5), ("pump", 2, 1, 1),
    ),
    (),
    (),
    (),
)
FIRST_BACK, FIRST_GATE = 3, 3


def fused_kernel(
    sp_count, tp_count,
    tok_hbm, gain_hbm, wp_hbm, wg_hbm, wb_hbm, out_hbm,
    wp, wg, wb, wb_own, gathered, scaled, halo, gate_buf, own_part, box, counts,
    pair, parts, arrived, returned, gain_ref, final,
    load_sem, w_send, z_recv, z_fine, y_recv, bx_send, bx_recv, tk_send, tk_recv, rt_send, rt_recv,
    ag_send, ag_recv, h_send, h_recv, px_send, px_recv, rs_send, rs_recv,
):
    g = lax.axis_index("grp")
    s = lax.axis_index("sp")
    t = lax.axis_index("tp")
    other = 1 - g
    c = t % 2
    base = t - c
    t1 = base + 1 - c
    t2 = (t + 2) % tp_count
    t3 = (t1 + 2) % tp_count
    far_base = (base + 2) % tp_count
    last = sp_count - 1
    toks, feats = tok_hbm.shape
    local_pool = wp.shape[2]
    cols_k = feats // CHUNKS
    rows_here = toks // GRID_W
    total_rows = rows_here * sp_count
    bf, f32 = jnp.bfloat16, jnp.float32

    low = s < 2
    is_mid = jnp.logical_and(s > 0, s < last)
    is_end = jnp.logical_not(is_mid)
    end_here = jnp.where(low, 0, last)
    mid_here = jnp.where(low, 1, last - 1)
    end_far = last - end_here
    mid_far = last - mid_here
    blocks = (
        jnp.where(is_mid, end_here, mid_here),
        jnp.where(is_mid, mid_far, mid_far),
        end_far,
    )
    s_parity = s % 2

    p_rows, g_rows = wp_hbm.shape[1], wg_hbm.shape[1]
    b_rows = wb_hbm.shape[1]

    def gate_cuts(layer):
        return 8 if layer == LAYERS - 1 else 4

    def view(layer, block, half, unit, row=None):
        if unit == 0:
            n = p_rows // 2
            return wp.at[layer, pl.ds(pl.multiple_of(block * p_rows + half * n, n), n), :]
        if unit in GATE_PART:
            n = g_rows // gate_cuts(layer)
            at = block * g_rows + half * (g_rows // 2) + GATE_PART[unit] * n
            return wg.at[layer, pl.ds(pl.multiple_of(at, n), n), :]
        n = b_rows // 2
        row = unit - 3 if row is None else row
        return wb.at[layer, block // 2, pl.ds(pl.multiple_of(row * b_rows + half * n, n), n), :]

    unit_rows = g_rows // 4

    def units(sem, count):
        ref = wg.at[pl.ds(0, 2 if count > 16 else 1), pl.ds(0, int(unit_rows * (count if count <= 16 else count // 2))), :]
        return pltpu.make_async_remote_copy(
            src_ref=ref, dst_ref=ref, send_sem=sem, recv_sem=sem,
            device_id={"grp": other}, device_id_type=MESH,
        )

    def w_copy(layer, flow, block, half, unit, target, recv):
        ref = view(layer, block, half, unit)
        return pltpu.make_async_remote_copy(
            src_ref=ref, dst_ref=ref, send_sem=w_send.at[flow], recv_sem=recv,
            device_id=target, device_id_type=MESH,
        )

    def kind(piece):
        return {POOL: 0, BACK: 2}.get(piece, 1)

    def z_sem(layer, k, unit):
        return z_recv.at[layer, k, unit] if unit < 5 else z_fine.at[k, unit - 5]

    def own_sem(layer, k, piece):
        return z_recv.at[layer, k, 3 + c] if piece == BACK else z_sem(layer, k, UNITS[piece][0])

    def amount(layer, piece):
        return 1 if piece in (POOL, BACK) else 4 / gate_cuts(layer)

    def own_copy(layer, flow, half, piece, plane, recv):
        if piece != BACK:
            return w_copy(layer, flow, s, half, UNITS[piece][0], {"sp": plane}, recv)
        n = b_rows // 2
        return pltpu.make_async_remote_copy(
            src_ref=wb_own.at[layer, pl.ds(pl.multiple_of(half * n, n), n), :],
            dst_ref=view(layer, s, half, 3, row=c),
            send_sem=w_send.at[flow], recv_sem=recv,
            device_id={"sp": plane, "tp": base + s_parity}, device_id_type=MESH,
        )

    def holds(block, piece, fn):
        if piece == BACK:
            pl.when(c == block % 2)(fn)
        else:
            fn()

    def pump(mid, layer, k, piece):
        block = blocks[k]

        def act():
            for unit in UNITS[piece]:
                units(z_sem(layer, k, unit), amount(layer, piece)).wait_recv()
                if k == 0 and mid:
                    w_copy(layer, 2, block, g, unit, {"sp": mid_far}, z_sem(layer, 2, unit)).start()
                    continue
                w_copy(
                    layer, 2 + k, block, g, unit, {"grp": other}, y_recv.at[layer, kind(piece)]
                ).start()
                if mid and layer > 0:
                    w_copy(
                        layer, 4 + k, block, g, unit, {"sp": end_here}, z_sem(layer, k, unit)
                    ).start()
        holds(block, piece, act)

    def own(mid, waited, layer, flow, piece):
        if (layer, kind(piece)) not in waited:
            waited.add((layer, kind(piece)))
            load(layer, kind(piece)).wait()
            if piece == BACK and (mid or layer > 0):
                @pl.when(c != s_parity)
                def _():
                    bx_copy(layer).start()
        if mid and flow == 0:
            own_copy(layer, 0, g, piece, mid_far, own_sem(layer, 1, piece)).start()
        elif mid:
            own_copy(layer, 1, g, piece, end_here, own_sem(layer, 0, piece)).start()
        elif flow == 0:
            own_copy(layer, 0, g, piece, mid_here, own_sem(layer, 0, piece)).start()
        else:
            own_copy(layer, 1, other, piece, mid_here, y_recv.at[layer, kind(piece)]).start()

    def bx_copy(layer):
        return pltpu.make_async_remote_copy(
            src_ref=wb_own.at[layer],
            dst_ref=wb.at[layer, s // 2, pl.ds(pl.multiple_of(c * b_rows, b_rows), b_rows), :],
            send_sem=bx_send.at[0], recv_sem=bx_recv.at[layer],
            device_id={"tp": t1}, device_id_type=MESH,
        )

    def wb_load(layer):
        return pltpu.make_async_copy(
            wb_hbm.at[layer],
            wb.at[layer, s // 2, pl.ds(pl.multiple_of(c * b_rows, b_rows), b_rows), :],
            load_sem.at[layer, 3],
        )

    def load(layer, piece):
        if piece == 0:
            src, dst = wp_hbm.at[layer], wp.at[layer, pl.ds(pl.multiple_of(s * p_rows, p_rows), p_rows), :]
        elif piece == 1:
            src, dst = wg_hbm.at[layer], wg.at[layer, pl.ds(pl.multiple_of(s * g_rows, g_rows), g_rows), :]
        else:
            src, dst = wb_hbm.at[layer], wb_own.at[layer]
        return pltpu.make_async_copy(src, dst, load_sem.at[layer, piece])

    def ready(layer, which):
        if which < 2:
            units(y_recv.at[layer, which], 3 * (1 + which)).wait_recv()
            return

        @pl.when(c == s_parity)
        def _():
            units(y_recv.at[layer, 2], 2).wait_recv()
            wb_load(layer).wait()
            units(bx_recv.at[layer], 2).wait_recv()

        @pl.when(c != s_parity)
        def _():
            units(y_recv.at[layer, 2], 4).wait_recv()

    def tok_load(k):
        return pltpu.make_async_copy(
            tok_hbm.at[:, pl.ds(k * cols_k, cols_k)], gathered.at[0, t, k], load_sem.at[LAYERS, k]
        )

    gain_load = pltpu.make_async_copy(gain_hbm, gain_ref, load_sem.at[LAYERS, CHUNKS])

    def out_copy(k):
        return pltpu.make_async_copy(
            final.at[k], out_hbm.at[:, pl.ds(k * cols_k, cols_k)], load_sem.at[0, k]
        )

    def guest_copy(k):
        return pltpu.make_async_remote_copy(
            src_ref=gathered.at[0, t, k], dst_ref=gathered.at[GUEST, t, k],
            send_sem=tk_send.at[0], recv_sem=tk_recv.at[k],
            device_id={"sp": mid_here}, device_id_type=MESH,
        )

    def return_copy(k):
        return pltpu.make_async_remote_copy(
            src_ref=returned.at[k], dst_ref=gathered.at[1, t, k],
            send_sem=rt_send.at[0], recv_sem=rt_recv.at[k],
            device_id={"sp": end_here}, device_id_type=MESH,
        )

    def ag_copy(slot, k, block, target, recv):
        return pltpu.make_async_remote_copy(
            src_ref=gathered.at[slot, block, k], dst_ref=gathered.at[slot, block, k],
            send_sem=ag_send.at[0], recv_sem=ag_recv.at[slot, recv],
            device_id={"tp": target}, device_id_type=MESH,
        )

    def start_gather(slot, k):
        ag_copy(slot, k, t, t2, k).start()
        ag_copy(slot, k, t, t1, 3).start()

    def pass_on(slot, k):
        units(ag_recv.at[slot, k], 1).wait_recv()
        ag_copy(slot, k, t2, t1, 2).start()

    spans = [w // 2 for w in pool_windows]

    def h_copy(layer, way, span):
        rows = (span if way == 0 else max(span - 1, 1)) * GRID_W
        at = toks - rows if way == 0 else 0
        return pltpu.make_async_remote_copy(
            src_ref=halo.at[layer, 1, pl.ds(at, rows), :],
            dst_ref=halo.at[layer, 0 if way == 0 else 2, pl.ds(at, rows), :],
            send_sem=h_send.at[layer, way], recv_sem=h_recv.at[layer, way],
            device_id={"sp": s + 1 if way == 0 else s - 1}, device_id_type=MESH,
        )

    def halo_do(layer, way, cond, op):
        for group_id, span in enumerate(spans):
            @pl.when(jnp.logical_and(cond, t == group_id))
            def _(span=span):
                op(h_copy(layer, way, span))

    def halo_start(layer):
        up_ok = jnp.logical_and(s < last, jnp.logical_or(layer > 0, s == 1))
        down_ok = jnp.logical_and(s > 0, jnp.logical_or(layer > 0, s == 2))
        halo_do(layer, 0, up_ok, lambda x: x.start())
        halo_do(layer, 1, down_ok, lambda x: x.start())

    def halo_wait(layer):
        from_up = jnp.logical_and(s > 0, jnp.logical_or(layer > 0, s == 2))
        from_down = jnp.logical_and(s < last, jnp.logical_or(layer > 0, s == 1))
        halo_do(layer, 0, from_up, lambda x: x.wait_recv())
        halo_do(layer, 1, from_down, lambda x: x.wait_recv())

    def px_copy(slot, row):
        return pltpu.make_async_remote_copy(
            src_ref=pair.at[slot, row], dst_ref=pair.at[slot, row],
            send_sem=px_send.at[0], recv_sem=px_recv.at[slot],
            device_id={"tp": t1}, device_id_type=MESH,
        )

    def rs_copy(slot, k):
        return pltpu.make_async_remote_copy(
            src_ref=parts.at[slot, k], dst_ref=arrived.at[slot, k],
            send_sem=rs_send.at[0], recv_sem=rs_recv.at[slot, k],
            device_id={"tp": t2}, device_id_type=MESH,
        )

    def absorb(layer, slot, which, block, total):
        for k in range(CHUNKS):
            at = pl.ds(pl.multiple_of(block * feats + k * cols_k, cols_k), cols_k)
            wide = gathered[slot, block, k].astype(f32)
            scaled[which, :, at] = (wide * gain_ref[pl.ds(layer, 1), at]).astype(bf)
            total = total + jnp.sum(wide * wide, axis=1, keepdims=True)
        return total

    def scale_of(total):
        return lax.rsqrt(total / (tp_count * feats) + norm_eps)

    def half_dot(layer, which, first, weights):
        at = pl.ds(pl.multiple_of(first * feats, feats), 2 * feats)
        return jnp.dot(scaled[which, :, at], weights[layer, at, :], preferred_element_type=f32)

    def gate_of(layer, which, scale):
        acc = jnp.dot(scaled[which], wg[layer], preferred_element_type=f32)
        value = jax.nn.sigmoid(acc * scale)
        for k in range(CHUNKS):
            gate_buf[which, k] = value[:, k * cols_k:(k + 1) * cols_k]

    def share_pooled(slot, which, sums, cells):
        pooled = (sums / counts[which] - cells.astype(f32)).astype(bf)
        pair[slot, c] = pooled
        px_copy(slot, c).start()

    def back_part(layer, slot, cols, k):
        at = pl.ds(k * cols_k, cols_k)
        acc = jnp.dot(pair[slot, 0], wb[layer, cols, 0:b_rows, at], preferred_element_type=f32)
        return acc + jnp.dot(
            pair[slot, 1], wb[layer, cols, b_rows:2 * b_rows, at], preferred_element_type=f32
        )

    def back(layer, slot, which):
        units(px_recv.at[slot], 1).wait_recv()
        for k in range(CHUNKS):
            parts[slot, k] = back_part(layer, slot, far_base // 2, k).astype(bf)
            rs_copy(slot, k).start()
        for k in range(CHUNKS):
            own_part[which, k] = back_part(layer, slot, base // 2, k)

    def update(slot, which, k):
        units(rs_recv.at[slot, k], 1).wait_recv()
        branch = own_part[which, k] + arrived[slot, k].astype(f32)
        return (gathered[slot, t, k].astype(f32) + gate_buf[which, k] * branch).astype(bf)

    for k in range(CHUNKS):
        tok_load(k).start()
    gain_load.start()
    for layer in range(LAYERS):
        for piece in (0, 2, 1):
            load(layer, piece).start()

        @pl.when(jnp.logical_and(c == s_parity, jnp.logical_or(is_mid, layer > 0)))
        def _(layer=layer):
            wb_load(layer).start()
    for layer in range(LAYERS):
        for slot in (0, 2):
            halo[layer, slot] = jnp.zeros(halo.shape[2:], halo.dtype)

    barrier = pltpu.get_barrier_semaphore()
    for target in ({"grp": other}, {"tp": t1}, {"tp": t2}):
        pl.semaphore_signal(barrier, inc=1, device_id=target, device_id_type=MESH)

    @pl.when(s > 0)
    def _():
        for peer in (t, t1):
            pl.semaphore_signal(barrier, inc=1, device_id={"sp": s - 1, "tp": peer}, device_id_type=MESH)

    @pl.when(s < last)
    def _():
        for peer in (t, t1):
            pl.semaphore_signal(barrier, inc=1, device_id={"sp": s + 1, "tp": peer}, device_id_type=MESH)

    pl.semaphore_wait(barrier, 3 + jnp.where(s > 0, 2, 0) + jnp.where(s < last, 2, 0))

    def setup():
        half_span = jnp.int32(spans[0])
        for group_id in range(1, GROUPS):
            half_span = jnp.where(t == group_id, spans[group_id], half_span)
        shift = GRID_W.bit_length() - 1
        out_tok = lax.broadcasted_iota(jnp.int32, (toks, toks), 0)
        in_tok = lax.broadcasted_iota(jnp.int32, (toks, toks), 1)
        out_row = lax.shift_right_logical(out_tok, shift)
        out_col = lax.bitwise_and(out_tok, GRID_W - 1)
        in_col = lax.bitwise_and(in_tok, GRID_W - 1)
        near_col = (in_col >= out_col - half_span) & (in_col < out_col + half_span)
        for slot in range(3):
            in_row = (slot - 1) * rows_here + lax.shift_right_logical(in_tok, shift)
            inside = near_col & (in_row >= out_row - half_span) & (in_row < out_row + half_span)
            box[slot] = jnp.where(inside, 1.0, 0.0).astype(bf)
        tok_at = lax.broadcasted_iota(jnp.int32, counts.shape[1:], 0)
        col_at = lax.bitwise_and(tok_at, GRID_W - 1)
        col_counts = jnp.minimum(col_at + half_span, GRID_W) - jnp.maximum(col_at - half_span, 0)
        for which, plane in ((0, s), (1, end_here)):
            row_at = plane * rows_here + lax.shift_right_logical(tok_at, shift)
            row_counts = jnp.minimum(row_at + half_span, total_rows) - jnp.maximum(row_at - half_span, 0)
            counts[which] = (row_counts * col_counts).astype(f32)

    def box_dot(slot, value):
        return jnp.dot(box[slot], value, preferred_element_type=f32)

    for k in range(CHUNKS):
        tok_load(k).wait()
    gain_load.wait()
    waited_mid, waited_end = set(), set()
    zero = jnp.zeros((toks, 1), f32)

    def relay(mid, item):
        if item[0] == "own":
            own(mid, waited_mid if mid else waited_end, *item[1:])
        else:
            pump(mid, *item[1:])

    def gather_step(layer, slot, which, k, total):
        if k == 0:
            total = absorb(layer, slot, which, t, zero)
            units(ag_recv.at[slot, 3], 2).wait_recv()
            total = absorb(layer, slot, which, t1, total)
        pass_on(slot, k)
        if k == CHUNKS - 1:
            total = absorb(layer, slot, which, t2, total)
        return total

    def pool_step(layer, slot, which, total):
        ready(layer, 0)
        acc = half_dot(layer, which, base, wp)
        units(ag_recv.at[slot, 2], 2).wait_recv()
        total = absorb(layer, slot, which, t3, total)
        scale = scale_of(total)
        acc = acc + half_dot(layer, which, far_base, wp)
        return (acc * scale).astype(bf), scale

    @pl.when(is_end)
    def _():
        for item in END_FIRST:
            if item[0] == "tok":
                guest_copy(item[1]).start()
            elif item[0] == "ret":
                if item[1] == 0:
                    setup()
                return_copy(item[1]).wait_recv()
                start_gather(1, item[1])
            else:
                relay(False, item)

    @pl.when(is_mid)
    def _():
        guest_side = jnp.where(low, 0, 2)
        total, scale = {}, {}
        for item in MID_FIRST:
            name = item[0]
            slot = item[1]
            which = 1 if slot == GUEST else 0
            if name == "gstart":
                for k in range(CHUNKS):
                    start_gather(0, k)
            elif name == "guest":
                guest_copy(slot).wait_recv()
                start_gather(GUEST, slot)
            elif name == "agf":
                if item == ("agf", 0, 0):
                    setup()
                total[slot] = gather_step(0, slot, which, item[2], total.get(slot))
            elif name == "pool" and slot == 0:
                halo[0, 1], scale[0] = pool_step(0, 0, 0, total[0])
                halo_start(0)
            elif name == "pool":
                units(ag_recv.at[GUEST, 2], 2).wait_recv()
                total[slot] = absorb(0, GUEST, 1, t3, total[slot])
                scale[slot] = scale_of(total[slot])
                acc = half_dot(0, 1, base, wp) + half_dot(0, 1, far_base, wp)
                halo[0, guest_side] = (acc * scale[slot]).astype(bf)
                cells = halo[0, guest_side]
                sums = box_dot(1, cells) + box_dot(2 - guest_side, halo[0, 1])
                share_pooled(GUEST, 1, sums, cells)
            elif name == "box":
                halo_wait(0)
                cells = halo[0, 1]
                sums = box_dot(0, halo[0, 0]) + box_dot(1, cells) + box_dot(2, halo[0, 2])
                share_pooled(0, 0, sums, cells)
            elif name == "back":
                if slot == FIRST_BACK:
                    ready(0, 2)
                back(0, slot, which)
            elif name == "gate":
                if slot == FIRST_GATE:
                    ready(0, 1)
                gate_of(0, which, scale[slot])
            elif name == "upd":
                k = item[2]
                value = update(slot, which, k)
                if slot == GUEST:
                    returned[k] = value
                    return_copy(k).start()
                else:
                    gathered[1, t, k] = value
                    start_gather(1, k)
            else:
                relay(True, item)

    steps = iter(zip(MID_REST, END_REST))

    def relays():
        for mid, items in zip((True, False), next(steps)):
            if items:
                @pl.when(is_mid if mid else is_end)
                def _(mid=mid, items=items):
                    for item in items:
                        relay(mid, item)

    for layer in range(1, LAYERS):
        total = None
        for k in range(CHUNKS):
            total = gather_step(layer, layer, 0, k, total)
            relays()
        cells, scale = pool_step(layer, layer, 0, total)
        halo[layer, 1] = cells
        halo_start(layer)
        relays()
        cells = halo[layer, 1]
        sums = box_dot(1, cells)
        halo_wait(layer)
        sums = sums + box_dot(0, halo[layer, 0]) + box_dot(2, halo[layer, 2])
        share_pooled(layer, 0, sums, cells)
        relays()
        ready(layer, 2)
        back(layer, layer, 0)
        relays()
        ready(layer, 1)
        gate_of(layer, 0, scale)
        relays()
        for k in range(CHUNKS):
            state = update(layer, 0, k)
            if layer + 1 < LAYERS:
                gathered[layer + 1, t, k] = state
                start_gather(layer + 1, k)
            else:
                out_hbm[:, k * cols_k:(k + 1) * cols_k] = state
            relays()

    def sent(sem, count):
        units(sem, count).wait_send()

    def sent_blocks(flow, k, layers):
        @pl.when(c == blocks[k] % 2)
        def _():
            sent(w_send.at[flow], 5 * layers)

        @pl.when(c != blocks[k] % 2)
        def _():
            sent(w_send.at[flow], 3 * layers)

    def sent_chain(layers, slots):
        @pl.when(c != s_parity)
        def _():
            sent(bx_send.at[0], 2 * layers)
        sent(ag_send.at[0], 6 * slots)
        sent(rs_send.at[0], 2 * slots)
        sent(px_send.at[0], slots)

    @pl.when(is_mid)
    def _():
        sent(w_send.at[0], 4 * LAYERS)
        sent(w_send.at[1], 4 * (LAYERS - 1))
        for k in range(3):
            sent_blocks(2 + k, k, LAYERS)
        for k in (1, 2):
            sent_blocks(4 + k, k, LAYERS - 1)
        sent(rt_send.at[0], CHUNKS)
        sent_chain(LAYERS, LAYERS + 1)

    @pl.when(is_end)
    def _():
        sent(w_send.at[0], 4 * LAYERS)
        sent(w_send.at[1], 4 * LAYERS)
        for k in range(3):
            sent_blocks(2 + k, k, LAYERS - 1)
        sent(tk_send.at[0], CHUNKS)
        sent_chain(LAYERS - 1, LAYERS - 1)
    for layer in range(LAYERS):
        outward = layer > 0
        halo_do(layer, 0, (s < last) if outward else (s == 1), lambda x: x.wait_send())
        halo_do(layer, 1, (s > 0) if outward else (s == 2), lambda x: x.wait_send())


def fused(tokens_in, norm_gain, w_pool_in, w_gate, w_back):
    sp_count, tp_count = lax.axis_size("sp"), lax.axis_size("tp")
    toks, feats = tokens_in.shape
    _, depth, local_pool = w_pool_in.shape
    b_rows, b_cols = w_back.shape[1:]
    cols_k = feats // CHUNKS
    bf, f32 = jnp.bfloat16, jnp.float32
    dma = pltpu.SemaphoreType.DMA
    slots = LAYERS + 1
    hbm = pl.BlockSpec(memory_space=pltpu.HBM)
    return pl.pallas_call(
        functools.partial(fused_kernel, sp_count, tp_count),
        out_shape=pltpu.VMEM((toks, feats), bf),
        in_specs=[hbm] * 5,
        out_specs=pl.BlockSpec(memory_space=pltpu.VMEM),
        scratch_shapes=[
            pltpu.VMEM((LAYERS, sp_count * depth, local_pool), bf),
            pltpu.VMEM((LAYERS, sp_count * depth, w_gate.shape[2]), bf),
            pltpu.VMEM((LAYERS, 2, 2 * b_rows, b_cols), bf),
            pltpu.VMEM((LAYERS, b_rows, b_cols), bf),
            pltpu.VMEM((slots, tp_count, CHUNKS, toks, cols_k), bf),
            pltpu.VMEM((2, toks, tp_count * feats), bf),
            pltpu.VMEM((LAYERS, 3, toks, local_pool), bf),
            pltpu.VMEM((2, CHUNKS, toks, cols_k), f32),
            pltpu.VMEM((2, CHUNKS, toks, cols_k), f32),
            pltpu.VMEM((3, toks, toks), bf),
            pltpu.VMEM((2, toks, local_pool), f32),
            pltpu.VMEM((slots, 2, toks, local_pool), bf),
            pltpu.VMEM((slots, CHUNKS, toks, cols_k), bf),
            pltpu.VMEM((slots, CHUNKS, toks, cols_k), bf),
            pltpu.VMEM((CHUNKS, toks, cols_k), bf),
            pltpu.VMEM(norm_gain.shape, f32),
            pltpu.VMEM((CHUNKS, toks, cols_k), bf),
            dma((LAYERS + 1, 4)),
            dma((7,)), dma((LAYERS, 3, 5)), dma((3, 2)), dma((LAYERS, 3)),
            dma((1,)), dma((LAYERS,)),
            dma((1,)), dma((CHUNKS,)), dma((1,)), dma((CHUNKS,)),
            dma((1,)), dma((slots, 4)),
            dma((LAYERS, 2)), dma((LAYERS, 2)),
            dma((1,)), dma((slots,)),
            dma((1,)), dma((slots, CHUNKS)),
        ],
        compiler_params=pltpu.CompilerParams(
            collective_id=0, has_side_effects=True, vmem_limit_bytes=56 * 1024 * 1024
        ),
    )(tokens_in, norm_gain, w_pool_in, w_gate, w_back)

def dispatch(tokens_in, norm_gain, w_pool_in, w_gate, w_back):
    fits = (
        lax.axis_size("grp") == 2
        and lax.axis_size("tp") == GROUPS == 4
        and lax.axis_size("sp") == lax.axis_size("tp")
        and w_pool_in.shape[2] * GROUPS == POOL_WIDTH
        and w_pool_in.shape[1] == tokens_in.shape[1] == w_gate.shape[2] == w_back.shape[2]
        and tokens_in.shape[1] == 2 * tokens_in.shape[0] == 2 * w_pool_in.shape[2]
        and tokens_in.shape[0] // GRID_W >= max(pool_windows) // 2
    )
    step = fused if fits else on_device
    return step(tokens_in, norm_gain, w_pool_in, w_gate, w_back)


def solution(mesh):
    return jax.shard_map(
        dispatch,
        mesh=mesh,
        in_specs=(
            P(("grp", "sp"), "tp"),
            P(),
            P(None, "sp", "tp"),
            P(None, "sp", "tp"),
            P(None, "tp", "sp"),
        ),
        out_specs=P(("grp", "sp"), "tp"),
        check_vma=False,
    )
```

```python
import jax
import jax.numpy as jnp
from jax import lax
from jax.experimental import pallas as pl
from jax.experimental.pallas import tpu as pltpu
from jax.sharding import PartitionSpec as P
import functools

POOL_WIDTH = 1024
GROUPS = 4
GRID_W = 32
LAYERS = 3


pool_windows = (2, 4, 8, 16)
norm_eps = 1e-06


def padded_2(value, sides, width):
    for axis, dim in sides:
        peers, length = (lax.axis_size(axis), value.shape[dim])
        up = [(i, (i + 1) % peers) for i in range(peers - 1)]
        down = [(j, i) for i, j in up]
        last = lax.slice_in_dim(value, length - width, length, axis=dim)
        initial = lax.slice_in_dim(value, 0, width, axis=dim)
        before = lax.ppermute(last, axis, up)
        after = lax.ppermute(initial, axis, down)
        value = jnp.concatenate([before, value, after], axis=dim)
    return value


def window_means(padded, rows_here, first_row, total_rows, window):
    reach = max(pool_windows) // 2
    half_span = window // 2
    width_cols = padded.shape[1] - 2 * reach
    row_sums = padded[reach - half_span : reach - half_span + rows_here]
    for offset in range(1 - half_span, half_span):
        row_sums = row_sums + padded[reach + offset : reach + offset + rows_here]
    box_sums = row_sums[:, reach - half_span : reach - half_span + width_cols]
    for offset in range(1 - half_span, half_span):
        box_sums = box_sums + row_sums[:, reach + offset : reach + offset + width_cols]
    row_index = first_row + jnp.arange(rows_here, dtype=jnp.int32)
    col_index = jnp.arange(width_cols, dtype=jnp.int32)
    row_counts = jnp.minimum(row_index + half_span, total_rows) - jnp.maximum(
        row_index - half_span, 0
    )
    col_counts = jnp.minimum(col_index + half_span, width_cols) - jnp.maximum(
        col_index - half_span, 0
    )
    counts = (row_counts[:, None] * col_counts[None, :]).astype(jnp.float32)
    return box_sums / counts[:, :, None]


def on_device(tokens_in, norm_gain, w_pool_in, w_gate, w_back):
    reach = max(pool_windows) // 2
    sp_count = lax.axis_size("sp")
    tp_count = lax.axis_size("tp")
    tp_pos = lax.axis_index("tp")
    sp_pos = lax.axis_index("sp")
    tok_rows = tokens_in.shape[0]
    rows_here = tok_rows // GRID_W
    total_rows = rows_here * sp_count
    first_row = sp_pos * rows_here
    local_pool = w_pool_in.shape[2]
    group_width = POOL_WIDTH // GROUPS
    channel_group = (tp_pos * local_pool + jnp.arange(local_pool, dtype=jnp.int32)) // group_width
    state = tokens_in
    for layer_id in range(LAYERS):
        whole_rows = lax.all_gather(state, "tp", axis=1, tiled=True)
        wide = whole_rows.astype(jnp.float32)
        normed = (
            wide
            * lax.rsqrt(jnp.mean(wide * wide, axis=-1, keepdims=True) + norm_eps)
            * norm_gain[layer_id]
        ).astype(jnp.bfloat16)
        pool_acc = jnp.dot(
            normed,
            lax.all_gather(w_pool_in[layer_id], "sp", axis=0, tiled=True),
            preferred_element_type=jnp.float32,
        )
        gate_acc = jnp.dot(
            normed,
            lax.all_gather(w_gate[layer_id], "sp", axis=0, tiled=True),
            preferred_element_type=jnp.float32,
        )
        pool_in = pool_acc.astype(jnp.bfloat16)
        gate = jax.nn.sigmoid(gate_acc)
        cells = pool_in.reshape(rows_here, GRID_W, local_pool)
        rimmed = padded_2(cells, (("sp", 0),), reach)
        padded = jnp.pad(rimmed.astype(jnp.float32), ((0, 0), (reach, reach), (0, 0)))
        means = jnp.zeros((rows_here, GRID_W, local_pool), jnp.float32)
        for group_id in range(GROUPS):
            in_group = (channel_group == group_id)[None, None, :]
            means = jnp.where(
                in_group,
                window_means(padded, rows_here, first_row, total_rows, pool_windows[group_id]),
                means,
            )
        pooled = (
            (means - cells.astype(jnp.float32)).reshape(tok_rows, local_pool).astype(jnp.bfloat16)
        )
        full_pooled = lax.all_gather(pooled, "tp", axis=1, tiled=True)
        back_rows = lax.all_gather(w_back[layer_id], "sp", axis=1, tiled=True)
        back_cols = lax.all_to_all(back_rows, "tp", split_axis=1, concat_axis=0, tiled=True)
        partials = jnp.einsum(
            "tnb,nbd->ntd",
            full_pooled.reshape(tok_rows, tp_count, local_pool),
            back_cols.reshape(tp_count, local_pool, back_cols.shape[1]),
            preferred_element_type=jnp.float32,
        ).astype(jnp.bfloat16)
        branch = jnp.sum(partials.astype(jnp.float32), axis=0)
        state = (state.astype(jnp.float32) + gate * branch).astype(jnp.bfloat16)
    return state


MESH = pl.DeviceIdType.MESH
POOL, GATE_A, GATE_B, BACK = range(4)
UNITS = {POOL: (0,), GATE_A: (1,), GATE_B: (2,), BACK: (3, 4), 4: (5,), 5: (6,)}
GATE_PART = {1: 0, 2: 1, 5: 2, 6: 3}
CHUNKS = 2
GUEST, AGAIN = LAYERS, LAYERS + 1


MID_FIRST = (
    ("own", 2, 1, 4), ("own", 2, 1, 2), ("own", 0, 0, 2), ("own", 0, 0, 0), ("own", 2, 1, 5),
    ("own", 1, 1, 0), ("pump", 0, 0, 0), ("own", 0, 0, 3), ("own", 2, 1, 0), ("pump", 0, 1, 2),
    ("pump", 0, 0, 3), ("own", 1, 0, 0), ("pump", 0, 1, 0), ("own", 1, 1, 3), ("gstart", 0),
    ("pump", 0, 2, 0), ("pump", 0, 1, 3), ("guest", 0), ("guest", 1), ("agf", 0, 0), ("own", 1, 0, 3),
    ("agf", 0, 1), ("pump", 0, 2, 3), ("pool", 0), ("pump", 0, 0, 2), ("own", 0, 0, 1), ("agf", 3, 0),
    ("pump", 1, 1, 0), ("pump", 0, 0, 1), ("own", 2, 0, 1), ("pump", 1, 1, 3), ("agf", 3, 1),
    ("own", 2, 1, 1), ("pool", 3), ("pump", 1, 0, 0), ("own", 1, 0, 1), ("own", 2, 1, 3), ("pump", 0, 2, 2),
    ("back", 3), ("pump", 0, 1, 1), ("box", 0), ("pump", 0, 2, 1), ("back", 0), ("pump", 2, 1, 1),
    ("pump", 1, 2, 0), ("own", 1, 0, 2), ("pump", 1, 0, 3), ("gate", 3), ("gate", 0), ("upd", 0, 0),
    ("upd", 0, 1), ("pump", 1, 1, 1), ("pump", 1, 0, 2), ("upd", 3, 0), ("upd", 3, 1), ("pump", 1, 1, 2),
    ("own", 2, 0, 2), ("pump", 1, 0, 1),
)
END_FIRST = (
    ("own", 0, 0, 0), ("own", 0, 0, 3), ("tok", 0), ("tok", 1), ("own", 0, 1, 0), ("own", 0, 0, 2),
    ("own", 0, 0, 1), ("own", 1, 0, 0), ("own", 0, 1, 3), ("own", 0, 1, 1), ("own", 1, 0, 3),
    ("own", 0, 1, 2), ("pump", 1, 1, 0), ("own", 1, 0, 2), ("own", 1, 0, 1), ("pump", 2, 0, 5),
    ("pump", 2, 0, 4), ("pump", 2, 0, 0), ("pump", 2, 0, 2), ("pump", 1, 0, 0), ("pump", 1, 2, 0),
    ("own", 2, 0, 3), ("own", 1, 1, 0), ("own", 1, 1, 2), ("ret", 0), ("own", 1, 1, 1), ("pump", 1, 1, 3),
    ("ret", 1),
)
MID_REST = (
    (
        ("pump", 1, 2, 3), ("pump", 1, 2, 2),
    ),
    (
        ("pump", 2, 1, 2), ("pump", 2, 0, 3), ("pump", 1, 2, 1),
    ),
    (
        ("agf", 4, 0), ("agf", 4, 1), ("own", 2, 0, 0), ("pump", 2, 2, 3), ("gate", 4), ("pump", 2, 0, 0),
    ),
    (),
    (
        ("own", 2, 0, 3), ("pump", 2, 2, 0), ("pump", 2, 1, 0), ("own", 2, 0, 5),
    ),
    (),
    (
        ("pump", 2, 1, 5),
    ),
    (
        ("pump", 2, 0, 2), ("pump", 2, 0, 5), ("pump", 2, 1, 3), ("pump", 2, 2, 5), ("pump", 2, 0, 1),
        ("pump", 2, 0, 4), ("pump", 2, 2, 2), ("own", 2, 0, 4),
    ),
    (),
    (),
    (
        ("pump", 2, 1, 4), ("pump", 2, 2, 4), ("pump", 2, 2, 1),
    ),
    (),
    (),
    (),
    (),
    (),
)
END_REST = (
    (
        ("pump", 1, 0, 3), ("pump", 2, 0, 3), ("own", 2, 0, 0),
    ),
    (),
    (
        ("own", 1, 1, 3), ("own", 2, 0, 1), ("pump", 1, 2, 3), ("own", 2, 0, 5),
    ),
    (
        ("own", 2, 0, 4),
    ),
    (
        ("own", 2, 0, 2), ("pump", 2, 1, 1), ("pump", 2, 1, 2), ("pump", 2, 2, 3), ("pump", 2, 0, 1),
        ("own", 2, 1, 4),
    ),
    (),
    (),
    (
        ("own", 2, 1, 3), ("pump", 2, 2, 0), ("own", 2, 1, 0), ("pump", 2, 1, 0),
    ),
    (),
    (
        ("own", 2, 1, 1), ("pump", 2, 1, 3), ("pump", 2, 1, 5),
    ),
    (
        ("own", 2, 1, 2), ("pump", 2, 2, 5), ("pump", 2, 2, 2),
    ),
    (),
    (
        ("pump", 2, 1, 4), ("pump", 2, 2, 4), ("own", 2, 1, 5), ("pump", 2, 2, 1),
    ),
    (),
    (),
    (),
)
AGAIN_FIRST = True
FIRST_BACK, FIRST_GATE = 3, 3


def fused_kernel(
    sp_count, tp_count,
    tok_hbm, gain_hbm, wp_hbm, wg_hbm, wb_hbm, out_ref,
    wp, wg, wb, wb_own, gathered, scaled, halo, gate_buf, own_part, box, counts,
    pair, parts, arrived, gate_sent, gain_ref,
    load_sem, w_send, z_recv, z_fine, y_recv, bx_send, bx_recv, tk_send, tk_recv, rt_send, rt_recv,
    ag_send, ag_recv, h_send, h_recv, px_send, px_recv, rs_send, rs_recv, gv_send, gv_recv,
):
    g = lax.axis_index("grp")
    s = lax.axis_index("sp")
    t = lax.axis_index("tp")
    other = 1 - g
    c = t % 2
    base = t - c
    t1 = base + 1 - c
    t2 = (t + 2) % tp_count
    t3 = (t1 + 2) % tp_count
    far_base = (base + 2) % tp_count
    last = sp_count - 1
    toks, feats = tok_hbm.shape
    local_pool = wp.shape[2]
    cols_k = feats // CHUNKS
    rows_here = toks // GRID_W
    total_rows = rows_here * sp_count
    bf, f32 = jnp.bfloat16, jnp.float32

    low = s < 2
    is_mid = jnp.logical_and(s > 0, s < last)
    is_end = jnp.logical_not(is_mid)
    end_here = jnp.where(low, 0, last)
    mid_here = jnp.where(low, 1, last - 1)
    end_far = last - end_here
    mid_far = last - mid_here
    blocks = (
        jnp.where(is_mid, end_here, mid_here),
        jnp.where(is_mid, mid_far, mid_far),
        end_far,
    )
    s_parity = s % 2

    p_rows, g_rows = wp_hbm.shape[1], wg_hbm.shape[1]
    b_rows = wb_hbm.shape[1]

    def gate_cuts(layer):
        return 8 if layer == LAYERS - 1 else 4

    def view(layer, block, half, unit, row=None):
        if unit == 0:
            n = p_rows // 2
            return wp.at[layer, pl.ds(pl.multiple_of(block * p_rows + half * n, n), n), :]
        if unit in GATE_PART:
            n = g_rows // gate_cuts(layer)
            at = block * g_rows + half * (g_rows // 2) + GATE_PART[unit] * n
            return wg.at[layer, pl.ds(pl.multiple_of(at, n), n), :]
        n = b_rows // 2
        row = unit - 3 if row is None else row
        return wb.at[layer, block // 2, pl.ds(pl.multiple_of(row * b_rows + half * n, n), n), :]

    unit_rows = g_rows // 4

    def units(sem, count):
        ref = wg.at[pl.ds(0, 2 if count > 16 else 1), pl.ds(0, int(unit_rows * (count if count <= 16 else count // 2))), :]
        return pltpu.make_async_remote_copy(
            src_ref=ref, dst_ref=ref, send_sem=sem, recv_sem=sem,
            device_id={"grp": other}, device_id_type=MESH,
        )

    def w_copy(layer, flow, block, half, unit, target, recv):
        ref = view(layer, block, half, unit)
        return pltpu.make_async_remote_copy(
            src_ref=ref, dst_ref=ref, send_sem=w_send.at[flow], recv_sem=recv,
            device_id=target, device_id_type=MESH,
        )

    def kind(piece):
        return {POOL: 0, BACK: 2}.get(piece, 1)

    def z_sem(layer, k, unit):
        return z_recv.at[layer, k, unit] if unit < 5 else z_fine.at[k, unit - 5]

    def own_sem(layer, k, piece):
        return z_recv.at[layer, k, 3 + c] if piece == BACK else z_sem(layer, k, UNITS[piece][0])

    def amount(layer, piece):
        return 1 if piece in (POOL, BACK) else 4 / gate_cuts(layer)

    def own_copy(layer, flow, half, piece, plane, recv):
        if piece != BACK:
            return w_copy(layer, flow, s, half, UNITS[piece][0], {"sp": plane}, recv)
        n = b_rows // 2
        return pltpu.make_async_remote_copy(
            src_ref=wb_own.at[layer, pl.ds(pl.multiple_of(half * n, n), n), :],
            dst_ref=view(layer, s, half, 3, row=c),
            send_sem=w_send.at[flow], recv_sem=recv,
            device_id={"sp": plane, "tp": base + s_parity}, device_id_type=MESH,
        )

    def holds(block, piece, fn):
        if piece == BACK:
            pl.when(c == block % 2)(fn)
        else:
            fn()

    def pump(mid, layer, k, piece):
        block = blocks[k]

        def act():
            for unit in UNITS[piece]:
                units(z_sem(layer, k, unit), amount(layer, piece)).wait_recv()
                if k == 0 and mid:
                    w_copy(layer, 2, block, g, unit, {"sp": mid_far}, z_sem(layer, 2, unit)).start()
                    continue
                w_copy(
                    layer, 2 + k, block, g, unit, {"grp": other}, y_recv.at[layer, kind(piece)]
                ).start()
                if mid and layer > 0 and (layer, kind(piece)) != (1, 1):
                    w_copy(
                        layer, 4 + k, block, g, unit, {"sp": end_here}, z_sem(layer, k, unit)
                    ).start()
        holds(block, piece, act)

    def own(mid, waited, layer, flow, piece):
        if (layer, kind(piece)) not in waited:
            waited.add((layer, kind(piece)))
            load(layer, kind(piece)).wait()
            if piece == BACK and (mid or layer > 0):
                @pl.when(c != s_parity)
                def _():
                    bx_copy(layer).start()
        if mid and flow == 0:
            own_copy(layer, 0, g, piece, mid_far, own_sem(layer, 1, piece)).start()
        elif mid:
            own_copy(layer, 1, g, piece, end_here, own_sem(layer, 0, piece)).start()
        elif flow == 0:
            own_copy(layer, 0, g, piece, mid_here, own_sem(layer, 0, piece)).start()
        else:
            own_copy(layer, 1, other, piece, mid_here, y_recv.at[layer, kind(piece)]).start()

    def bx_copy(layer):
        return pltpu.make_async_remote_copy(
            src_ref=wb_own.at[layer],
            dst_ref=wb.at[layer, s // 2, pl.ds(pl.multiple_of(c * b_rows, b_rows), b_rows), :],
            send_sem=bx_send.at[0], recv_sem=bx_recv.at[layer],
            device_id={"tp": t1}, device_id_type=MESH,
        )

    def wb_load(layer):
        return pltpu.make_async_copy(
            wb_hbm.at[layer],
            wb.at[layer, s // 2, pl.ds(pl.multiple_of(c * b_rows, b_rows), b_rows), :],
            load_sem.at[layer, 3],
        )

    def load(layer, piece):
        if piece == 0:
            src, dst = wp_hbm.at[layer], wp.at[layer, pl.ds(pl.multiple_of(s * p_rows, p_rows), p_rows), :]
        elif piece == 1:
            src, dst = wg_hbm.at[layer], wg.at[layer, pl.ds(pl.multiple_of(s * g_rows, g_rows), g_rows), :]
        else:
            src, dst = wb_hbm.at[layer], wb_own.at[layer]
        return pltpu.make_async_copy(src, dst, load_sem.at[layer, piece])

    def ready(layer, which):
        if which < 2:
            units(y_recv.at[layer, which], 3 * (1 + which)).wait_recv()
            return

        @pl.when(c == s_parity)
        def _():
            units(y_recv.at[layer, 2], 2).wait_recv()
            wb_load(layer).wait()
            units(bx_recv.at[layer], 2).wait_recv()

        @pl.when(c != s_parity)
        def _():
            units(y_recv.at[layer, 2], 4).wait_recv()

    def tok_load(k):
        return pltpu.make_async_copy(
            tok_hbm.at[:, pl.ds(k * cols_k, cols_k)], gathered.at[0, t, k], load_sem.at[LAYERS, k]
        )

    gain_load = pltpu.make_async_copy(gain_hbm, gain_ref, load_sem.at[LAYERS, CHUNKS])

    def guest_copy(k):
        return pltpu.make_async_remote_copy(
            src_ref=gathered.at[0, t, k], dst_ref=gathered.at[GUEST, t, k],
            send_sem=tk_send.at[0], recv_sem=tk_recv.at[k],
            device_id={"sp": mid_here}, device_id_type=MESH,
        )

    def return_copy(k):
        return pltpu.make_async_remote_copy(
            src_ref=gathered.at[AGAIN, t, k], dst_ref=gathered.at[1, t, k],
            send_sem=rt_send.at[0], recv_sem=rt_recv.at[k],
            device_id={"sp": end_here}, device_id_type=MESH,
        )

    def ag_copy(slot, k, block, target, recv):
        return pltpu.make_async_remote_copy(
            src_ref=gathered.at[slot, block, k], dst_ref=gathered.at[slot, block, k],
            send_sem=ag_send.at[0], recv_sem=ag_recv.at[slot, recv],
            device_id={"tp": target}, device_id_type=MESH,
        )

    def start_gather(slot, k):
        ag_copy(slot, k, t, t2, k).start()
        ag_copy(slot, k, t, t1, 3).start()

    def pass_on(slot, k):
        units(ag_recv.at[slot, k], 1).wait_recv()
        ag_copy(slot, k, t2, t1, 2).start()

    spans = [w // 2 for w in pool_windows]

    def h_copy(layer, way, span):
        rows = (span if way == 0 else max(span - 1, 1)) * GRID_W
        at = toks - rows if way == 0 else 0
        return pltpu.make_async_remote_copy(
            src_ref=halo.at[layer, 1, pl.ds(at, rows), :],
            dst_ref=halo.at[layer, 0 if way == 0 else 2, pl.ds(at, rows), :],
            send_sem=h_send.at[layer, way], recv_sem=h_recv.at[layer, way],
            device_id={"sp": s + 1 if way == 0 else s - 1}, device_id_type=MESH,
        )

    def halo_do(layer, way, cond, op):
        for group_id, span in enumerate(spans):
            @pl.when(jnp.logical_and(cond, t == group_id))
            def _(span=span):
                op(h_copy(layer, way, span))

    def halo_start(layer):
        up_ok = jnp.logical_and(s < last, jnp.logical_or(layer > 0, s == 1))
        down_ok = jnp.logical_and(s > 0, jnp.logical_or(layer > 0, s == 2))
        halo_do(layer, 0, up_ok, lambda x: x.start())
        halo_do(layer, 1, down_ok, lambda x: x.start())

    def halo_wait(layer):
        from_up = jnp.logical_and(s > 0, jnp.logical_or(layer > 0, s == 2))
        from_down = jnp.logical_and(s < last, jnp.logical_or(layer > 0, s == 1))
        halo_do(layer, 0, from_up, lambda x: x.wait_recv())
        halo_do(layer, 1, from_down, lambda x: x.wait_recv())

    def px_copy(slot, row):
        return pltpu.make_async_remote_copy(
            src_ref=pair.at[slot, row], dst_ref=pair.at[slot, row],
            send_sem=px_send.at[0], recv_sem=px_recv.at[slot],
            device_id={"tp": t1}, device_id_type=MESH,
        )

    def rs_copy(slot, k):
        return pltpu.make_async_remote_copy(
            src_ref=parts.at[slot, k], dst_ref=arrived.at[slot, k],
            send_sem=rs_send.at[0], recv_sem=rs_recv.at[slot, k],
            device_id={"tp": t2}, device_id_type=MESH,
        )

    def absorb(layer, slot, which, block, total):
        for k in range(CHUNKS):
            at = pl.ds(pl.multiple_of(block * feats + k * cols_k, cols_k), cols_k)
            wide = gathered[slot, block, k].astype(f32)
            scaled[which, :, at] = (wide * gain_ref[pl.ds(layer, 1), at]).astype(bf)
            total = total + jnp.sum(wide * wide, axis=1, keepdims=True)
        return total

    def scale_of(total):
        return lax.rsqrt(total / (tp_count * feats) + norm_eps)

    def half_dot(layer, which, first, weights):
        at = pl.ds(pl.multiple_of(first * feats, feats), 2 * feats)
        return jnp.dot(scaled[which, :, at], weights[layer, at, :], preferred_element_type=f32)

    def gate_of(layer, which, scale):
        acc = jnp.dot(scaled[which], wg[layer], preferred_element_type=f32)
        value = jax.nn.sigmoid(acc * scale)
        for k in range(CHUNKS):
            gate_buf[which, k] = value[:, k * cols_k:(k + 1) * cols_k]

    def share_pooled(slot, which, sums, cells):
        pooled = (sums / counts[which] - cells.astype(f32)).astype(bf)
        pair[slot, c] = pooled
        px_copy(slot, c).start()

    def back_part(layer, slot, cols, k):
        at = pl.ds(k * cols_k, cols_k)
        acc = jnp.dot(pair[slot, 0], wb[layer, cols, 0:b_rows, at], preferred_element_type=f32)
        return acc + jnp.dot(
            pair[slot, 1], wb[layer, cols, b_rows:2 * b_rows, at], preferred_element_type=f32
        )

    def back(layer, slot, which):
        units(px_recv.at[slot], 1).wait_recv()
        for k in range(CHUNKS):
            parts[slot, k] = back_part(layer, slot, far_base // 2, k).astype(bf)
            rs_copy(slot, k).start()
        for k in range(CHUNKS):
            own_part[which, k] = back_part(layer, slot, base // 2, k)

    def update(slot, which, k):
        units(rs_recv.at[slot, k], 1).wait_recv()
        branch = own_part[which, k] + arrived[slot, k].astype(f32)
        return (gathered[slot, t, k].astype(f32) + gate_buf[which, k] * branch).astype(bf)

    for k in range(CHUNKS):
        tok_load(k).start()
    gain_load.start()
    for layer in range(LAYERS):
        for piece in (0, 2, 1):
            load(layer, piece).start()

        @pl.when(jnp.logical_and(c == s_parity, jnp.logical_or(is_mid, layer > 0)))
        def _(layer=layer):
            wb_load(layer).start()
    for layer in range(LAYERS):
        for slot in (0, 2):
            halo[layer, slot] = jnp.zeros(halo.shape[2:], halo.dtype)

    barrier = pltpu.get_barrier_semaphore()
    for target in ({"grp": other}, {"tp": t1}, {"tp": t2}):
        pl.semaphore_signal(barrier, inc=1, device_id=target, device_id_type=MESH)

    @pl.when(s > 0)
    def _():
        for peer in (t, t1):
            pl.semaphore_signal(barrier, inc=1, device_id={"sp": s - 1, "tp": peer}, device_id_type=MESH)

    @pl.when(s < last)
    def _():
        for peer in (t, t1):
            pl.semaphore_signal(barrier, inc=1, device_id={"sp": s + 1, "tp": peer}, device_id_type=MESH)

    pl.semaphore_wait(barrier, 3 + jnp.where(s > 0, 2, 0) + jnp.where(s < last, 2, 0))

    def setup():
        half_span = jnp.int32(spans[0])
        for group_id in range(1, GROUPS):
            half_span = jnp.where(t == group_id, spans[group_id], half_span)
        shift = GRID_W.bit_length() - 1
        out_tok = lax.broadcasted_iota(jnp.int32, (toks, toks), 0)
        in_tok = lax.broadcasted_iota(jnp.int32, (toks, toks), 1)
        out_row = lax.shift_right_logical(out_tok, shift)
        out_col = lax.bitwise_and(out_tok, GRID_W - 1)
        in_col = lax.bitwise_and(in_tok, GRID_W - 1)
        near_col = (in_col >= out_col - half_span) & (in_col < out_col + half_span)
        for slot in range(3):
            in_row = (slot - 1) * rows_here + lax.shift_right_logical(in_tok, shift)
            inside = near_col & (in_row >= out_row - half_span) & (in_row < out_row + half_span)
            box[slot] = jnp.where(inside, 1.0, 0.0).astype(bf)
        tok_at = lax.broadcasted_iota(jnp.int32, counts.shape[1:], 0)
        col_at = lax.bitwise_and(tok_at, GRID_W - 1)
        col_counts = jnp.minimum(col_at + half_span, GRID_W) - jnp.maximum(col_at - half_span, 0)
        for which, plane in ((0, s), (1, end_here)):
            row_at = plane * rows_here + lax.shift_right_logical(tok_at, shift)
            row_counts = jnp.minimum(row_at + half_span, total_rows) - jnp.maximum(row_at - half_span, 0)
            counts[which] = (row_counts * col_counts).astype(f32)

    def box_dot(slot, value):
        return jnp.dot(box[slot], value, preferred_element_type=f32)

    for k in range(CHUNKS):
        tok_load(k).wait()
    gain_load.wait()
    waited_mid, waited_end = set(), set()
    zero = jnp.zeros((toks, 1), f32)

    def relay(mid, item):
        if item[0] == "own":
            own(mid, waited_mid if mid else waited_end, *item[1:])
        elif item[0] == "agf":
            pass_on(AGAIN, item[2])
        elif item[0] == "gate":
            again_gate()
        else:
            pump(mid, *item[1:])

    def gate_copy(k):
        return pltpu.make_async_remote_copy(
            src_ref=gate_sent.at[k], dst_ref=gate_sent.at[k],
            send_sem=gv_send.at[0], recv_sem=gv_recv.at[0],
            device_id={"sp": end_here}, device_id_type=MESH,
        )

    def again_gate():
        for which in (3, 2):
            units(ag_recv.at[AGAIN, which], 2).wait_recv()
        total = zero
        for block in (t, t1, t2, t3):
            total = absorb(1, AGAIN, 1, block, total)
        if AGAIN_FIRST:
            ready(1, 1)
        gate_of(1, 1, scale_of(total))
        for k in range(CHUNKS):
            gate_sent[k] = gate_buf[1, k].astype(bf)
            gate_copy(k).start()

    def gather_step(layer, slot, which, k, total):
        if k == 0:
            total = absorb(layer, slot, which, t, zero)
            units(ag_recv.at[slot, 3], 2).wait_recv()
            total = absorb(layer, slot, which, t1, total)
        pass_on(slot, k)
        if k == CHUNKS - 1:
            total = absorb(layer, slot, which, t2, total)
        return total

    def pool_step(layer, slot, which, total):
        ready(layer, 0)
        acc = half_dot(layer, which, base, wp)
        units(ag_recv.at[slot, 2], 2).wait_recv()
        total = absorb(layer, slot, which, t3, total)
        scale = scale_of(total)
        acc = acc + half_dot(layer, which, far_base, wp)
        return (acc * scale).astype(bf), scale

    @pl.when(is_end)
    def _():
        for item in END_FIRST:
            if item[0] == "tok":
                guest_copy(item[1]).start()
            elif item[0] == "ret":
                if item[1] == 0:
                    setup()
                return_copy(item[1]).wait_recv()
                start_gather(1, item[1])
            else:
                relay(False, item)

    @pl.when(is_mid)
    def _():
        guest_side = jnp.where(low, 0, 2)
        total, scale = {}, {}
        for item in MID_FIRST:
            name = item[0]
            slot = item[1]
            which = 1 if slot == GUEST else 0
            if name == "gstart":
                for k in range(CHUNKS):
                    start_gather(0, k)
            elif name == "guest":
                guest_copy(slot).wait_recv()
                start_gather(GUEST, slot)
            elif name == "agf":
                if item == ("agf", 0, 0):
                    setup()
                total[slot] = gather_step(0, slot, which, item[2], total.get(slot))
            elif name == "pool" and slot == 0:
                halo[0, 1], scale[0] = pool_step(0, 0, 0, total[0])
                halo_start(0)
            elif name == "pool":
                units(ag_recv.at[GUEST, 2], 2).wait_recv()
                total[slot] = absorb(0, GUEST, 1, t3, total[slot])
                scale[slot] = scale_of(total[slot])
                acc = half_dot(0, 1, base, wp) + half_dot(0, 1, far_base, wp)
                halo[0, guest_side] = (acc * scale[slot]).astype(bf)
                cells = halo[0, guest_side]
                sums = box_dot(1, cells) + box_dot(2 - guest_side, halo[0, 1])
                share_pooled(GUEST, 1, sums, cells)
            elif name == "box":
                halo_wait(0)
                cells = halo[0, 1]
                sums = box_dot(0, halo[0, 0]) + box_dot(1, cells) + box_dot(2, halo[0, 2])
                share_pooled(0, 0, sums, cells)
            elif name == "back":
                if slot == FIRST_BACK:
                    ready(0, 2)
                back(0, slot, which)
            elif name == "gate":
                if slot == FIRST_GATE:
                    ready(0, 1)
                gate_of(0, which, scale[slot])
            elif name == "upd":
                k = item[2]
                value = update(slot, which, k)
                if slot == GUEST:
                    gathered[AGAIN, t, k] = value
                    return_copy(k).start()
                    start_gather(AGAIN, k)
                else:
                    gathered[1, t, k] = value
                    start_gather(1, k)
            else:
                relay(True, item)

    steps = iter(zip(MID_REST, END_REST))

    def relays():
        for mid, items in zip((True, False), next(steps)):
            if items:
                @pl.when(is_mid if mid else is_end)
                def _(mid=mid, items=items):
                    for item in items:
                        relay(mid, item)

    for layer in range(1, LAYERS):
        total = None
        for k in range(CHUNKS):
            total = gather_step(layer, layer, 0, k, total)
            relays()
        cells, scale = pool_step(layer, layer, 0, total)
        halo[layer, 1] = cells
        halo_start(layer)
        relays()
        cells = halo[layer, 1]
        sums = box_dot(1, cells)
        halo_wait(layer)
        sums = sums + box_dot(0, halo[layer, 0]) + box_dot(2, halo[layer, 2])
        share_pooled(layer, 0, sums, cells)
        relays()
        ready(layer, 2)
        back(layer, layer, 0)
        relays()
        if layer == 1:
            @pl.when(is_mid)
            def _(scale=scale):
                if not AGAIN_FIRST:
                    ready(1, 1)
                gate_of(1, 0, scale)

            @pl.when(is_end)
            def _():
                units(gv_recv.at[0], CHUNKS).wait_recv()
                for k in range(CHUNKS):
                    gate_buf[0, k] = gate_sent[k].astype(f32)
        else:
            ready(layer, 1)
            gate_of(layer, 0, scale)
        relays()
        for k in range(CHUNKS):
            state = update(layer, 0, k)
            if layer + 1 < LAYERS:
                gathered[layer + 1, t, k] = state
                start_gather(layer + 1, k)
            else:
                out_ref[:, k * cols_k:(k + 1) * cols_k] = state
            relays()

    def sent(sem, count):
        units(sem, count).wait_send()

    def sent_blocks(flow, k, most, least):
        @pl.when(c == blocks[k] % 2)
        def _():
            sent(w_send.at[flow], most)

        @pl.when(c != blocks[k] % 2)
        def _():
            sent(w_send.at[flow], least)

    def sent_chain(layers, slots, gathers):
        @pl.when(c != s_parity)
        def _():
            sent(bx_send.at[0], 2 * layers)
        sent(ag_send.at[0], 6 * gathers)
        sent(rs_send.at[0], 2 * slots)
        sent(px_send.at[0], slots)

    @pl.when(is_mid)
    def _():
        sent(w_send.at[0], 4 * LAYERS)
        sent(w_send.at[1], 4 * (LAYERS - 1) - 2)
        for k in range(3):
            sent_blocks(2 + k, k, 5 * LAYERS, 3 * LAYERS)
        for k in (1, 2):
            sent_blocks(4 + k, k, 5 * (LAYERS - 1) - 2, 3 * (LAYERS - 1) - 2)
        sent(rt_send.at[0], CHUNKS)
        sent(gv_send.at[0], CHUNKS)
        sent_chain(LAYERS, LAYERS + 1, LAYERS + 2)

    @pl.when(is_end)
    def _():
        sent(w_send.at[0], 4 * LAYERS)
        sent(w_send.at[1], 4 * LAYERS)
        for k in range(3):
            sent_blocks(2 + k, k, 5 * (LAYERS - 1) - 2, 3 * (LAYERS - 1) - 2)
        sent(tk_send.at[0], CHUNKS)
        sent_chain(LAYERS - 1, LAYERS - 1, LAYERS - 1)
    for layer in range(LAYERS):
        outward = layer > 0
        halo_do(layer, 0, (s < last) if outward else (s == 1), lambda x: x.wait_send())
        halo_do(layer, 1, (s > 0) if outward else (s == 2), lambda x: x.wait_send())


def fused(tokens_in, norm_gain, w_pool_in, w_gate, w_back):
    sp_count, tp_count = lax.axis_size("sp"), lax.axis_size("tp")
    toks, feats = tokens_in.shape
    _, depth, local_pool = w_pool_in.shape
    b_rows, b_cols = w_back.shape[1:]
    cols_k = feats // CHUNKS
    bf, f32 = jnp.bfloat16, jnp.float32
    dma = pltpu.SemaphoreType.DMA
    slots = LAYERS + 1
    hbm = pl.BlockSpec(memory_space=pltpu.HBM)
    return pl.pallas_call(
        functools.partial(fused_kernel, sp_count, tp_count),
        out_shape=pltpu.VMEM((toks, feats), bf),
        in_specs=[hbm] * 5,
        out_specs=pl.BlockSpec(memory_space=pltpu.VMEM),
        scratch_shapes=[
            pltpu.VMEM((LAYERS, sp_count * depth, local_pool), bf),
            pltpu.VMEM((LAYERS, sp_count * depth, w_gate.shape[2]), bf),
            pltpu.VMEM((LAYERS, 2, 2 * b_rows, b_cols), bf),
            pltpu.VMEM((LAYERS, b_rows, b_cols), bf),
            pltpu.VMEM((slots + 1, tp_count, CHUNKS, toks, cols_k), bf),
            pltpu.VMEM((2, toks, tp_count * feats), bf),
            pltpu.VMEM((LAYERS, 3, toks, local_pool), bf),
            pltpu.VMEM((2, CHUNKS, toks, cols_k), f32),
            pltpu.VMEM((2, CHUNKS, toks, cols_k), f32),
            pltpu.VMEM((3, toks, toks), bf),
            pltpu.VMEM((2, toks, local_pool), f32),
            pltpu.VMEM((slots, 2, toks, local_pool), bf),
            pltpu.VMEM((slots, CHUNKS, toks, cols_k), bf),
            pltpu.VMEM((slots, CHUNKS, toks, cols_k), bf),
            pltpu.VMEM((CHUNKS, toks, cols_k), bf),
            pltpu.VMEM(norm_gain.shape, f32),
            dma((LAYERS + 1, 4)),
            dma((7,)), dma((LAYERS, 3, 5)), dma((3, 2)), dma((LAYERS, 3)),
            dma((1,)), dma((LAYERS,)),
            dma((1,)), dma((CHUNKS,)), dma((1,)), dma((CHUNKS,)),
            dma((1,)), dma((slots + 1, 4)),
            dma((LAYERS, 2)), dma((LAYERS, 2)),
            dma((1,)), dma((slots,)),
            dma((1,)), dma((slots, CHUNKS)),
            dma((1,)), dma((1,)),
        ],
        compiler_params=pltpu.CompilerParams(
            collective_id=0, has_side_effects=True, vmem_limit_bytes=56 * 1024 * 1024
        ),
    )(tokens_in, norm_gain, w_pool_in, w_gate, w_back)

def dispatch(tokens_in, norm_gain, w_pool_in, w_gate, w_back):
    fits = (
        lax.axis_size("grp") == 2
        and lax.axis_size("tp") == GROUPS == 4
        and lax.axis_size("sp") == lax.axis_size("tp")
        and w_pool_in.shape[2] * GROUPS == POOL_WIDTH
        and w_pool_in.shape[1] == tokens_in.shape[1] == w_gate.shape[2] == w_back.shape[2]
        and tokens_in.shape[1] == 2 * tokens_in.shape[0] == 2 * w_pool_in.shape[2]
        and tokens_in.shape[0] // GRID_W >= max(pool_windows) // 2
    )
    step = fused if fits else on_device
    return step(tokens_in, norm_gain, w_pool_in, w_gate, w_back)


def solution(mesh):
    return jax.shard_map(
        dispatch,
        mesh=mesh,
        in_specs=(
            P(("grp", "sp"), "tp"),
            P(),
            P(None, "sp", "tp"),
            P(None, "sp", "tp"),
            P(None, "tp", "sp"),
        ),
        out_specs=P(("grp", "sp"), "tp"),
        check_vma=False,
    )
```

```python
import jax
import jax.numpy as jnp
from jax import lax
from jax.experimental import pallas as pl
from jax.experimental.pallas import tpu as pltpu
from jax.sharding import PartitionSpec as P
import functools

POOL_WIDTH = 1024
GROUPS = 4
GRID_W = 32
LAYERS = 3


pool_windows = (2, 4, 8, 16)
norm_eps = 1e-06


def padded_2(value, sides, width):
    for axis, dim in sides:
        peers, length = (lax.axis_size(axis), value.shape[dim])
        up = [(i, (i + 1) % peers) for i in range(peers - 1)]
        down = [(j, i) for i, j in up]
        last = lax.slice_in_dim(value, length - width, length, axis=dim)
        initial = lax.slice_in_dim(value, 0, width, axis=dim)
        before = lax.ppermute(last, axis, up)
        after = lax.ppermute(initial, axis, down)
        value = jnp.concatenate([before, value, after], axis=dim)
    return value


def window_means(padded, rows_here, first_row, total_rows, window):
    reach = max(pool_windows) // 2
    half_span = window // 2
    width_cols = padded.shape[1] - 2 * reach
    row_sums = padded[reach - half_span : reach - half_span + rows_here]
    for offset in range(1 - half_span, half_span):
        row_sums = row_sums + padded[reach + offset : reach + offset + rows_here]
    box_sums = row_sums[:, reach - half_span : reach - half_span + width_cols]
    for offset in range(1 - half_span, half_span):
        box_sums = box_sums + row_sums[:, reach + offset : reach + offset + width_cols]
    row_index = first_row + jnp.arange(rows_here, dtype=jnp.int32)
    col_index = jnp.arange(width_cols, dtype=jnp.int32)
    row_counts = jnp.minimum(row_index + half_span, total_rows) - jnp.maximum(
        row_index - half_span, 0
    )
    col_counts = jnp.minimum(col_index + half_span, width_cols) - jnp.maximum(
        col_index - half_span, 0
    )
    counts = (row_counts[:, None] * col_counts[None, :]).astype(jnp.float32)
    return box_sums / counts[:, :, None]


def on_device(tokens_in, norm_gain, w_pool_in, w_gate, w_back):
    reach = max(pool_windows) // 2
    sp_count = lax.axis_size("sp")
    tp_count = lax.axis_size("tp")
    tp_pos = lax.axis_index("tp")
    sp_pos = lax.axis_index("sp")
    tok_rows = tokens_in.shape[0]
    rows_here = tok_rows // GRID_W
    total_rows = rows_here * sp_count
    first_row = sp_pos * rows_here
    local_pool = w_pool_in.shape[2]
    group_width = POOL_WIDTH // GROUPS
    channel_group = (tp_pos * local_pool + jnp.arange(local_pool, dtype=jnp.int32)) // group_width
    state = tokens_in
    for layer_id in range(LAYERS):
        whole_rows = lax.all_gather(state, "tp", axis=1, tiled=True)
        wide = whole_rows.astype(jnp.float32)
        normed = (
            wide
            * lax.rsqrt(jnp.mean(wide * wide, axis=-1, keepdims=True) + norm_eps)
            * norm_gain[layer_id]
        ).astype(jnp.bfloat16)
        pool_acc = jnp.dot(
            normed,
            lax.all_gather(w_pool_in[layer_id], "sp", axis=0, tiled=True),
            preferred_element_type=jnp.float32,
        )
        gate_acc = jnp.dot(
            normed,
            lax.all_gather(w_gate[layer_id], "sp", axis=0, tiled=True),
            preferred_element_type=jnp.float32,
        )
        pool_in = pool_acc.astype(jnp.bfloat16)
        gate = jax.nn.sigmoid(gate_acc)
        cells = pool_in.reshape(rows_here, GRID_W, local_pool)
        rimmed = padded_2(cells, (("sp", 0),), reach)
        padded = jnp.pad(rimmed.astype(jnp.float32), ((0, 0), (reach, reach), (0, 0)))
        means = jnp.zeros((rows_here, GRID_W, local_pool), jnp.float32)
        for group_id in range(GROUPS):
            in_group = (channel_group == group_id)[None, None, :]
            means = jnp.where(
                in_group,
                window_means(padded, rows_here, first_row, total_rows, pool_windows[group_id]),
                means,
            )
        pooled = (
            (means - cells.astype(jnp.float32)).reshape(tok_rows, local_pool).astype(jnp.bfloat16)
        )
        full_pooled = lax.all_gather(pooled, "tp", axis=1, tiled=True)
        back_rows = lax.all_gather(w_back[layer_id], "sp", axis=1, tiled=True)
        back_cols = lax.all_to_all(back_rows, "tp", split_axis=1, concat_axis=0, tiled=True)
        partials = jnp.einsum(
            "tnb,nbd->ntd",
            full_pooled.reshape(tok_rows, tp_count, local_pool),
            back_cols.reshape(tp_count, local_pool, back_cols.shape[1]),
            preferred_element_type=jnp.float32,
        ).astype(jnp.bfloat16)
        branch = jnp.sum(partials.astype(jnp.float32), axis=0)
        state = (state.astype(jnp.float32) + gate * branch).astype(jnp.bfloat16)
    return state


MESH = pl.DeviceIdType.MESH
POOL, GATE_A, GATE_B, BACK = range(4)
UNITS = {POOL: (0,), GATE_A: (1,), GATE_B: (2,), BACK: (3, 4), 4: (5,), 5: (6,)}
GATE_PART = {1: 0, 2: 1, 5: 2, 6: 3}
CHUNKS = 2
GUEST, AGAIN = LAYERS, LAYERS + 1


MID_FIRST = (
    ("own", 2, 1, 0), ("own", 2, 1, 2), ("own", 0, 0, 0), ("own", 0, 0, 2), ("gstart", 0),
    ("pump", 0, 1, 0), ("pump", 0, 0, 0), ("own", 0, 0, 3), ("guest", 0), ("pump", 0, 1, 2),
    ("own", 2, 1, 4), ("pump", 0, 2, 0), ("pump", 0, 0, 3), ("pump", 0, 1, 3), ("own", 1, 0, 3),
    ("agf", 0, 0), ("own", 1, 1, 3), ("agf", 0, 1), ("own", 1, 1, 0), ("own", 1, 0, 0), ("own", 2, 1, 3),
    ("guest", 1), ("pump", 0, 2, 3), ("pool", 0), ("pump", 0, 0, 2), ("pump", 1, 1, 0), ("agf", 3, 0),
    ("agf", 3, 1), ("own", 0, 0, 1), ("pump", 0, 0, 1), ("pump", 1, 1, 3), ("pool", 3), ("box", 0),
    ("own", 2, 1, 1), ("own", 2, 1, 5), ("own", 2, 0, 1), ("pump", 1, 0, 0), ("pump", 0, 2, 2), ("back", 3),
    ("own", 1, 0, 1), ("pump", 0, 1, 1), ("own", 1, 0, 2), ("back", 0), ("pump", 0, 2, 1),
    ("pump", 2, 1, 1), ("pump", 1, 2, 0), ("gate", 3), ("pump", 1, 0, 3), ("gate", 0), ("upd", 0, 0),
    ("upd", 0, 1), ("upd", 3, 0), ("upd", 3, 1), ("pump", 1, 0, 2), ("own", 2, 0, 2), ("pump", 1, 1, 1),
    ("pump", 1, 0, 1), ("pump", 1, 1, 2), ("pump", 1, 2, 3),
)
END_FIRST = (
    ("own", 0, 0, 0), ("tok", 0), ("own", 0, 0, 3), ("own", 0, 1, 0), ("tok", 1), ("own", 0, 0, 2),
    ("own", 0, 0, 1), ("own", 1, 0, 0), ("own", 0, 1, 3), ("own", 0, 1, 2), ("own", 0, 1, 1),
    ("own", 1, 0, 2), ("own", 1, 0, 3), ("own", 1, 0, 1), ("own", 1, 1, 2), ("pump", 1, 0, 0),
    ("pump", 1, 1, 0), ("own", 2, 0, 3), ("pump", 1, 1, 3), ("pump", 2, 0, 2), ("pump", 1, 0, 3),
    ("pump", 2, 0, 0), ("own", 1, 1, 0), ("own", 1, 1, 1), ("pump", 1, 2, 0), ("pump", 2, 0, 5), ("ret", 0),
    ("ret", 1),
)
MID_REST = (
    (
        ("pump", 1, 2, 2), ("pump", 2, 0, 3),
    ),
    (
        ("pump", 2, 1, 2), ("pump", 1, 2, 1), ("agf", 4, 0),
    ),
    (
        ("own", 2, 0, 0), ("agf", 4, 1), ("pump", 2, 2, 3), ("gate", 4), ("pump", 2, 0, 0),
        ("own", 2, 0, 3),
    ),
    (),
    (),
    (
        ("pump", 2, 2, 0), ("own", 2, 0, 5), ("pump", 2, 0, 1), ("pump", 2, 1, 0),
    ),
    (),
    (
        ("pump", 2, 0, 5), ("pump", 2, 1, 3), ("pump", 2, 1, 5), ("pump", 2, 0, 2), ("pump", 2, 2, 2),
        ("pump", 2, 0, 4),
    ),
    (),
    (
        ("pump", 2, 2, 5), ("own", 2, 0, 4),
    ),
    (
        ("pump", 2, 1, 4), ("pump", 2, 2, 4), ("pump", 2, 2, 1),
    ),
    (),
    (),
    (),
    (),
    (),
)
END_REST = (
    (
        ("pump", 2, 0, 4), ("pump", 2, 1, 1),
    ),
    (
        ("pump", 1, 2, 3), ("own", 2, 0, 0),
    ),
    (
        ("own", 1, 1, 3), ("own", 2, 0, 4), ("pump", 2, 0, 3), ("own", 2, 0, 5), ("own", 2, 0, 1),
        ("own", 2, 0, 2), ("pump", 2, 1, 2),
    ),
    (
        ("pump", 2, 2, 3), ("own", 2, 1, 2), ("own", 2, 1, 3),
    ),
    (
        ("own", 2, 1, 0),
    ),
    (),
    (
        ("own", 2, 1, 5), ("pump", 2, 0, 1), ("own", 2, 1, 4),
    ),
    (
        ("pump", 2, 2, 0), ("pump", 2, 1, 0),
    ),
    (),
    (
        ("pump", 2, 1, 3),
    ),
    (
        ("pump", 2, 1, 5), ("pump", 2, 2, 2),
    ),
    (
        ("pump", 2, 2, 5),
    ),
    (
        ("own", 2, 1, 1), ("pump", 2, 1, 4), ("pump", 2, 2, 4), ("pump", 2, 2, 1),
    ),
    (),
    (),
    (),
)
AGAIN_FIRST = True
FIRST_BACK, FIRST_GATE = 3, 3


def fused_kernel(
    sp_count, tp_count,
    tok_hbm, gain_hbm, wp_hbm, wg_hbm, wb_hbm, out_ref,
    wp, wg, wb, wb_own, gathered, scaled, halo, gate_buf, own_part, box, counts,
    pair, parts, arrived, gate_sent, gain_ref,
    load_sem, w_send, z_recv, z_fine, y_recv, bx_send, bx_recv, tk_send, tk_recv, rt_send, rt_recv,
    ag_send, ag_recv, h_send, h_recv, px_send, px_recv, rs_send, rs_recv, gv_send, gv_recv,
):
    g = lax.axis_index("grp")
    s = lax.axis_index("sp")
    t = lax.axis_index("tp")
    other = 1 - g
    c = t % 2
    base = t - c
    t1 = base + 1 - c
    t2 = (t + 2) % tp_count
    t3 = (t1 + 2) % tp_count
    far_base = (base + 2) % tp_count
    last = sp_count - 1
    toks, feats = tok_hbm.shape
    local_pool = wp.shape[2]
    cols_k = feats // CHUNKS
    rows_here = toks // GRID_W
    total_rows = rows_here * sp_count
    bf, f32 = jnp.bfloat16, jnp.float32

    low = s < 2
    is_mid = jnp.logical_and(s > 0, s < last)
    is_end = jnp.logical_not(is_mid)
    end_here = jnp.where(low, 0, last)
    mid_here = jnp.where(low, 1, last - 1)
    end_far = last - end_here
    mid_far = last - mid_here
    blocks = (
        jnp.where(is_mid, end_here, mid_here),
        jnp.where(is_mid, mid_far, mid_far),
        end_far,
    )
    s_parity = s % 2

    p_rows, g_rows = wp_hbm.shape[1], wg_hbm.shape[1]
    b_rows = wb_hbm.shape[1]

    def gate_cuts(layer):
        return 8 if layer == LAYERS - 1 else 4

    def view(layer, block, half, unit, row=None):
        if unit == 0:
            n = p_rows // 2
            return wp.at[layer, pl.ds(pl.multiple_of(block * p_rows + half * n, n), n), :]
        if unit in GATE_PART:
            n = g_rows // gate_cuts(layer)
            at = block * g_rows + half * (g_rows // 2) + GATE_PART[unit] * n
            return wg.at[layer, pl.ds(pl.multiple_of(at, n), n), :]
        n = b_rows // 2
        row = unit - 3 if row is None else row
        return wb.at[layer, block // 2, pl.ds(pl.multiple_of(row * b_rows + half * n, n), n), :]

    unit_rows = g_rows // 4

    def units(sem, count):
        ref = wg.at[pl.ds(0, 2 if count > 16 else 1), pl.ds(0, int(unit_rows * (count if count <= 16 else count // 2))), :]
        return pltpu.make_async_remote_copy(
            src_ref=ref, dst_ref=ref, send_sem=sem, recv_sem=sem,
            device_id={"grp": other}, device_id_type=MESH,
        )

    def w_copy(layer, flow, block, half, unit, target, recv):
        ref = view(layer, block, half, unit)
        return pltpu.make_async_remote_copy(
            src_ref=ref, dst_ref=ref, send_sem=w_send.at[flow], recv_sem=recv,
            device_id=target, device_id_type=MESH,
        )

    def kind(piece):
        return {POOL: 0, BACK: 2}.get(piece, 1)

    def z_sem(layer, k, unit):
        return z_recv.at[layer, k, unit] if unit < 5 else z_fine.at[k, unit - 5]

    def own_sem(layer, k, piece):
        return z_recv.at[layer, k, 3 + c] if piece == BACK else z_sem(layer, k, UNITS[piece][0])

    def amount(layer, piece):
        return 1 if piece in (POOL, BACK) else 4 / gate_cuts(layer)

    def own_copy(layer, flow, half, piece, plane, recv):
        if piece != BACK:
            return w_copy(layer, flow, s, half, UNITS[piece][0], {"sp": plane}, recv)
        n = b_rows // 2
        return pltpu.make_async_remote_copy(
            src_ref=wb_own.at[layer, pl.ds(pl.multiple_of(half * n, n), n), :],
            dst_ref=view(layer, s, half, 3, row=c),
            send_sem=w_send.at[flow], recv_sem=recv,
            device_id={"sp": plane, "tp": base + s_parity}, device_id_type=MESH,
        )

    def holds(block, piece, fn):
        if piece == BACK:
            pl.when(c == block % 2)(fn)
        else:
            fn()

    def pump(mid, layer, k, piece):
        block = blocks[k]

        def act():
            for unit in UNITS[piece]:
                units(z_sem(layer, k, unit), amount(layer, piece)).wait_recv()
                if k == 0 and mid:
                    w_copy(layer, 2, block, g, unit, {"sp": mid_far}, z_sem(layer, 2, unit)).start()
                    continue
                w_copy(
                    layer, 2 + k, block, g, unit, {"grp": other}, y_recv.at[layer, kind(piece)]
                ).start()
                if mid and layer > 0 and (layer, kind(piece)) != (1, 1):
                    w_copy(
                        layer, 4 + k, block, g, unit, {"sp": end_here}, z_sem(layer, k, unit)
                    ).start()
        holds(block, piece, act)

    def own(mid, waited, layer, flow, piece):
        if (layer, kind(piece)) not in waited:
            waited.add((layer, kind(piece)))
            load(layer, kind(piece)).wait()
            if piece == BACK and (mid or layer > 0):
                @pl.when(c != s_parity)
                def _():
                    bx_copy(layer).start()
        if mid and flow == 0:
            own_copy(layer, 0, g, piece, mid_far, own_sem(layer, 1, piece)).start()
        elif mid:
            own_copy(layer, 1, g, piece, end_here, own_sem(layer, 0, piece)).start()
        elif flow == 0:
            own_copy(layer, 0, g, piece, mid_here, own_sem(layer, 0, piece)).start()
        else:
            own_copy(layer, 1, other, piece, mid_here, y_recv.at[layer, kind(piece)]).start()

    def bx_copy(layer):
        return pltpu.make_async_remote_copy(
            src_ref=wb_own.at[layer],
            dst_ref=wb.at[layer, s // 2, pl.ds(pl.multiple_of(c * b_rows, b_rows), b_rows), :],
            send_sem=bx_send.at[0], recv_sem=bx_recv.at[layer],
            device_id={"tp": t1}, device_id_type=MESH,
        )

    def wb_load(layer):
        return pltpu.make_async_copy(
            wb_hbm.at[layer],
            wb.at[layer, s // 2, pl.ds(pl.multiple_of(c * b_rows, b_rows), b_rows), :],
            load_sem.at[layer, 3],
        )

    def load(layer, piece):
        if piece == 0:
            src, dst = wp_hbm.at[layer], wp.at[layer, pl.ds(pl.multiple_of(s * p_rows, p_rows), p_rows), :]
        elif piece == 1:
            src, dst = wg_hbm.at[layer], wg.at[layer, pl.ds(pl.multiple_of(s * g_rows, g_rows), g_rows), :]
        else:
            src, dst = wb_hbm.at[layer], wb_own.at[layer]
        return pltpu.make_async_copy(src, dst, load_sem.at[layer, piece])

    def ready(layer, which):
        if which < 2:
            units(y_recv.at[layer, which], 3 * (1 + which)).wait_recv()
            return

        @pl.when(c == s_parity)
        def _():
            units(y_recv.at[layer, 2], 2).wait_recv()
            wb_load(layer).wait()
            units(bx_recv.at[layer], 2).wait_recv()

        @pl.when(c != s_parity)
        def _():
            units(y_recv.at[layer, 2], 4).wait_recv()

    def tok_load(k):
        return pltpu.make_async_copy(
            tok_hbm.at[:, pl.ds(k * cols_k, cols_k)], gathered.at[0, t, k], load_sem.at[LAYERS, k]
        )

    gain_load = pltpu.make_async_copy(gain_hbm, gain_ref, load_sem.at[LAYERS, CHUNKS])

    def guest_copy(k):
        return pltpu.make_async_remote_copy(
            src_ref=gathered.at[0, t, k], dst_ref=gathered.at[GUEST, t, k],
            send_sem=tk_send.at[0], recv_sem=tk_recv.at[k],
            device_id={"sp": mid_here}, device_id_type=MESH,
        )

    def return_copy(k):
        return pltpu.make_async_remote_copy(
            src_ref=gathered.at[AGAIN, t, k], dst_ref=gathered.at[1, t, k],
            send_sem=rt_send.at[0], recv_sem=rt_recv.at[k],
            device_id={"sp": end_here}, device_id_type=MESH,
        )

    def ag_copy(slot, k, block, target, recv):
        return pltpu.make_async_remote_copy(
            src_ref=gathered.at[slot, block, k], dst_ref=gathered.at[slot, block, k],
            send_sem=ag_send.at[0], recv_sem=ag_recv.at[slot, recv],
            device_id={"tp": target}, device_id_type=MESH,
        )

    def start_gather(slot, k):
        ag_copy(slot, k, t, t2, k).start()
        ag_copy(slot, k, t, t1, 3).start()

    def pass_on(slot, k):
        units(ag_recv.at[slot, k], 1).wait_recv()
        ag_copy(slot, k, t2, t1, 2).start()

    spans = [w // 2 for w in pool_windows]

    def h_copy(layer, way, span):
        rows = (span if way == 0 else max(span - 1, 1)) * GRID_W
        at = toks - rows if way == 0 else 0
        return pltpu.make_async_remote_copy(
            src_ref=halo.at[layer, 1, pl.ds(at, rows), :],
            dst_ref=halo.at[layer, 0 if way == 0 else 2, pl.ds(at, rows), :],
            send_sem=h_send.at[layer, way], recv_sem=h_recv.at[layer, way],
            device_id={"sp": s + 1 if way == 0 else s - 1}, device_id_type=MESH,
        )

    def halo_do(layer, way, cond, op):
        for group_id, span in enumerate(spans):
            @pl.when(jnp.logical_and(cond, t == group_id))
            def _(span=span):
                op(h_copy(layer, way, span))

    def halo_start(layer):
        up_ok = jnp.logical_and(s < last, jnp.logical_or(layer > 0, s == 1))
        down_ok = jnp.logical_and(s > 0, jnp.logical_or(layer > 0, s == 2))
        halo_do(layer, 0, up_ok, lambda x: x.start())
        halo_do(layer, 1, down_ok, lambda x: x.start())

    def halo_wait(layer):
        from_up = jnp.logical_and(s > 0, jnp.logical_or(layer > 0, s == 2))
        from_down = jnp.logical_and(s < last, jnp.logical_or(layer > 0, s == 1))
        halo_do(layer, 0, from_up, lambda x: x.wait_recv())
        halo_do(layer, 1, from_down, lambda x: x.wait_recv())

    def px_copy(slot, row):
        return pltpu.make_async_remote_copy(
            src_ref=pair.at[slot, row], dst_ref=pair.at[slot, row],
            send_sem=px_send.at[0], recv_sem=px_recv.at[slot],
            device_id={"tp": t1}, device_id_type=MESH,
        )

    def rs_copy(slot, k):
        return pltpu.make_async_remote_copy(
            src_ref=parts.at[slot, k], dst_ref=arrived.at[slot, k],
            send_sem=rs_send.at[0], recv_sem=rs_recv.at[slot, k],
            device_id={"tp": t2}, device_id_type=MESH,
        )

    def absorb(layer, slot, which, block, total):
        for k in range(CHUNKS):
            at = pl.ds(pl.multiple_of(block * feats + k * cols_k, cols_k), cols_k)
            wide = gathered[slot, block, k].astype(f32)
            scaled[which, :, at] = (wide * gain_ref[pl.ds(layer, 1), at]).astype(bf)
            total = total + jnp.sum(wide * wide, axis=1, keepdims=True)
        return total

    def scale_of(total):
        return lax.rsqrt(total / (tp_count * feats) + norm_eps)

    def half_dot(layer, which, first, weights):
        at = pl.ds(pl.multiple_of(first * feats, feats), 2 * feats)
        return jnp.dot(scaled[which, :, at], weights[layer, at, :], preferred_element_type=f32)

    def gate_of(layer, which, scale):
        acc = jnp.dot(scaled[which], wg[layer], preferred_element_type=f32)
        value = jax.nn.sigmoid(acc * scale)
        for k in range(CHUNKS):
            gate_buf[which, k] = value[:, k * cols_k:(k + 1) * cols_k]

    def share_pooled(slot, which, sums, cells):
        pooled = (sums / counts[which] - cells.astype(f32)).astype(bf)
        pair[slot, c] = pooled
        px_copy(slot, c).start()

    def back_part(layer, slot, cols, k):
        at = pl.ds(k * cols_k, cols_k)
        acc = jnp.dot(pair[slot, 0], wb[layer, cols, 0:b_rows, at], preferred_element_type=f32)
        return acc + jnp.dot(
            pair[slot, 1], wb[layer, cols, b_rows:2 * b_rows, at], preferred_element_type=f32
        )

    def back(layer, slot, which):
        units(px_recv.at[slot], 1).wait_recv()
        for k in range(CHUNKS):
            parts[slot, k] = back_part(layer, slot, far_base // 2, k).astype(bf)
            rs_copy(slot, k).start()
        for k in range(CHUNKS):
            own_part[which, k] = back_part(layer, slot, base // 2, k)

    def update(slot, which, k):
        units(rs_recv.at[slot, k], 1).wait_recv()
        branch = own_part[which, k] + arrived[slot, k].astype(f32)
        return (gathered[slot, t, k].astype(f32) + gate_buf[which, k] * branch).astype(bf)

    for k in range(CHUNKS):
        tok_load(k).start()
    gain_load.start()
    for layer in range(LAYERS):
        for piece in (0, 2, 1):
            load(layer, piece).start()

        @pl.when(jnp.logical_and(c == s_parity, jnp.logical_or(is_mid, layer > 0)))
        def _(layer=layer):
            wb_load(layer).start()
    for layer in range(LAYERS):
        for slot in (0, 2):
            halo[layer, slot] = jnp.zeros(halo.shape[2:], halo.dtype)

    barrier = pltpu.get_barrier_semaphore()
    for target in ({"grp": other}, {"tp": t1}, {"tp": t2}):
        pl.semaphore_signal(barrier, inc=1, device_id=target, device_id_type=MESH)

    @pl.when(s > 0)
    def _():
        for peer in (t, t1):
            pl.semaphore_signal(barrier, inc=1, device_id={"sp": s - 1, "tp": peer}, device_id_type=MESH)

    @pl.when(s < last)
    def _():
        for peer in (t, t1):
            pl.semaphore_signal(barrier, inc=1, device_id={"sp": s + 1, "tp": peer}, device_id_type=MESH)

    pl.semaphore_wait(barrier, 3 + jnp.where(s > 0, 2, 0) + jnp.where(s < last, 2, 0))

    def setup():
        half_span = jnp.int32(spans[0])
        for group_id in range(1, GROUPS):
            half_span = jnp.where(t == group_id, spans[group_id], half_span)
        shift = GRID_W.bit_length() - 1
        out_tok = lax.broadcasted_iota(jnp.int32, (toks, toks), 0)
        in_tok = lax.broadcasted_iota(jnp.int32, (toks, toks), 1)
        out_row = lax.shift_right_logical(out_tok, shift)
        out_col = lax.bitwise_and(out_tok, GRID_W - 1)
        in_col = lax.bitwise_and(in_tok, GRID_W - 1)
        near_col = (in_col >= out_col - half_span) & (in_col < out_col + half_span)
        for slot in range(3):
            in_row = (slot - 1) * rows_here + lax.shift_right_logical(in_tok, shift)
            inside = near_col & (in_row >= out_row - half_span) & (in_row < out_row + half_span)
            box[slot] = jnp.where(inside, 1.0, 0.0).astype(bf)
        tok_at = lax.broadcasted_iota(jnp.int32, counts.shape[1:], 0)
        col_at = lax.bitwise_and(tok_at, GRID_W - 1)
        col_counts = jnp.minimum(col_at + half_span, GRID_W) - jnp.maximum(col_at - half_span, 0)
        for which, plane in ((0, s), (1, end_here)):
            row_at = plane * rows_here + lax.shift_right_logical(tok_at, shift)
            row_counts = jnp.minimum(row_at + half_span, total_rows) - jnp.maximum(row_at - half_span, 0)
            counts[which] = (row_counts * col_counts).astype(f32)

    def box_dot(slot, value):
        return jnp.dot(box[slot], value, preferred_element_type=f32)

    for k in range(CHUNKS):
        tok_load(k).wait()
    gain_load.wait()
    waited_mid, waited_end = set(), set()
    zero = jnp.zeros((toks, 1), f32)

    def relay(mid, item):
        if item[0] == "own":
            own(mid, waited_mid if mid else waited_end, *item[1:])
        elif item[0] == "agf":
            pass_on(AGAIN, item[2])
        elif item[0] == "gate":
            again_gate()
        else:
            pump(mid, *item[1:])

    def gate_copy(k):
        return pltpu.make_async_remote_copy(
            src_ref=gate_sent.at[k], dst_ref=gate_sent.at[k],
            send_sem=gv_send.at[0], recv_sem=gv_recv.at[0],
            device_id={"sp": end_here}, device_id_type=MESH,
        )

    def again_gate():
        for which in (3, 2):
            units(ag_recv.at[AGAIN, which], 2).wait_recv()
        total = zero
        for block in (t, t1, t2, t3):
            total = absorb(1, AGAIN, 1, block, total)
        if AGAIN_FIRST:
            ready(1, 1)
        gate_of(1, 1, scale_of(total))
        for k in range(CHUNKS):
            gate_sent[k] = gate_buf[1, k].astype(bf)
            gate_copy(k).start()

    def gather_step(layer, slot, which, k, total):
        if k == 0:
            total = absorb(layer, slot, which, t, zero)
            units(ag_recv.at[slot, 3], 2).wait_recv()
            total = absorb(layer, slot, which, t1, total)
        pass_on(slot, k)
        if k == CHUNKS - 1:
            total = absorb(layer, slot, which, t2, total)
        return total

    def pool_step(layer, slot, which, total):
        ready(layer, 0)
        acc = half_dot(layer, which, base, wp)
        units(ag_recv.at[slot, 2], 2).wait_recv()
        total = absorb(layer, slot, which, t3, total)
        scale = scale_of(total)
        acc = acc + half_dot(layer, which, far_base, wp)
        return (acc * scale).astype(bf), scale

    @pl.when(is_end)
    def _():
        for item in END_FIRST:
            if item[0] == "tok":
                guest_copy(item[1]).start()
            elif item[0] == "ret":
                if item[1] == 0:
                    setup()
                return_copy(item[1]).wait_recv()
                start_gather(1, item[1])
            else:
                relay(False, item)

    @pl.when(is_mid)
    def _():
        guest_side = jnp.where(low, 0, 2)
        total, scale = {}, {}
        for item in MID_FIRST:
            name = item[0]
            slot = item[1]
            which = 1 if slot == GUEST else 0
            if name == "gstart":
                for k in range(CHUNKS):
                    start_gather(0, k)
            elif name == "guest":
                guest_copy(slot).wait_recv()
                start_gather(GUEST, slot)
            elif name == "agf":
                if item == ("agf", 0, 0):
                    setup()
                total[slot] = gather_step(0, slot, which, item[2], total.get(slot))
            elif name == "pool" and slot == 0:
                halo[0, 1], scale[0] = pool_step(0, 0, 0, total[0])
                halo_start(0)
            elif name == "pool":
                units(ag_recv.at[GUEST, 2], 2).wait_recv()
                total[slot] = absorb(0, GUEST, 1, t3, total[slot])
                scale[slot] = scale_of(total[slot])
                acc = half_dot(0, 1, base, wp) + half_dot(0, 1, far_base, wp)
                halo[0, guest_side] = (acc * scale[slot]).astype(bf)
                cells = halo[0, guest_side]
                sums = box_dot(1, cells) + box_dot(2 - guest_side, halo[0, 1])
                share_pooled(GUEST, 1, sums, cells)
            elif name == "box":
                halo_wait(0)
                cells = halo[0, 1]
                sums = box_dot(0, halo[0, 0]) + box_dot(1, cells) + box_dot(2, halo[0, 2])
                share_pooled(0, 0, sums, cells)
            elif name == "back":
                if slot == FIRST_BACK:
                    ready(0, 2)
                back(0, slot, which)
            elif name == "gate":
                if slot == FIRST_GATE:
                    ready(0, 1)
                gate_of(0, which, scale[slot])
            elif name == "upd":
                k = item[2]
                value = update(slot, which, k)
                if slot == GUEST:
                    gathered[AGAIN, t, k] = value
                    return_copy(k).start()
                    start_gather(AGAIN, k)
                else:
                    gathered[1, t, k] = value
                    start_gather(1, k)
            else:
                relay(True, item)

    steps = iter(zip(MID_REST, END_REST))

    def relays():
        for mid, items in zip((True, False), next(steps)):
            if items:
                @pl.when(is_mid if mid else is_end)
                def _(mid=mid, items=items):
                    for item in items:
                        relay(mid, item)

    for layer in range(1, LAYERS):
        total = None
        for k in range(CHUNKS):
            total = gather_step(layer, layer, 0, k, total)
            relays()
        cells, scale = pool_step(layer, layer, 0, total)
        halo[layer, 1] = cells
        halo_start(layer)
        relays()
        cells = halo[layer, 1]
        sums = box_dot(1, cells)
        halo_wait(layer)
        sums = sums + box_dot(0, halo[layer, 0]) + box_dot(2, halo[layer, 2])
        share_pooled(layer, 0, sums, cells)
        relays()
        ready(layer, 2)
        back(layer, layer, 0)
        relays()
        if layer == 1:
            @pl.when(is_mid)
            def _(scale=scale):
                if not AGAIN_FIRST:
                    ready(1, 1)
                gate_of(1, 0, scale)

            @pl.when(is_end)
            def _():
                units(gv_recv.at[0], CHUNKS).wait_recv()
                for k in range(CHUNKS):
                    gate_buf[0, k] = gate_sent[k].astype(f32)
        else:
            ready(layer, 1)
            gate_of(layer, 0, scale)
        relays()
        for k in range(CHUNKS):
            state = update(layer, 0, k)
            if layer + 1 < LAYERS:
                gathered[layer + 1, t, k] = state
                start_gather(layer + 1, k)
            else:
                out_ref[:, k * cols_k:(k + 1) * cols_k] = state
            relays()

    def sent(sem, count):
        units(sem, count).wait_send()

    def sent_blocks(flow, k, most, least):
        @pl.when(c == blocks[k] % 2)
        def _():
            sent(w_send.at[flow], most)

        @pl.when(c != blocks[k] % 2)
        def _():
            sent(w_send.at[flow], least)

    def sent_chain(layers, slots, gathers):
        @pl.when(c != s_parity)
        def _():
            sent(bx_send.at[0], 2 * layers)
        sent(ag_send.at[0], 6 * gathers)
        sent(rs_send.at[0], 2 * slots)
        sent(px_send.at[0], slots)

    @pl.when(is_mid)
    def _():
        sent(w_send.at[0], 4 * LAYERS)
        sent(w_send.at[1], 4 * (LAYERS - 1) - 2)
        for k in range(3):
            sent_blocks(2 + k, k, 5 * LAYERS, 3 * LAYERS)
        for k in (1, 2):
            sent_blocks(4 + k, k, 5 * (LAYERS - 1) - 2, 3 * (LAYERS - 1) - 2)
        sent(rt_send.at[0], CHUNKS)
        sent(gv_send.at[0], CHUNKS)
        sent_chain(LAYERS, LAYERS + 1, LAYERS + 2)

    @pl.when(is_end)
    def _():
        sent(w_send.at[0], 4 * LAYERS)
        sent(w_send.at[1], 4 * LAYERS)
        for k in range(3):
            sent_blocks(2 + k, k, 5 * (LAYERS - 1) - 2, 3 * (LAYERS - 1) - 2)
        sent(tk_send.at[0], CHUNKS)
        sent_chain(LAYERS - 1, LAYERS - 1, LAYERS - 1)
    for layer in range(LAYERS):
        outward = layer > 0
        halo_do(layer, 0, (s < last) if outward else (s == 1), lambda x: x.wait_send())
        halo_do(layer, 1, (s > 0) if outward else (s == 2), lambda x: x.wait_send())


def fused(tokens_in, norm_gain, w_pool_in, w_gate, w_back):
    sp_count, tp_count = lax.axis_size("sp"), lax.axis_size("tp")
    toks, feats = tokens_in.shape
    _, depth, local_pool = w_pool_in.shape
    b_rows, b_cols = w_back.shape[1:]
    cols_k = feats // CHUNKS
    bf, f32 = jnp.bfloat16, jnp.float32
    dma = pltpu.SemaphoreType.DMA
    slots = LAYERS + 1
    hbm = pl.BlockSpec(memory_space=pltpu.HBM)
    return pl.pallas_call(
        functools.partial(fused_kernel, sp_count, tp_count),
        out_shape=pltpu.VMEM((toks, feats), bf),
        in_specs=[hbm] * 5,
        out_specs=pl.BlockSpec(memory_space=pltpu.VMEM),
        scratch_shapes=[
            pltpu.VMEM((LAYERS, sp_count * depth, local_pool), bf),
            pltpu.VMEM((LAYERS, sp_count * depth, w_gate.shape[2]), bf),
            pltpu.VMEM((LAYERS, 2, 2 * b_rows, b_cols), bf),
            pltpu.VMEM((LAYERS, b_rows, b_cols), bf),
            pltpu.VMEM((slots + 1, tp_count, CHUNKS, toks, cols_k), bf),
            pltpu.VMEM((2, toks, tp_count * feats), bf),
            pltpu.VMEM((LAYERS, 3, toks, local_pool), bf),
            pltpu.VMEM((2, CHUNKS, toks, cols_k), f32),
            pltpu.VMEM((2, CHUNKS, toks, cols_k), f32),
            pltpu.VMEM((3, toks, toks), bf),
            pltpu.VMEM((2, toks, local_pool), f32),
            pltpu.VMEM((slots, 2, toks, local_pool), bf),
            pltpu.VMEM((slots, CHUNKS, toks, cols_k), bf),
            pltpu.VMEM((slots, CHUNKS, toks, cols_k), bf),
            pltpu.VMEM((CHUNKS, toks, cols_k), bf),
            pltpu.VMEM(norm_gain.shape, f32),
            dma((LAYERS + 1, 4)),
            dma((7,)), dma((LAYERS, 3, 5)), dma((3, 2)), dma((LAYERS, 3)),
            dma((1,)), dma((LAYERS,)),
            dma((1,)), dma((CHUNKS,)), dma((1,)), dma((CHUNKS,)),
            dma((1,)), dma((slots + 1, 4)),
            dma((LAYERS, 2)), dma((LAYERS, 2)),
            dma((1,)), dma((slots,)),
            dma((1,)), dma((slots, CHUNKS)),
            dma((1,)), dma((1,)),
        ],
        compiler_params=pltpu.CompilerParams(
            collective_id=0, has_side_effects=True, vmem_limit_bytes=56 * 1024 * 1024
        ),
    )(tokens_in, norm_gain, w_pool_in, w_gate, w_back)

def dispatch(tokens_in, norm_gain, w_pool_in, w_gate, w_back):
    fits = (
        lax.axis_size("grp") == 2
        and lax.axis_size("tp") == GROUPS == 4
        and lax.axis_size("sp") == lax.axis_size("tp")
        and w_pool_in.shape[2] * GROUPS == POOL_WIDTH
        and w_pool_in.shape[1] == tokens_in.shape[1] == w_gate.shape[2] == w_back.shape[2]
        and tokens_in.shape[1] == 2 * tokens_in.shape[0] == 2 * w_pool_in.shape[2]
        and tokens_in.shape[0] // GRID_W >= max(pool_windows) // 2
    )
    step = fused if fits else on_device
    return step(tokens_in, norm_gain, w_pool_in, w_gate, w_back)


def solution(mesh):
    return jax.shard_map(
        dispatch,
        mesh=mesh,
        in_specs=(
            P(("grp", "sp"), "tp"),
            P(),
            P(None, "sp", "tp"),
            P(None, "sp", "tp"),
            P(None, "tp", "sp"),
        ),
        out_specs=P(("grp", "sp"), "tp"),
        check_vma=False,
    )
```
